32 devices in a mesh: sp: 4 (over z), fs: 4 (over y, x), tp: 2 (over core).
Axes of the slice: x: 2, y: 2, z: 4, core: 2. Of those that a mesh axis runs over, the one named last changes fastest.
Arguments:
- tokens: bfloat16 [4, 640, 2048], P('fs', 'sp', 'tp'), may hold values from -6 to 6
- mix_gain: float32 [2048], replicated, may hold values from 0.1 to 1.9
- conv_b_weight: bfloat16 [2048, 1024], P(('sp', 'fs'), 'tp'), may hold values from -0.125 to 0.125
- conv_c_weight: bfloat16 [2048, 1024], P(('sp', 'fs'), 'tp'), may hold values from -0.125 to 0.125
- conv_v_weight: bfloat16 [2048, 1024], P(('sp', 'fs'), 'tp'), may hold values from -0.125 to 0.125
- conv_taps: float32 [3, 1024], P(None, 'tp'), may hold values from -3.5 to 3.5
- query_weight: bfloat16 [2048, 2048], P(('sp', 'fs'), 'tp'), may hold values from -0.125 to 0.125
- query_rope_weight: bfloat16 [2048, 1024], P(('sp', 'fs'), 'tp'), may hold values from -4.5 to 4.5
- latent_weight: bfloat16 [2048, 512], P(('sp', 'fs')), may hold values from -0.125 to 0.125
- key_rope_weight: bfloat16 [2048, 64], replicated, may hold values from -1 to 1
- latent_gain: float32 [512], replicated, may hold values from 0.1 to 1.9
- key_up_weight: bfloat16 [512, 2048], P(None, 'tp'), may hold values from -0.25 to 0.25
- value_up_weight: bfloat16 [512, 2048], P(None, 'tp'), may hold values from -0.25 to 0.25
- head_gain: float32 [2048], P('tp'), may hold values from 0.1 to 1.9
- conv_out_weight: bfloat16 [1024, 2048], P('tp', ('sp', 'fs')), may hold values from -0.109375 to 0.109375
- attn_out_weight: bfloat16 [2048, 2048], P('tp', ('sp', 'fs')), may hold values from -0.109375 to 0.109375
Outputs:
- mixed: bfloat16 [4, 640, 2048], P('fs', ('sp', 'tp'))
The draws below stay inside these ranges and needn't reach their ends.
All inputs are finite; a program needn't handle non-finite values.
Results may differ from the reference program's by a relative error of at most 0.025.
Values may be sent and summed in bfloat16 or wider, within the bound.
A program may use at most 128 MiB of HBM per device.

```python
import math
import jax
import jax.numpy as jnp
from jax import lax

D = 2048
CONV = 1024
H = 16
NOPE = 128
ROPE = 64
VD = 128
KVL = 512
SEG = 64
SEQS = 4
LENGTH = 640
N_TP = 2


def rope_base(key):
    base = jax.random.normal(jax.random.fold_in(key, 101), (D, ROPE), jnp.float32)
    return jnp.clip(base, -4.0, 4.0) * D ** (-0.5)


def draw_key_rope_weight(key, part):
    return rope_base(key).astype(jnp.bfloat16)


def draw_query_rope_weight(key, part):
    fresh = jax.random.normal(jax.random.fold_in(key, 102), (D, H, ROPE), jnp.float32)
    fresh = jnp.clip(fresh, -4.0, 4.0) * D ** (-0.5)
    shaped = fresh
    return shaped.reshape(D, H * ROPE).astype(jnp.bfloat16)


def block_levels(rng, dims, split, least, high):
    loudness = 1.0
    for dim, parts in split:
        heights = jax.random.uniform(jax.random.fold_in(jax.random.fold_in(rng, 6), dim), (parts,), jnp.float32, least / len(split), high / len(split))
        loudness = loudness * jnp.repeat(jnp.exp(heights), dims[dim] // parts).reshape((-1,) + (1,) * (len(dims) - 1 - dim))
    return loudness


def bell_draw(stream_key, dims, width, bound, shards=(), kind=jnp.bfloat16):
    values = width * jax.random.normal(stream_key, dims, jnp.float32)
    if shards:
        values = values * block_levels(stream_key, dims, shards, -0.22, 0.18)
    return jnp.clip(values, -bound, bound).astype(kind)


def setup_inputs(seed: int = 0) -> dict:
    seeds = jax.random.split(jax.random.key(seed), 17)
    return {
        "tokens": bell_draw(seeds[0], (SEQS, LENGTH, D), 1.0, 6.0, ((0, 4), (1, 4), (2, 2))),
        "mix_gain": jnp.clip(1.0 + 0.18 * jax.random.normal(seeds[1], (D,), jnp.float32), 0.1, 1.9),
        "conv_b_weight": bell_draw(seeds[2], (D, CONV), D ** -0.5, 0.125, ((0, 16), (1, 2))),
        "conv_c_weight": bell_draw(seeds[3], (D, CONV), D ** -0.5, 0.125, ((0, 16), (1, 2))),
        "conv_v_weight": bell_draw(seeds[4], (D, CONV), D ** -0.5, 0.125, ((0, 16), (1, 2))),
        "conv_taps": bell_draw(seeds[5], (3, CONV), 3 ** -0.5, 3.5, ((1, 2),), jnp.float32),
        "query_weight": bell_draw(seeds[6], (D, H * NOPE), D ** -0.5, 0.125, ((0, 16), (1, 2))),
        "query_rope_weight": draw_query_rope_weight(jax.random.fold_in(seeds[16], 71), 0),
        "latent_weight": bell_draw(seeds[8], (D, KVL), D ** -0.5, 0.125, ((0, 16),)),
        "key_rope_weight": draw_key_rope_weight(jax.random.fold_in(seeds[16], 71), 0),
        "latent_gain": jnp.clip(1.0 + 0.18 * jax.random.normal(seeds[10], (KVL,), jnp.float32), 0.1, 1.9),
        "key_up_weight": bell_draw(seeds[11], (KVL, H * NOPE), KVL ** -0.5, 0.25, ((1, 2),)),
        "value_up_weight": bell_draw(seeds[12], (KVL, H * VD), KVL ** -0.5, 0.25, ((1, 2),)),
        "head_gain": jnp.clip(1.0 + 0.18 * jax.random.normal(seeds[13], (H * VD,), jnp.float32), 0.1, 1.9),
        "conv_out_weight": bell_draw(seeds[14], (CONV, D), (CONV + H * VD) ** -0.5, 0.109375, ((0, 2), (1, 16))),
        "attn_out_weight": bell_draw(seeds[15], (H * VD, D), (CONV + H * VD) ** -0.5, 0.109375, ((0, 2), (1, 16))),
    }


norm_epsilon = 1e-06
rope_theta = 10000.0

def rms_scale(values, gain):
    return values * lax.rsqrt(lax.optimization_barrier(jnp.mean(values * values, axis=-1, keepdims=True)) + norm_epsilon) * gain

def rope_tables(positions):
    half_width = ROPE // 2
    frequency = rope_theta ** (-jnp.arange(half_width, dtype=jnp.float32) * 2.0 / ROPE)
    angles = positions[:, None] * frequency[None, :]
    return (jnp.cos(angles), jnp.sin(angles))

def rotate(values, cosine, sine):
    half_width = ROPE // 2
    first = values[..., :half_width]
    second = values[..., half_width:]
    return jnp.concatenate([first * cosine - second * sine, second * cosine + first * sine], axis=-1)

def matmul(left, right):
    return jnp.dot(left, right, preferred_element_type=jnp.float32)

def one_sequence(sequence, mix_gain, conv_b_weight, conv_c_weight, conv_v_weight, conv_taps, query_weight, query_rope_weight, latent_weight, key_rope_weight, latent_gain, key_up_weight, value_up_weight, head_gain, conv_out_weight, attn_out_weight):
    length = sequence.shape[0]
    normed = rms_scale(sequence.astype(jnp.float32), mix_gain).astype(jnp.bfloat16)
    gate_b = matmul(normed, conv_b_weight).astype(jnp.bfloat16)
    gate_c = matmul(normed, conv_c_weight).astype(jnp.bfloat16)
    values_v = matmul(normed, conv_v_weight).astype(jnp.bfloat16)
    product = (gate_c.astype(jnp.float32) * values_v.astype(jnp.float32)).astype(jnp.bfloat16)
    padded = jnp.concatenate([jnp.zeros((2, CONV), jnp.bfloat16), product], axis=0).astype(jnp.float32)
    convolved = conv_taps[0] * padded[0:length] + conv_taps[1] * padded[1:length + 1] + conv_taps[2] * padded[2:length + 2]
    conv_y = (gate_b.astype(jnp.float32) * convolved).astype(jnp.bfloat16)
    positions = jnp.arange(length, dtype=jnp.float32)
    cosine, sine = rope_tables(positions)
    query_nope = matmul(normed, query_weight).astype(jnp.bfloat16).reshape(length, H, NOPE)
    query_rot = rotate(matmul(normed, query_rope_weight).reshape(length, H, ROPE), cosine[:, None, :], sine[:, None, :]).astype(jnp.bfloat16)
    latent_raw = matmul(normed, latent_weight).astype(jnp.bfloat16)
    latent = rms_scale(latent_raw.astype(jnp.float32), latent_gain).astype(jnp.bfloat16)
    key_rot = rotate(matmul(normed, key_rope_weight), cosine, sine).astype(jnp.bfloat16)
    query_latent = jnp.einsum('thn,khn->thk', query_nope.astype(jnp.float32), key_up_weight.reshape(KVL, H, NOPE).astype(jnp.float32)).astype(jnp.bfloat16)
    attn_scale = (NOPE + ROPE) ** (-0.5)
    block_rows = math.gcd(length, 512)
    latent_wide = latent.astype(jnp.float32)
    key_wide = key_rot.astype(jnp.float32)
    key_segment = jnp.arange(length, dtype=jnp.int32) // SEG

    def attend(block_index):
        begin_row = (block_index * block_rows).astype(jnp.int32)
        block_latent = lax.dynamic_slice_in_dim(query_latent, begin_row, block_rows, 0).astype(jnp.float32)
        block_rot = lax.dynamic_slice_in_dim(query_rot, begin_row, block_rows, 0).astype(jnp.float32)
        scores = (jnp.einsum('thk,jk->thj', block_latent, latent_wide) + jnp.einsum('thr,jr->thj', block_rot, key_wide)) * attn_scale
        query_segment = (begin_row + jnp.arange(block_rows, dtype=jnp.int32)) // SEG
        allowed = key_segment[None, None, :] <= query_segment[:, None, None]
        scores = jnp.where(allowed, scores, -1e+30)
        highest = lax.optimization_barrier(jnp.max(scores, axis=-1, keepdims=True))
        weights = jnp.where(allowed, jnp.exp(scores - highest), 0.0)
        summed = lax.optimization_barrier(jnp.sum(weights, axis=-1))
        numer = jnp.einsum('thj,jk->thk', weights.astype(jnp.bfloat16).astype(jnp.float32), latent_wide)
        return (numer / summed[..., None]).astype(jnp.bfloat16)
    attended = lax.map(attend, jnp.arange(length // block_rows, dtype=jnp.int32)).reshape(length, H, KVL)
    head_out = jnp.einsum('thk,khv->thv', attended.astype(jnp.float32), value_up_weight.reshape(KVL, H, VD).astype(jnp.float32))
    attn_y = rms_scale(head_out, head_gain.reshape(H, VD)).astype(jnp.bfloat16).reshape(length, H * VD)
    conv_share = CONV // N_TP
    head_share = H * VD // N_TP
    combined = jnp.zeros((length, D), jnp.float32)
    for share in range(N_TP):
        conv_cols = slice(share * conv_share, (share + 1) * conv_share)
        head_cols = slice(share * head_share, (share + 1) * head_share)
        partial_out = matmul(conv_y[:, conv_cols], conv_out_weight[conv_cols]) + matmul(attn_y[:, head_cols], attn_out_weight[head_cols])
        rounded = lax.optimization_barrier(partial_out.astype(jnp.bfloat16))
        combined = combined + rounded.astype(jnp.float32)
    return combined.astype(jnp.bfloat16)

def reference(tokens, mix_gain, conv_b_weight, conv_c_weight, conv_v_weight, conv_taps, query_weight, query_rope_weight, latent_weight, key_rope_weight, latent_gain, key_up_weight, value_up_weight, head_gain, conv_out_weight, attn_out_weight):
    results = []
    for sequence_index in range(SEQS):
        results.append(one_sequence(tokens[sequence_index], mix_gain, conv_b_weight, conv_c_weight, conv_v_weight, conv_taps, query_weight, query_rope_weight, latent_weight, key_rope_weight, latent_gain, key_up_weight, value_up_weight, head_gain, conv_out_weight, attn_out_weight))
    return jnp.stack(results, axis=0)
```

```python
import functools
import math

import jax
import jax.numpy as jnp
from jax import lax
from jax.experimental import pallas as pl
from jax.experimental.pallas import tpu as pltpu
from jax.sharding import PartitionSpec as P

NOPE = 128
ROPE = 64
VD = 128
KVL = 512
SEG = 64


norm_epsilon = 1e-06
rope_theta = 10000.0


def passed_along(block, axis, distance):
    devices = range(lax.axis_size(axis))
    route = [(i - distance, i) for i in devices if i - distance in devices]
    return lax.ppermute(block, axis, route)


def rms_scale(values, gain):
    return (
        values * lax.rsqrt(jnp.mean(values * values, axis=-1, keepdims=True) + norm_epsilon) * gain
    )


def rope_tables(positions):
    half_width = ROPE // 2
    frequency = rope_theta ** (-jnp.arange(half_width, dtype=jnp.float32) * 2.0 / ROPE)
    angles = positions[:, None] * frequency[None, :]
    return (jnp.cos(angles), jnp.sin(angles))


def rotate(values, cosine, sine):
    half_width = ROPE // 2
    first = values[..., :half_width]
    second = values[..., half_width:]
    return jnp.concatenate(
        [first * cosine - second * sine, second * cosine + first * sine], axis=-1
    )


def general_shards(
    tokens,
    mix_gain,
    conv_b_weight,
    conv_c_weight,
    conv_v_weight,
    conv_taps,
    query_weight,
    query_rope_weight,
    latent_weight,
    key_rope_weight,
    latent_gain,
    key_up_weight,
    value_up_weight,
    head_gain,
    conv_out_weight,
    attn_out_weight,
):
    full_rows = lax.all_gather(tokens[0], "tp", axis=1, tiled=True)
    tok_rows = full_rows.shape[0]
    normed = rms_scale(full_rows.astype(jnp.float32), mix_gain).astype(jnp.bfloat16)
    offset = lax.axis_index("sp") * tok_rows
    token_index = offset + jnp.arange(tok_rows, dtype=jnp.int32)
    cosine, sine = rope_tables(token_index.astype(jnp.float32))
    local_heads = query_weight.shape[1] // NOPE
    count_sp = lax.axis_size("sp")
    count_fs = lax.axis_size("fs")
    count_tp = lax.axis_size("tp")
    fs_index = lax.axis_index("fs")
    row_piece = normed.shape[1] // (count_sp * count_fs)
    all_normed = lax.all_gather(normed, "fs", axis=0, tiled=True)
    picked = lax.dynamic_index_in_dim(
        all_normed.reshape(-1, count_sp, count_fs, row_piece), fs_index, 2, keepdims=False
    ).reshape(-1, count_sp * row_piece)
    gathered = (
        lax.all_gather(conv_b_weight, "sp", axis=0, tiled=True),
        lax.all_gather(conv_c_weight, "sp", axis=0, tiled=True),
        lax.all_gather(conv_v_weight, "sp", axis=0, tiled=True),
        lax.all_gather(query_weight, "sp", axis=0, tiled=True),
        lax.all_gather(query_rope_weight, "sp", axis=0, tiled=True),
        lax.all_gather(latent_weight, "sp", axis=0, tiled=True),
    )

    def project_in():
        return jnp.concatenate(
            [jnp.dot(picked, member, preferred_element_type=jnp.float32) for member in gathered],
            axis=1,
        )

    joined = lax.psum_scatter(
        project_in().astype(jnp.bfloat16), "fs", scatter_dimension=0, tiled=True
    ).astype(jnp.float32)
    bounds = []
    running_total = 0
    for member in gathered[:-1]:
        running_total = running_total + member.shape[1]
        bounds.append(running_total)
    sums = tuple(jnp.split(joined, bounds, axis=1))
    latent_raw = sums[5].astype(jnp.bfloat16)
    gate_b = sums[0].astype(jnp.bfloat16)
    gate_c = sums[1].astype(jnp.bfloat16)
    values_v = sums[2].astype(jnp.bfloat16)
    query_nope = sums[3].astype(jnp.bfloat16).reshape(tok_rows, local_heads, NOPE)
    query_rot = rotate(
        sums[4].reshape(tok_rows, local_heads, ROPE), cosine[:, None, :], sine[:, None, :]
    ).astype(jnp.bfloat16)
    latent = rms_scale(latent_raw.astype(jnp.float32), latent_gain).astype(jnp.bfloat16)
    key_rot = rotate(
        jnp.dot(normed, key_rope_weight, preferred_element_type=jnp.float32), cosine, sine
    ).astype(jnp.bfloat16)
    query_latent = jnp.einsum(
        "thn,khn->thk",
        query_nope,
        key_up_weight.reshape(KVL, local_heads, NOPE),
        preferred_element_type=jnp.float32,
    ).astype(jnp.bfloat16)
    attn_scale = (NOPE + ROPE) ** (-0.5)
    product = (gate_c.astype(jnp.float32) * values_v.astype(jnp.float32)).astype(jnp.bfloat16)
    previous = passed_along(product[tok_rows - 2 :], "sp", 1)
    padded = jnp.concatenate([previous, product], axis=0).astype(jnp.float32)
    convolved = (
        conv_taps[0] * padded[0:tok_rows]
        + conv_taps[1] * padded[1 : tok_rows + 1]
        + conv_taps[2] * padded[2 : tok_rows + 2]
    )
    conv_y = (gate_b.astype(jnp.float32) * convolved).astype(jnp.bfloat16)
    query_segment = token_index // SEG
    last_segment = (offset + tok_rows - 1) // SEG

    def key_block(running, latent_block, rot_block, first_key):
        peak_old, denom_old, accum_old = running
        block_rows = latent_block.shape[0]
        scores = (
            jnp.einsum(
                "thk,jk->thj", query_latent, latent_block, preferred_element_type=jnp.float32
            )
            + jnp.einsum("thr,jr->thj", query_rot, rot_block, preferred_element_type=jnp.float32)
        ) * attn_scale
        key_segment = (first_key + jnp.arange(block_rows, dtype=jnp.int32)) // SEG
        allowed = key_segment[None, None, :] <= query_segment[:, None, None]
        peak_new = jnp.maximum(peak_old, jnp.max(jnp.where(allowed, scores, -1e30), axis=-1))
        weights = jnp.where(allowed, jnp.exp(scores - peak_new[..., None]), 0.0)
        rescale = jnp.exp(peak_old - peak_new)
        denom_new = denom_old * rescale + jnp.sum(weights, axis=-1)
        accum_new = accum_old * rescale[..., None] + jnp.einsum(
            "thj,jk->thk",
            weights.astype(jnp.bfloat16),
            latent_block,
            preferred_element_type=jnp.float32,
        )
        return (peak_new, denom_new, accum_new)

    starting = (
        jnp.full((tok_rows, local_heads), -1e30, jnp.float32),
        jnp.zeros((tok_rows, local_heads), jnp.float32),
        jnp.zeros((tok_rows, local_heads, KVL), jnp.float32),
    )
    latent_piece = lax.all_gather(latent, "sp", axis=0, tiled=True)
    rot_piece = lax.all_gather(key_rot, "sp", axis=0, tiled=True)
    piece_rows = latent_piece.shape[0]
    splits = max(1, piece_rows // 512)
    while piece_rows % splits:
        splits = splits - 1
    block_rows = piece_rows // splits

    def visit(state, block_index):
        block_begin = block_index * block_rows
        latent_block = lax.dynamic_slice_in_dim(latent_piece, block_begin, block_rows, 0)
        rot_block = lax.dynamic_slice_in_dim(rot_piece, block_begin, block_rows, 0)
        updated = lax.cond(
            block_begin // SEG <= last_segment,
            lambda inner: key_block(inner, latent_block, rot_block, block_begin),
            lambda inner: inner,
            state,
        )
        return (updated, None)

    peak, denom, accum = lax.scan(visit, starting, jnp.arange(splits, dtype=jnp.int32))[0]
    attended = (accum / denom[..., None]).astype(jnp.bfloat16)
    head_out = jnp.einsum(
        "thk,khv->thv",
        attended,
        value_up_weight.reshape(KVL, local_heads, VD),
        preferred_element_type=jnp.float32,
    )
    normed_heads = rms_scale(head_out, head_gain.reshape(local_heads, VD))
    attn_y = normed_heads.astype(jnp.bfloat16).reshape(tok_rows, local_heads * VD)
    share_rows = tok_rows // count_tp
    conv_all, attn_all = (
        lax.all_gather(conv_y, "fs", axis=0, tiled=True),
        lax.all_gather(attn_y, "fs", axis=0, tiled=True),
    )
    conv_sorted = (
        conv_all.reshape(count_fs, count_tp, share_rows, -1)
        .transpose(1, 0, 2, 3)
        .reshape(count_fs * tok_rows, -1)
    )
    attn_sorted = (
        attn_all.reshape(count_fs, count_tp, share_rows, -1)
        .transpose(1, 0, 2, 3)
        .reshape(count_fs * tok_rows, -1)
    )
    conv_cols_sp, attn_cols_sp = (
        lax.all_gather(conv_out_weight, "sp", axis=1, tiled=True),
        lax.all_gather(attn_out_weight, "sp", axis=1, tiled=True),
    )
    col_sums = lax.psum_scatter(
        (
            jnp.dot(conv_sorted, conv_cols_sp, preferred_element_type=jnp.float32)
            + jnp.dot(attn_sorted, attn_cols_sp, preferred_element_type=jnp.float32)
        ).astype(jnp.bfloat16),
        "tp",
        scatter_dimension=0,
        tiled=True,
    )
    col_piece = conv_cols_sp.shape[1] // count_sp
    outgoing = col_sums.reshape(count_fs, share_rows, count_sp * col_piece)
    arrived = lax.all_to_all(outgoing, "fs", split_axis=0, concat_axis=2, tiled=True)
    result = (
        arrived.reshape(share_rows, count_fs, count_sp, col_piece)
        .transpose(0, 2, 1, 3)
        .reshape(share_rows, count_fs * count_sp * col_piece)
    )
    return result[None]


MESH = pl.DeviceIdType.MESH


class Place:
    def __init__(self):
        self.z = lax.axis_index("sp")
        self.f = lax.axis_index("fs")
        self.c = lax.axis_index("tp")

    def to(self, z=None, f=None, c=None):
        return {
            "sp": self.z if z is None else z,
            "fs": self.f if f is None else f,
            "tp": self.c if c is None else c,
        }


def flip(index, bit):
    digit = (index // bit) % 2
    return index + bit * (1 - 2 * digit)


def remote(src, dst, send, recv, device):
    return pltpu.make_async_remote_copy(
        src_ref=src, dst_ref=dst, send_sem=send, recv_sem=recv, device_id=device, device_id_type=MESH
    )


def greet(devices):
    barrier = pltpu.get_barrier_semaphore()
    for device in devices:
        pl.semaphore_signal(barrier, inc=1, device_id=device, device_id_type=MESH)
    pl.semaphore_wait(barrier, len(devices))


def orders(n):
    arrival, compute, passing = [], [], []
    for z in range(n):
        first = z + 1 if z < n - 1 else z - 1
        far = sorted((d for d in range(n) if d != z), key=lambda d: (-abs(d - z), min(d, n - 1 - d)))
        arrival.append(sorted(range(n), key=lambda d: (abs(d - z), d)))
        compute.append([first] + sorted((d for d in far if d != first), key=lambda d: -abs(d - z)) + [z])
        passing.append(far)
    return arrival, compute, passing


def layer_kernel(
    n,
    parts,
    order,
    tok_in,
    mix_gain_in,
    lat_gain_in,
    head_gain_in,
    taps_in,
    cb,
    cc,
    cv,
    qw,
    qr,
    lw,
    krw_in,
    key_up_in,
    value_up_in,
    co,
    ao,
    out,
    tok,
    normed,
    win,
    wout,
    wlat,
    lat,
    krot,
    gain,
    krw,
    taps,
    lat_gain,
    key_up,
    value_up,
    head_gain,
    gate,
    prod,
    q_nope,
    q_rot,
    keys,
    values,
    cosine,
    sine,
    part,
    pair,
    moving,
    fetched,
    wsem,
    fsem,
    lsem,
    tsem,
    psem,
    latsem,
    ssem,
    pairsem,
    zsem,
):
    here = Place()
    z, f, c = here.z, here.f, here.c
    fx, fy = flip(f, 1), flip(f, 2)
    other = 1 - c
    is_end = (z == 0) | (z == n - 1)
    rows = cb.shape[0]
    members = (cb, cc, cv, qw, qr)
    widths = [m.shape[1] // n for m in members]
    starts = [sum(widths[:i]) for i in range(len(widths))]
    lat_half = lw.shape[1] // 2
    tr = tok_in.shape[1]
    hr = tr // 2
    length = n * tr
    outs = (co, ao)
    heights = [m.shape[0] // n for m in outs]
    tops = [sum(heights[:i]) for i in range(len(heights))]
    out_cols = co.shape[1]
    head_rows = prod.shape[0] - length

    steps = [(1 + j, s) for j in range(n - 1) for s in (-1, 1)]

    def chosen(table, t):
        found = jnp.int32(0)
        for zz in range(n):
            for tt in range(len(table[zz])):
                found = jnp.where((z == zz) & (t == tt), table[zz][tt], found)
        return found

    def arrive_at(t):
        return chosen(order[0], t)

    def turn_of(t):
        return chosen(order[1], t)

    def pass_of(t):
        return chosen(order[2], t)

    greet(
        [here.to(z=lax.rem(z + j, n)) for j in range(1, n)]
        + [here.to(f=fx), here.to(f=fy), here.to(c=other)]
    )

    def in_block(zs, fs):
        return win.at[pl.ds(pl.multiple_of((zs * 4 + fs) * rows, rows), rows), :]

    def out_block(zs, fs):
        return wout.at[:, pl.ds(pl.multiple_of((zs * 4 + fs) * out_cols, out_cols), out_cols)]

    def low_block(zs, fs):
        return wlat.at[pl.ds(pl.multiple_of((zs * 4 + fs) * rows, rows), rows), :]

    blocks = (in_block, out_block, low_block)

    def pieces(kind, dest):
        found = []
        if kind == 0:
            dst = (z * 4 + f) * rows
            for m, w, s in zip(members, widths, starts):
                src = m.at[:, pl.ds(pl.multiple_of(dest * w, w), w)]
                found.append((src, win.at[pl.ds(pl.multiple_of(dst, rows), rows), pl.ds(s, w)]))
        elif kind == 1:
            dst = (z * 4 + f) * out_cols
            for m, h, s in zip(outs, heights, tops):
                src = m.at[pl.ds(pl.multiple_of(dest * h, h), h), :]
                found.append((src, wout.at[pl.ds(s, h), pl.ds(pl.multiple_of(dst, out_cols), out_cols)]))
        else:
            found.append((lw.at[:, pl.ds(pl.multiple_of(c * lat_half, lat_half), lat_half)], low_block(z, f)))
        return found

    def send_own(kind):
        for src, dst in pieces(kind, z):
            remote(src, dst, wsem.at[kind, 2, z], wsem.at[kind, 3, z], here.to(f=fx)).start()
            remote(src, dst, wsem.at[kind, 4, z], wsem.at[kind, 5, z], here.to(f=fy)).start()
            pltpu.make_async_copy(src, dst, lsem.at[kind]).start()

    def can(sign):
        return (z + sign >= 0) & (z + sign < n)

    def within(zs):
        return (zs >= 0) & (zs < n)

    def reached(distance, sign):
        dest = z + sign * distance
        if distance == 1:
            return within(dest)
        return (dest > 0) & (dest < n - 1)

    def serves(sign):
        return z + sign == (n - 1 if sign > 0 else 0)

    def send_z(kind, distance, sign):
        dest = z + sign * distance

        @pl.when(reached(distance, sign) if kind == 2 else within(dest))
        def _():
            for src, dst in pieces(kind, dest):
                remote(src, dst, wsem.at[kind, 0, dest], wsem.at[kind, 1, z], here.to(z=dest)).start()

    def plane_copy(kind, zs, role, fs, to):
        block = blocks[kind](zs, fs)
        return remote(block, block, wsem.at[kind, role, zs], wsem.at[kind, role + 1, zs], here.to(f=to))

    def end_copy(zs, sign):
        block = low_block(zs, f)
        return remote(block, block, fsem.at[zs], wsem.at[2, 1, zs], here.to(z=z + sign))

    def relay_z(kind, distance, sign):
        zs = z + sign * distance

        @pl.when(within(zs))
        def _():
            block = blocks[kind](zs, f)
            remote(block, block, wsem.at[kind, 0, zs], wsem.at[kind, 1, zs], here.to(z=zs)).wait_recv()
            if kind == 2:
                pl.when(serves(-sign))(lambda: end_copy(zs, -sign).start())
            plane_copy(kind, zs, 2, f, fx).start()
            plane_copy(kind, zs, 4, f, fy).start()

    def relay_plane(kind, zs):
        plane_copy(kind, zs, 2, fx, fx).wait_recv()

        @pl.when(zs % 2 == 0)
        def _():
            plane_copy(kind, zs, 6, fx, fy).start()

        plane_copy(kind, zs, 4, fy, fy).wait_recv()

        @pl.when(zs % 2 == 1)
        def _():
            plane_copy(kind, zs, 6, fy, fx).start()

    def relay_done(kind, zs):
        plane_copy(kind, zs, 6, flip(fx, 2), fx).wait_recv()

    def tok_block(owner, zs, i):
        return tok.at[owner, pl.ds(pl.multiple_of(zs * tr + i * hr, hr), hr), :]

    own_tok = [tok_in.at[0, i * hr : (i + 1) * hr, :] for i in range(2)]

    def tok_copy(zs, sign, hop, i, src=None):
        d = (sign + 1) // 2
        block = tok_block(c, zs, i)
        return remote(
            block if src is None else src, block, tsem.at[d, 0, hop, i], tsem.at[d, 1, hop, i], here.to(z=z + sign)
        )

    def partner_copy(zs, owner, i, src=None):
        block = tok_block(owner, zs, i)
        return remote(
            block if src is None else src, block, psem.at[0, zs, i], psem.at[1, zs, i], here.to(c=other)
        )

    def own_copy(i):
        return pltpu.make_async_copy(own_tok[i], tok_block(c, z, i), lsem.at[3 + i])

    channels = widths[0]
    heads = widths[3] // NOPE
    rot_w = widths[4]
    share = tr // 2

    def columns_of(array, width):
        return array.at[:, pl.ds(pl.multiple_of(z * width, width), width)]

    small = [
        (mix_gain_in, gain.at[0:1, :]),
        (krw_in, krw.at[0:ROPE, :]),
        (krw_in, krw.at[ROPE : 2 * ROPE, :]),
        (taps_in, taps),
        (lat_gain_in, lat_gain.at[0:1, :]),
        (columns_of(key_up_in, heads * NOPE), key_up),
        (columns_of(value_up_in, heads * VD), value_up),
        (columns_of(head_gain_in, heads * VD), head_gain.at[0:1, :]),
    ]

    send_own(2)
    for distance, sign in steps:
        send_z(2, distance, sign)
    for i in range(2):
        partner_copy(z, c, i, own_tok[i]).start()
        own_copy(i).start()
    for kind in (0, 1):
        send_own(kind)

    def send_inward(kind, distance, sign):
        pl.when(jnp.logical_not(serves(sign)))(lambda: send_z(kind, distance, sign))

    def send_outward(kind, sign):
        pl.when(serves(sign))(lambda: send_z(kind, 1, sign))

    def send_tok(sign):
        for i in range(2):
            pl.when(can(sign))(lambda i=i: tok_copy(z, sign, 0, i, own_tok[i]).start())

    for kind in (0, 1):
        for distance, sign in steps:
            send_inward(kind, distance, sign)
    for sign in (-1, 1):
        pl.when(jnp.logical_not(serves(sign)))(lambda sign=sign: send_tok(sign))
    for i, (src, dst) in enumerate(small):
        pltpu.make_async_copy(src, dst, ssem.at[i]).start()

    def relay_tok(distance, sign, i):
        zs = z + sign * distance

        @pl.when(within(zs))
        def _():
            tok_copy(zs, -sign, distance - 1, i).wait_recv()
            if distance < n - 1:
                pl.when(can(-sign))(lambda: tok_copy(zs, -sign, distance, i).start())
            partner_copy(zs, c, i).start()

    def relay_toks(distance):
        for i in range(2):
            for sign in (-1, 1):
                relay_tok(distance, sign, i)

    def each_zs(fn):
        def body(i, carry):
            fn(lax.rem(z + i, n))
            return carry

        lax.fori_loop(0, n, body, 0)

    def at_distance(distance, fn):
        for sign in (-1, 1):
            zs = z + sign * distance
            pl.when(within(zs))(lambda zs=zs: fn(zs))

    lane = lax.broadcasted_iota(jnp.int32, (tr, rot_w), 1)
    quarter = lane % (ROPE // 2)
    first_half = (lane % ROPE) < ROPE // 2
    frequency = jnp.exp(quarter.astype(jnp.float32) * (-2.0 / ROPE * math.log(rope_theta)))

    def tables(i, carry):
        at = pl.ds(pl.multiple_of(i * tr, tr), tr)
        position = (i * tr + lax.broadcasted_iota(jnp.int32, (tr, rot_w), 0)).astype(jnp.float32)
        angle = position * frequency
        cosine[at, :] = jnp.cos(angle)
        turned = jnp.sin(angle)
        sine[at, :] = jnp.where(first_half, -turned, turned)
        return carry

    lax.fori_loop(0, n, tables, 0)
    prod[0:head_rows, :] = jnp.zeros((head_rows, channels), prod.dtype)

    def rotated(x, at):
        swapped = jnp.where(
            first_half, pltpu.roll(x, rot_w - ROPE // 2, 1), pltpu.roll(x, ROPE // 2, 1)
        )
        return (x * cosine[at, :] + swapped * sine[at, :]).astype(jnp.bfloat16)

    for i, (src, dst) in enumerate(small):
        pltpu.make_async_copy(src, dst, ssem.at[i]).wait()
    wide = tok.shape[2]

    def norm_block(zs):
        for i in range(2):
            partner_copy(zs, other, i).wait_recv()

        def norm_chunk(i, carry):
            at = pl.ds(pl.multiple_of(zs * tr + i * hr, hr), hr)
            first = tok[0, at, :].astype(jnp.float32)
            second = tok[1, at, :].astype(jnp.float32)
            mean = (
                jnp.sum(first * first, axis=-1, keepdims=True)
                + jnp.sum(second * second, axis=-1, keepdims=True)
            ) / (2 * wide)
            scale = lax.rsqrt(mean + norm_epsilon)
            normed[at, 0:wide] = (first * scale * gain[0:1, 0:wide]).astype(jnp.bfloat16)
            normed[at, wide : 2 * wide] = (second * scale * gain[0:1, wide : 2 * wide]).astype(jnp.bfloat16)
            return carry

        lax.fori_loop(0, 2, norm_chunk, 0)

    def rows_of(zs):
        return pl.ds(pl.multiple_of(zs * tr, tr), tr)

    def lat_block(zs, owner):
        return lat.at[owner, rows_of(zs), :]

    def rot_block(zs, owner):
        return krot.at[pl.ds(pl.multiple_of(zs * tr + owner * hr, hr), hr), :]

    shared = (lat_block, rot_block)

    def lat_copy(k, dest):
        block = shared[k](z, c)
        return remote(block, block, latsem.at[k, 0, dest], latsem.at[k, 1, z], here.to(z=dest))

    def lat_arrival(k, zs):
        block = shared[k](zs, c)
        return remote(block, block, latsem.at[k, 0, zs], latsem.at[k, 1, zs], here.to(z=zs))

    def lat_forward(k, zs, sign):
        block = shared[k](zs, c)
        return remote(block, block, latsem.at[k, 4, zs], latsem.at[k, 1, zs], here.to(z=z + sign))

    def lat_partner(k, zs, owner):
        block = shared[k](zs, owner)
        return remote(block, block, latsem.at[k, 2, zs], latsem.at[k, 3, zs], here.to(c=other))

    def relay_lat(distance):
        for sign in (-1, 1):
            zs = z + sign * distance

            @pl.when(within(zs))
            def _(zs=zs, sign=sign):
                for k in range(2):
                    lat_arrival(k, zs).wait_recv()
                    pl.when(serves(-sign))(lambda k=k: lat_forward(k, zs, -sign).start())
                    lat_partner(k, zs, c).start()

    def own_latents():
        at = rows_of(z)
        block = normed[at, :]
        lat[c, at, :] = jnp.dot(block, wlat[...], preferred_element_type=jnp.float32).astype(jnp.bfloat16)
        key_raw = lax.dot_general(
            block, krw[...], (((1,), (1,)), ((), ())), preferred_element_type=jnp.float32
        )
        krot[at, :] = rotated(key_raw, at)

    def relay_weights_z(distance):
        for sign in (-1, 1):
            for kind in (0, 1):
                relay_z(kind, distance, sign)

    def relay_weights_plane(zs):
        for kind in (0, 1):
            relay_plane(kind, zs)

    for sign in (-1, 1):
        relay_z(2, 1, sign)
    relay_plane(2, z)
    pl.when(jnp.logical_not(is_end))(lambda: [relay_z(2, 2, sign) for sign in (-1, 1)] and None)
    for sign in (-1, 1):
        for kind in (0, 1):
            send_outward(kind, sign)
        pl.when(serves(sign))(lambda sign=sign: send_tok(sign))
    for i in range(2):
        own_copy(i).wait()
    norm_block(z)
    pl.when(is_end)(lambda: [relay_z(2, 2, sign) for sign in (-1, 1)] and None)
    for distance in range(3, n):
        for sign in (-1, 1):
            relay_z(2, distance, sign)
    relay_plane(0, z)
    relay_plane(1, z)
    for sign in (-1, 1):
        relay_z(0, 1, sign)
    for distance in range(1, n):
        at_distance(distance, lambda zs: relay_plane(2, zs))
    for sign in (-1, 1):
        relay_z(0, 2, sign)
    at_distance(1, lambda zs: relay_plane(0, zs))
    pltpu.make_async_copy(low_block(z, f), low_block(z, f), lsem.at[2]).wait()
    each_zs(lambda zs: relay_done(2, zs))
    own_latents()
    for distance, sign in steps:
        dest = z + sign * distance

        @pl.when(reached(distance, sign))
        def _(dest=dest):
            for k in range(2):
                lat_copy(k, dest).start()

    lat_partner(0, z, c).start()
    for distance in range(3, n):
        for sign in (-1, 1):
            relay_z(0, distance, sign)
    for sign in (-1, 1):
        relay_z(1, 1, sign)
    for sign in (-1, 1):
        relay_z(1, 2, sign)
    at_distance(2, lambda zs: relay_plane(0, zs))
    for distance in range(3, n):
        for sign in (-1, 1):
            relay_z(1, distance, sign)
    relay_toks(1)
    at_distance(1, lambda zs: relay_plane(1, zs))
    norm_block(arrive_at(1))
    relay_lat(1)
    for distance in range(3, n):
        at_distance(distance, lambda zs: relay_plane(0, zs))
    at_distance(2, lambda zs: relay_plane(1, zs))
    relay_lat(2)
    relay_toks(2)
    for distance in range(3, n):
        at_distance(distance, lambda zs: relay_plane(1, zs))
        relay_lat(distance)
    for t in range(2, n - 1):
        norm_block(arrive_at(t))

    def lat_waits(zs):
        lat_partner(0, zs, other).wait_recv()
        pl.when(zs != z)(lambda: lat_partner(1, zs, other).wait_recv())

    def expand(i, carry):
        lat_waits(i)
        at = rows_of(i)
        raw = jnp.concatenate([lat[0, at, :], lat[1, at, :]], axis=1).astype(jnp.float32)
        mean = jnp.mean(raw * raw, axis=-1, keepdims=True)
        low = (raw * lax.rsqrt(mean + norm_epsilon) * lat_gain[0:1, :]).astype(jnp.bfloat16)
        wide_keys = jnp.dot(low, key_up[...], preferred_element_type=jnp.float32).astype(jnp.bfloat16)
        key_rot = krot[at, :]
        for h in range(heads):
            keys[h, at, 0:NOPE] = wide_keys[:, h * NOPE : (h + 1) * NOPE]
            keys[h, at, NOPE:] = key_rot
        values[at, :] = jnp.dot(low, value_up[...], preferred_element_type=jnp.float32).astype(jnp.bfloat16)
        return carry

    lax.fori_loop(0, n, expand, 0)
    for kind in (0, 1):
        pltpu.make_async_copy(blocks[kind](z, f), blocks[kind](z, f), lsem.at[kind]).wait()
    each_zs(lambda zs: [relay_done(kind, zs) for kind in (0, 1)] and None)

    def project(zs):
        at = rows_of(zs)
        joined = jnp.dot(normed[at, :], win[...], preferred_element_type=jnp.float32)
        gates = joined[:, channels : 3 * channels].astype(jnp.bfloat16).astype(jnp.float32)
        gate[at, :] = joined[:, 0:channels].astype(jnp.bfloat16)
        below = pl.ds(pl.multiple_of(zs * tr + head_rows, head_rows), tr)
        prod[below, :] = (gates[:, 0:channels] * gates[:, channels : 2 * channels]).astype(jnp.bfloat16)
        start = 3 * channels
        q_nope[at, :] = joined[:, start : start + heads * NOPE].astype(jnp.bfloat16)
        q_rot[at, :] = rotated(joined[:, start + heads * NOPE :], at)

    shift = SEG.bit_length() - 1
    row_index = lax.broadcasted_iota(jnp.int32, (tr, length), 0)
    key_segment = jnp.right_shift(lax.broadcasted_iota(jnp.int32, (tr, length), 1), shift)
    own_lanes = lane // ROPE
    own_channels = pl.ds(pl.multiple_of(z * channels, channels), channels)

    def block_output(dest):
        at = rows_of(dest)
        allowed = key_segment <= jnp.right_shift(row_index + dest * tr, shift)
        padded = prod[pl.ds(pl.multiple_of(dest * tr, head_rows), tr + head_rows), :].astype(jnp.float32)
        convolved = (
            taps[0:1, own_channels] * pltpu.roll(padded, 2, 0)[head_rows:]
            + taps[1:2, own_channels] * pltpu.roll(padded, 1, 0)[head_rows:]
            + taps[2:3, own_channels] * padded[head_rows:]
        )
        outputs = [(gate[at, :].astype(jnp.float32) * convolved).astype(jnp.bfloat16)]
        rot = q_rot[at, :]
        for h in range(heads):
            query = jnp.concatenate(
                [
                    q_nope[at, h * NOPE : (h + 1) * NOPE],
                    jnp.where(own_lanes == h, rot, jnp.zeros_like(rot)),
                ],
                axis=1,
            )
            scores = lax.dot_general(
                query, keys[h], (((1,), (1,)), ((), ())), preferred_element_type=jnp.float32
            ) * (NOPE + ROPE) ** (-0.5)
            scores = jnp.where(allowed, scores, -1e30)
            weights = jnp.exp(scores - jnp.max(scores, axis=-1, keepdims=True))
            denom = jnp.sum(weights, axis=-1, keepdims=True)
            head_out = (
                jnp.dot(
                    weights.astype(jnp.bfloat16),
                    values[:, h * VD : (h + 1) * VD],
                    preferred_element_type=jnp.float32,
                )
                / denom
            )
            mean = jnp.mean(head_out * head_out, axis=-1, keepdims=True)
            gained = head_out * lax.rsqrt(mean + norm_epsilon) * head_gain[0:1, h * VD : (h + 1) * VD]
            outputs.append(gained.astype(jnp.bfloat16))
        mixed = jnp.concatenate(outputs, axis=1)
        part[dest] = jnp.dot(mixed, wout[...], preferred_element_type=jnp.float32).astype(jnp.bfloat16)

    def part_rows(dest, core):
        return part.at[dest, pl.ds(pl.multiple_of(core * share, share), share), :]

    def pair_copy(dest):
        return remote(
            part_rows(dest, other), pair.at[dest], pairsem.at[0, dest], pairsem.at[1, dest], here.to(c=other)
        )

    piece_w = out.shape[1] // parts

    def cut(g):
        return slice(g * piece_w, (g + 1) * piece_w)

    def line_copy(d, dest, g):
        return remote(
            moving.at[dest, :, cut(g)],
            fetched.at[d, dest, :, cut(g)],
            zsem.at[d, 0, dest, g],
            zsem.at[d, 1, dest, g],
            here.to(z=z + 2 * d - 1),
        )

    def summed(dest, g):
        kept = part[dest, pl.ds(pl.multiple_of(c * share, share), share), cut(g)]
        return kept.astype(jnp.float32) + pair[dest, :, cut(g)].astype(jnp.float32)

    def toward(dest):
        return jnp.where(dest > z, 1, 0)

    def pass_first(dest):
        pair_copy(dest).wait_recv()
        for g in range(parts):
            moving[dest, :, cut(g)] = summed(dest, g).astype(jnp.bfloat16)
            line_copy(toward(dest), dest, g).start()

    def pass_on(dest):
        d = toward(dest)
        pair_copy(dest).wait_recv()
        for g in range(parts):
            line_copy(d, dest, g).wait_recv()
            moving[dest, :, cut(g)] = (
                summed(dest, g) + fetched[d, dest, :, cut(g)].astype(jnp.float32)
            ).astype(jnp.bfloat16)
            line_copy(d, dest, g).start()

    def project_arrived(t, carry):
        project(arrive_at(t))
        return carry

    lax.fori_loop(0, n - 1, project_arrived, 0)

    def turn(t, carry):
        @pl.when(t == 1)
        def _():
            pl.when(is_end)(lambda: pass_first(turn_of(0)))
            for distance in range(3, n):
                relay_toks(distance)
            last = arrive_at(n - 1)
            norm_block(last)
            project(last)

        dest = turn_of(t)
        block_output(dest)
        pair_copy(dest).start()
        pl.when((t >= 2) & is_end)(lambda: pass_first(turn_of(t - 1)))
        return carry

    lax.fori_loop(0, n, turn, 0)

    @pl.when(jnp.logical_not(is_end))
    def _():
        def passing(t, carry):
            pass_on(pass_of(t))
            return carry

        lax.fori_loop(0, n - 1, passing, 0)

    pair_copy(z).wait_recv()
    low, high = z > 0, z < n - 1
    for g in range(parts):
        pl.when(low)(lambda: line_copy(1, z, g).wait_recv())
        pl.when(high)(lambda: line_copy(0, z, g).wait_recv())

        @pl.when(low & high)
        def _():
            out[:, cut(g)] = (
                summed(z, g)
                + fetched[1, z, :, cut(g)].astype(jnp.float32)
                + fetched[0, z, :, cut(g)].astype(jnp.float32)
            ).astype(jnp.bfloat16)

        @pl.when(jnp.logical_not(low & high))
        def _():
            d = jnp.where(low, 1, 0)
            out[:, cut(g)] = (summed(z, g) + fetched[d, z, :, cut(g)].astype(jnp.float32)).astype(jnp.bfloat16)

    for j in range(1, n):
        zs = lax.rem(z + j, n)
        for kind in (0, 1):
            block = blocks[kind](zs, f)
            remote(block, block, wsem.at[kind, 0, zs], wsem.at[kind, 1, zs], here.to(z=zs)).wait_send()
        for g in range(parts):
            line_copy(toward(zs), zs, g).wait_send()
        lat_partner(1, zs, c).wait_send()
    for distance, sign in steps:
        dest = z + sign * distance

        @pl.when(reached(distance, sign))
        def _(dest=dest):
            block = low_block(dest, f)
            remote(block, block, wsem.at[2, 0, dest], wsem.at[2, 1, dest], here.to(z=dest)).wait_send()
            for k in range(2):
                lat_copy(k, dest).wait_send()

        @pl.when(within(dest) & serves(-sign))
        def _(dest=dest, sign=sign):
            end_copy(dest, -sign).wait_send()
            for k in range(2):
                lat_forward(k, dest, -sign).wait_send()

    def sent(zs):
        for kind in (0, 1, 2):
            plane_copy(kind, zs, 2, f, fx).wait_send()
            plane_copy(kind, zs, 4, f, fy).wait_send()
            plane_copy(kind, zs, 6, fx, fy).wait_send()
        for i in range(2):
            partner_copy(zs, c, i).wait_send()
        lat_partner(0, zs, c).wait_send()
        pair_copy(zs).wait_send()

    each_zs(sent)
    for sign in (-1, 1):
        for i in range(2):
            pl.when(can(sign))(lambda sign=sign, i=i: tok_copy(z, sign, 0, i).wait_send())
            for distance in range(1, n - 1):
                zs = z - sign * distance
                pl.when(within(zs) & can(sign))(
                    lambda sign=sign, distance=distance, i=i: tok_copy(z, sign, distance, i).wait_send()
                )


def split_shards(
    tokens,
    mix_gain,
    conv_b_weight,
    conv_c_weight,
    conv_v_weight,
    conv_taps,
    query_weight,
    query_rope_weight,
    latent_weight,
    key_rope_weight,
    latent_gain,
    key_up_weight,
    value_up_weight,
    head_gain,
    conv_out_weight,
    attn_out_weight,
):
    n = lax.axis_size("sp")
    tr = tokens.shape[1]
    wide = tokens.shape[2]
    length = n * tr
    features = 2 * wide
    heads = query_weight.shape[1] // NOPE // n
    channels = conv_b_weight.shape[1] // n
    low_rank = latent_weight.shape[1]
    proj_w = 3 * channels + heads * (NOPE + ROPE)
    out_rows = (conv_out_weight.shape[0] + attn_out_weight.shape[0]) // n
    columns = attn_out_weight.shape[1] * n * 4
    share = tr // 2
    parts = 4
    head_rows = 16
    bf16, f32 = jnp.bfloat16, jnp.float32
    dma = pltpu.SemaphoreType.DMA
    result = pl.pallas_call(
        functools.partial(layer_kernel, n, parts, orders(n)),
        out_shape=jax.ShapeDtypeStruct((share, columns), bf16),
        in_specs=[pl.BlockSpec(memory_space=pltpu.HBM)] * 16,
        out_specs=pl.BlockSpec(memory_space=pltpu.VMEM),
        scratch_shapes=[
            pltpu.VMEM((2, length, wide), bf16),
            pltpu.VMEM((length, features), bf16),
            pltpu.VMEM((features, proj_w), bf16),
            pltpu.VMEM((out_rows, columns), bf16),
            pltpu.VMEM((features, low_rank // 2), bf16),
            pltpu.VMEM((2, length, low_rank // 2), bf16),
            pltpu.VMEM((length, 2 * ROPE), bf16),
            pltpu.VMEM((8, features), f32),
            pltpu.VMEM((2 * ROPE, features), bf16),
            pltpu.VMEM(conv_taps.shape, f32),
            pltpu.VMEM((8, low_rank), f32),
            pltpu.VMEM((low_rank, heads * NOPE), bf16),
            pltpu.VMEM((low_rank, heads * VD), bf16),
            pltpu.VMEM((8, heads * VD), f32),
            pltpu.VMEM((length, channels), bf16),
            pltpu.VMEM((length + head_rows, channels), bf16),
            pltpu.VMEM((length, heads * NOPE), bf16),
            pltpu.VMEM((length, heads * ROPE), bf16),
            pltpu.VMEM((heads, length, NOPE + 2 * ROPE), bf16),
            pltpu.VMEM((length, heads * VD), bf16),
            pltpu.VMEM((length, heads * ROPE), f32),
            pltpu.VMEM((length, heads * ROPE), f32),
            pltpu.VMEM((n, tr, columns), bf16),
            pltpu.VMEM((n, share, columns), bf16),
            pltpu.VMEM((n, share, columns), bf16),
            pltpu.VMEM((2, n, share, columns), bf16),
            dma((3, 8, n)),
            dma((n,)),
            dma((5,)),
            dma((2, 2, n, 2)),
            dma((2, n, 2)),
            dma((2, 5, n)),
            dma((8,)),
            dma((2, n)),
            dma((2, 2, n, parts)),
        ],
        compiler_params=pltpu.CompilerParams(
            collective_id=0, has_side_effects=True, vmem_limit_bytes=60 * 1024 * 1024
        ),
        name="whole_layer",
    )(
        tokens,
        mix_gain[None],
        latent_gain[None],
        head_gain[None],
        conv_taps,
        conv_b_weight,
        conv_c_weight,
        conv_v_weight,
        query_weight,
        query_rope_weight,
        latent_weight,
        key_rope_weight.T,
        key_up_weight,
        value_up_weight,
        conv_out_weight,
        attn_out_weight,
    )
    return result[None]


def splits_well(mesh):
    n = mesh.shape["sp"]
    return n == 4 and mesh.shape["fs"] == 4 and mesh.shape["tp"] == 2


def shards(*arrays):
    n = lax.axis_size("sp")
    conv, query, rope, low_rank = (arrays[i].shape[1] for i in (2, 6, 7, 8))
    heads = query // NOPE
    even = heads == n * 128 // ROPE and all(w % (128 * n) == 0 for w in (conv, query, rope, low_rank))
    if even and arrays[0].shape[1] % 32 == 0 and arrays[15].shape[1] % 128 == 0:
        return split_shards(*arrays)
    return general_shards(*arrays)


def solution(mesh):
    return jax.shard_map(
        shards if splits_well(mesh) else general_shards,
        mesh=mesh,
        in_specs=(
            P("fs", "sp", "tp"),
            P(),
            P(("sp", "fs"), "tp"),
            P(("sp", "fs"), "tp"),
            P(("sp", "fs"), "tp"),
            P(None, "tp"),
            P(("sp", "fs"), "tp"),
            P(("sp", "fs"), "tp"),
            P(("sp", "fs"), None),
            P(),
            P(),
            P(None, "tp"),
            P(None, "tp"),
            P("tp"),
            P("tp", ("sp", "fs")),
            P("tp", ("sp", "fs")),
        ),
        out_specs=P("fs", ("sp", "tp"), None),
        check_vma=False,
    )
```

```python
import functools
import math

import jax
import jax.numpy as jnp
from jax import lax
from jax.experimental import pallas as pl
from jax.experimental.pallas import tpu as pltpu
from jax.sharding import PartitionSpec as P

NOPE = 128
ROPE = 64
VD = 128
KVL = 512
SEG = 64


norm_epsilon = 1e-06
rope_theta = 10000.0


def passed_along(block, axis, distance):
    devices = range(lax.axis_size(axis))
    route = [(i - distance, i) for i in devices if i - distance in devices]
    return lax.ppermute(block, axis, route)


def rms_scale(values, gain):
    return (
        values * lax.rsqrt(jnp.mean(values * values, axis=-1, keepdims=True) + norm_epsilon) * gain
    )


def rope_tables(positions):
    half_width = ROPE // 2
    frequency = rope_theta ** (-jnp.arange(half_width, dtype=jnp.float32) * 2.0 / ROPE)
    angles = positions[:, None] * frequency[None, :]
    return (jnp.cos(angles), jnp.sin(angles))


def rotate(values, cosine, sine):
    half_width = ROPE // 2
    first = values[..., :half_width]
    second = values[..., half_width:]
    return jnp.concatenate(
        [first * cosine - second * sine, second * cosine + first * sine], axis=-1
    )


def general_shards(
    tokens,
    mix_gain,
    conv_b_weight,
    conv_c_weight,
    conv_v_weight,
    conv_taps,
    query_weight,
    query_rope_weight,
    latent_weight,
    key_rope_weight,
    latent_gain,
    key_up_weight,
    value_up_weight,
    head_gain,
    conv_out_weight,
    attn_out_weight,
):
    full_rows = lax.all_gather(tokens[0], "tp", axis=1, tiled=True)
    tok_rows = full_rows.shape[0]
    normed = rms_scale(full_rows.astype(jnp.float32), mix_gain).astype(jnp.bfloat16)
    offset = lax.axis_index("sp") * tok_rows
    token_index = offset + jnp.arange(tok_rows, dtype=jnp.int32)
    cosine, sine = rope_tables(token_index.astype(jnp.float32))
    local_heads = query_weight.shape[1] // NOPE
    count_sp = lax.axis_size("sp")
    count_fs = lax.axis_size("fs")
    count_tp = lax.axis_size("tp")
    fs_index = lax.axis_index("fs")
    row_piece = normed.shape[1] // (count_sp * count_fs)
    all_normed = lax.all_gather(normed, "fs", axis=0, tiled=True)
    picked = lax.dynamic_index_in_dim(
        all_normed.reshape(-1, count_sp, count_fs, row_piece), fs_index, 2, keepdims=False
    ).reshape(-1, count_sp * row_piece)
    gathered = (
        lax.all_gather(conv_b_weight, "sp", axis=0, tiled=True),
        lax.all_gather(conv_c_weight, "sp", axis=0, tiled=True),
        lax.all_gather(conv_v_weight, "sp", axis=0, tiled=True),
        lax.all_gather(query_weight, "sp", axis=0, tiled=True),
        lax.all_gather(query_rope_weight, "sp", axis=0, tiled=True),
        lax.all_gather(latent_weight, "sp", axis=0, tiled=True),
    )

    def project_in():
        return jnp.concatenate(
            [jnp.dot(picked, member, preferred_element_type=jnp.float32) for member in gathered],
            axis=1,
        )

    joined = lax.psum_scatter(
        project_in().astype(jnp.bfloat16), "fs", scatter_dimension=0, tiled=True
    ).astype(jnp.float32)
    bounds = []
    running_total = 0
    for member in gathered[:-1]:
        running_total = running_total + member.shape[1]
        bounds.append(running_total)
    sums = tuple(jnp.split(joined, bounds, axis=1))
    latent_raw = sums[5].astype(jnp.bfloat16)
    gate_b = sums[0].astype(jnp.bfloat16)
    gate_c = sums[1].astype(jnp.bfloat16)
    values_v = sums[2].astype(jnp.bfloat16)
    query_nope = sums[3].astype(jnp.bfloat16).reshape(tok_rows, local_heads, NOPE)
    query_rot = rotate(
        sums[4].reshape(tok_rows, local_heads, ROPE), cosine[:, None, :], sine[:, None, :]
    ).astype(jnp.bfloat16)
    latent = rms_scale(latent_raw.astype(jnp.float32), latent_gain).astype(jnp.bfloat16)
    key_rot = rotate(
        jnp.dot(normed, key_rope_weight, preferred_element_type=jnp.float32), cosine, sine
    ).astype(jnp.bfloat16)
    query_latent = jnp.einsum(
        "thn,khn->thk",
        query_nope,
        key_up_weight.reshape(KVL, local_heads, NOPE),
        preferred_element_type=jnp.float32,
    ).astype(jnp.bfloat16)
    attn_scale = (NOPE + ROPE) ** (-0.5)
    product = (gate_c.astype(jnp.float32) * values_v.astype(jnp.float32)).astype(jnp.bfloat16)
    previous = passed_along(product[tok_rows - 2 :], "sp", 1)
    padded = jnp.concatenate([previous, product], axis=0).astype(jnp.float32)
    convolved = (
        conv_taps[0] * padded[0:tok_rows]
        + conv_taps[1] * padded[1 : tok_rows + 1]
        + conv_taps[2] * padded[2 : tok_rows + 2]
    )
    conv_y = (gate_b.astype(jnp.float32) * convolved).astype(jnp.bfloat16)
    query_segment = token_index // SEG
    last_segment = (offset + tok_rows - 1) // SEG

    def key_block(running, latent_block, rot_block, first_key):
        peak_old, denom_old, accum_old = running
        block_rows = latent_block.shape[0]
        scores = (
            jnp.einsum(
                "thk,jk->thj", query_latent, latent_block, preferred_element_type=jnp.float32
            )
            + jnp.einsum("thr,jr->thj", query_rot, rot_block, preferred_element_type=jnp.float32)
        ) * attn_scale
        key_segment = (first_key + jnp.arange(block_rows, dtype=jnp.int32)) // SEG
        allowed = key_segment[None, None, :] <= query_segment[:, None, None]
        peak_new = jnp.maximum(peak_old, jnp.max(jnp.where(allowed, scores, -1e30), axis=-1))
        weights = jnp.where(allowed, jnp.exp(scores - peak_new[..., None]), 0.0)
        rescale = jnp.exp(peak_old - peak_new)
        denom_new = denom_old * rescale + jnp.sum(weights, axis=-1)
        accum_new = accum_old * rescale[..., None] + jnp.einsum(
            "thj,jk->thk",
            weights.astype(jnp.bfloat16),
            latent_block,
            preferred_element_type=jnp.float32,
        )
        return (peak_new, denom_new, accum_new)

    starting = (
        jnp.full((tok_rows, local_heads), -1e30, jnp.float32),
        jnp.zeros((tok_rows, local_heads), jnp.float32),
        jnp.zeros((tok_rows, local_heads, KVL), jnp.float32),
    )
    latent_piece = lax.all_gather(latent, "sp", axis=0, tiled=True)
    rot_piece = lax.all_gather(key_rot, "sp", axis=0, tiled=True)
    piece_rows = latent_piece.shape[0]
    splits = max(1, piece_rows // 512)
    while piece_rows % splits:
        splits = splits - 1
    block_rows = piece_rows // splits

    def visit(state, block_index):
        block_begin = block_index * block_rows
        latent_block = lax.dynamic_slice_in_dim(latent_piece, block_begin, block_rows, 0)
        rot_block = lax.dynamic_slice_in_dim(rot_piece, block_begin, block_rows, 0)
        updated = lax.cond(
            block_begin // SEG <= last_segment,
            lambda inner: key_block(inner, latent_block, rot_block, block_begin),
            lambda inner: inner,
            state,
        )
        return (updated, None)

    peak, denom, accum = lax.scan(visit, starting, jnp.arange(splits, dtype=jnp.int32))[0]
    attended = (accum / denom[..., None]).astype(jnp.bfloat16)
    head_out = jnp.einsum(
        "thk,khv->thv",
        attended,
        value_up_weight.reshape(KVL, local_heads, VD),
        preferred_element_type=jnp.float32,
    )
    normed_heads = rms_scale(head_out, head_gain.reshape(local_heads, VD))
    attn_y = normed_heads.astype(jnp.bfloat16).reshape(tok_rows, local_heads * VD)
    share_rows = tok_rows // count_tp
    conv_all, attn_all = (
        lax.all_gather(conv_y, "fs", axis=0, tiled=True),
        lax.all_gather(attn_y, "fs", axis=0, tiled=True),
    )
    conv_sorted = (
        conv_all.reshape(count_fs, count_tp, share_rows, -1)
        .transpose(1, 0, 2, 3)
        .reshape(count_fs * tok_rows, -1)
    )
    attn_sorted = (
        attn_all.reshape(count_fs, count_tp, share_rows, -1)
        .transpose(1, 0, 2, 3)
        .reshape(count_fs * tok_rows, -1)
    )
    conv_cols_sp, attn_cols_sp = (
        lax.all_gather(conv_out_weight, "sp", axis=1, tiled=True),
        lax.all_gather(attn_out_weight, "sp", axis=1, tiled=True),
    )
    col_sums = lax.psum_scatter(
        (
            jnp.dot(conv_sorted, conv_cols_sp, preferred_element_type=jnp.float32)
            + jnp.dot(attn_sorted, attn_cols_sp, preferred_element_type=jnp.float32)
        ).astype(jnp.bfloat16),
        "tp",
        scatter_dimension=0,
        tiled=True,
    )
    col_piece = conv_cols_sp.shape[1] // count_sp
    outgoing = col_sums.reshape(count_fs, share_rows, count_sp * col_piece)
    arrived = lax.all_to_all(outgoing, "fs", split_axis=0, concat_axis=2, tiled=True)
    result = (
        arrived.reshape(share_rows, count_fs, count_sp, col_piece)
        .transpose(0, 2, 1, 3)
        .reshape(share_rows, count_fs * count_sp * col_piece)
    )
    return result[None]


MESH = pl.DeviceIdType.MESH


class Place:
    def __init__(self):
        self.z = lax.axis_index("sp")
        self.f = lax.axis_index("fs")
        self.c = lax.axis_index("tp")

    def to(self, z=None, f=None, c=None):
        return {
            "sp": self.z if z is None else z,
            "fs": self.f if f is None else f,
            "tp": self.c if c is None else c,
        }


def flip(index, bit):
    digit = (index // bit) % 2
    return index + bit * (1 - 2 * digit)


def remote(src, dst, send, recv, device):
    return pltpu.make_async_remote_copy(
        src_ref=src, dst_ref=dst, send_sem=send, recv_sem=recv, device_id=device, device_id_type=MESH
    )


def greet(devices):
    barrier = pltpu.get_barrier_semaphore()
    for device in devices:
        pl.semaphore_signal(barrier, inc=1, device_id=device, device_id_type=MESH)
    pl.semaphore_wait(barrier, len(devices))


def orders(n):
    columns = sorted(range(n), key=lambda g: (max(g, n - 1 - g), g))
    arrival, steps, passes = [], [], []
    slots = {}
    for z in (0, n - 1):
        by = [abs(z - d) for d in range(n)]
        g = columns
        sent = [(by[d], g[k]) for d, k in ((1, 0), (1, 1), (2, 0), (2, 1), (1, 2), (3, 0), (3, 1), (3, 2), (3, 3), (2, 2), (2, 3), (1, 3))]
        slots[z] = sent
    for z in range(n):
        end = 0 if 2 * z < n else n - 1
        near = sorted((d for d in range(n) if d != z), key=lambda d: (abs(d - z), abs(d - end)))
        arrival.append([z] + near)
        if z == end:
            steps.append(slots[z] + [(z, g) for g in columns])
            passes.append([(z, 0)])
            continue
        opposite = n - 1 - end
        seen = [(i, step) for i, step in enumerate(slots[end]) if step[0] not in (z, end)]
        seen += [(i + 2.2, step) for i, step in enumerate(slots[opposite]) if step[0] == end]
        passes.append([step for _, step in sorted(seen)])
        steps.append([(d, g) for g in columns for d in near + [z]])
    first_column, first_block = [], []
    for listed in steps:
        blocks_seen, columns_seen, at_column, at_block = set(), set(), [], []
        for d, g in listed:
            at_column.append(n if g in columns_seen else columns.index(g))
            at_block.append(0 if d in blocks_seen else 1)
            columns_seen.add(g)
            blocks_seen.add(d)
        first_column.append(at_column)
        first_block.append(at_block)
    split = lambda table, i: [[pair[i] for pair in row] for row in table]
    return arrival, columns, split(steps, 0), split(steps, 1), first_column, first_block, split(passes, 0), split(passes, 1)


def layer_kernel(
    n,
    order,
    tok_in,
    mix_gain_in,
    lat_gain_in,
    head_gain_in,
    taps_in,
    cb,
    cc,
    cv,
    qw,
    qr,
    lw,
    krw_in,
    key_up_in,
    value_up_in,
    co,
    ao,
    out,
    tok,
    normed,
    win,
    wout,
    wlat,
    lat,
    krot,
    gain,
    krw,
    taps,
    lat_gain,
    key_up,
    value_up,
    head_gain,
    gate,
    prod,
    q_nope,
    q_rot,
    keys,
    values,
    cosine,
    sine,
    part,
    pair,
    moving,
    fetched,
    wsem,
    lsem,
    tsem,
    psem,
    latsem,
    ssem,
    pairsem,
    zsem,
    gone,
    mix,
    summed_out,
):
    here = Place()
    z, f, c = here.z, here.f, here.c
    fx, fy = flip(f, 1), flip(f, 2)
    other = 1 - c
    is_end = (z == 0) | (z == n - 1)
    near = jnp.where(2 * z < n, -1, 1)
    sides = (near, -near)
    rows = cb.shape[0]
    members = (cb, cc, cv, qw, qr)
    widths = [m.shape[1] // n for m in members]
    starts = [sum(widths[:i]) for i in range(len(widths))]
    lat_half = lw.shape[1] // 2
    tr = tok_in.shape[1]
    hr = tr // 2
    length = n * tr
    outs = (co, ao)
    heights = [m.shape[0] // n for m in outs]
    tops = [sum(heights[:i]) for i in range(len(heights))]
    out_cols = co.shape[1]
    head_rows = prod.shape[0] - length

    steps = [(1 + j, s) for j in range(n - 1) for s in (-1, 1)]

    def chosen(table, t):
        found = jnp.int32(0)
        for zz in range(n):
            for tt in range(len(table[zz])):
                found = jnp.where((z == zz) & (t == tt), table[zz][tt], found)
        return found

    def arrive_at(t):
        return chosen(order[0], t)

    def packed(table, bits):
        words = []
        for row in table:
            word = sum(v << (bits * t) for t, v in enumerate(row))
            words.append(word - (1 << 32) if word >= 1 << 31 else word)
        mine = jnp.int32(words[0])
        for zz in range(1, n):
            mine = jnp.where(z == zz, jnp.int32(words[zz]), mine)
        return lambda t: jnp.right_shift(mine, bits * t) & ((1 << bits) - 1)

    step_block, step_column = packed(order[2], 2), packed(order[3], 2)
    column_opens = packed([[int(k < n) for k in row] for row in order[4]], 1)
    block_opens = packed(order[5], 1)
    pass_block, pass_column = packed(order[6], 2), packed(order[7], 2)
    column_at = packed([order[1]] * n, 2)

    greet(
        [here.to(z=lax.rem(z + j, n)) for j in range(1, n)]
        + [here.to(f=fx), here.to(f=fy), here.to(c=other)]
    )

    def in_block(zs, fs):
        return win.at[pl.ds(pl.multiple_of((zs * 4 + fs) * rows, rows), rows), :]

    def out_block(zs, fs):
        return wout.at[:, pl.ds(pl.multiple_of((zs * 4 + fs) * out_cols, out_cols), out_cols)]

    def low_block(zs, fs):
        return wlat.at[pl.ds(pl.multiple_of((zs * 4 + fs) * rows, rows), rows), :]

    blocks = (in_block, out_block, low_block)

    def pieces(kind, dest):
        found = []
        if kind == 0:
            dst = (z * 4 + f) * rows
            for m, w, s in zip(members, widths, starts):
                src = m.at[:, pl.ds(pl.multiple_of(dest * w, w), w)]
                found.append((src, win.at[pl.ds(pl.multiple_of(dst, rows), rows), pl.ds(s, w)]))
        elif kind == 1:
            dst = (z * 4 + f) * out_cols
            for m, h, s in zip(outs, heights, tops):
                src = m.at[pl.ds(pl.multiple_of(dest * h, h), h), :]
                found.append((src, wout.at[pl.ds(s, h), pl.ds(pl.multiple_of(dst, out_cols), out_cols)]))
        else:
            found.append((lw.at[:, pl.ds(pl.multiple_of(c * lat_half, lat_half), lat_half)], low_block(z, f)))
        return found

    def send_own(kind):
        for src, dst in pieces(kind, z):
            remote(src, dst, gone.at[kind], wsem.at[kind, 1, z], here.to(f=fx)).start()
            remote(src, dst, gone.at[kind], wsem.at[kind, 2, z], here.to(f=fy)).start()
            pltpu.make_async_copy(src, dst, lsem.at[kind]).start()

    def can(sign):
        return (z + sign >= 0) & (z + sign < n)

    def within(zs):
        return (zs >= 0) & (zs < n)

    def reached(distance, sign):
        dest = z + sign * distance
        if distance == 1:
            return within(dest)
        return (dest > 0) & (dest < n - 1)

    def serves(sign):
        return z + sign == jnp.where(sign > 0, n - 1, 0)

    def send_z(kind, distance, sign):
        dest = z + sign * distance

        @pl.when(reached(distance, sign) if kind == 2 else within(dest))
        def _():
            for src, dst in pieces(kind, dest):
                remote(src, dst, gone.at[kind], wsem.at[kind, 0, z], here.to(z=dest)).start()

    def plane_copy(kind, zs, role, fs, to):
        block = blocks[kind](zs, fs)
        return remote(block, block, gone.at[kind], wsem.at[kind, role, zs], here.to(f=to))

    def end_copy(zs, sign):
        block = low_block(zs, f)
        return remote(block, block, gone.at[2], wsem.at[2, 0, zs], here.to(z=z + sign))

    def relay_z(kind, distance, sign):
        zs = z + sign * distance

        @pl.when(within(zs))
        def _():
            block = blocks[kind](zs, f)
            remote(block, block, gone.at[kind], wsem.at[kind, 0, zs], here.to(z=zs)).wait_recv()
            if kind == 2:
                pl.when(serves(-sign))(lambda: end_copy(zs, -sign).start())
            plane_copy(kind, zs, 1, f, fx).start()
            plane_copy(kind, zs, 2, f, fy).start()

    def relay_plane(kind, zs):
        plane_copy(kind, zs, 1, fx, fx).wait_recv()

        @pl.when(zs % 2 == 0)
        def _():
            plane_copy(kind, zs, 3, fx, fy).start()

        plane_copy(kind, zs, 2, fy, fy).wait_recv()

        @pl.when(zs % 2 == 1)
        def _():
            plane_copy(kind, zs, 3, fy, fx).start()

    def relay_done(kind, zs):
        plane_copy(kind, zs, 3, flip(fx, 2), fx).wait_recv()

    def tok_block(owner, zs, i):
        return tok.at[owner, pl.ds(pl.multiple_of(zs * tr + i * hr, hr), hr), :]

    def half_at(sign, i):
        return jnp.where(sign > 0, 1 - i, i)

    own_tok = [tok_in.at[0, i * hr : (i + 1) * hr, :] for i in range(2)]

    def tok_copy(zs, sign, hop, i, src=None):
        block = tok_block(c, zs, i)
        return remote(
            block if src is None else src, block, gone.at[3], tsem.at[zs, i], here.to(z=z + sign)
        )

    def partner_copy(zs, owner, i, src=None):
        block = tok_block(owner, zs, i)
        return remote(
            block if src is None else src, block, gone.at[4], psem.at[zs, i], here.to(c=other)
        )

    def own_copy(i):
        return pltpu.make_async_copy(own_tok[i], tok_block(c, z, i), lsem.at[3 + i])

    channels = widths[0]
    heads = widths[3] // NOPE
    rot_w = widths[4]
    share = tr // 2

    def columns_of(array, width):
        return array.at[:, pl.ds(pl.multiple_of(z * width, width), width)]

    small = [
        (mix_gain_in, gain.at[0:1, :]),
        (krw_in, krw.at[0:ROPE, :]),
        (krw_in, krw.at[ROPE : 2 * ROPE, :]),
        (taps_in, taps),
        (lat_gain_in, lat_gain.at[0:1, :]),
        (columns_of(key_up_in, heads * NOPE), key_up),
        (columns_of(value_up_in, heads * VD), value_up),
        (columns_of(head_gain_in, heads * VD), head_gain.at[0:1, :]),
    ]

    send_own(2)
    for distance, sign in steps:
        send_z(2, distance, sign)
    for i in range(2):
        partner_copy(z, c, i, own_tok[i]).start()
        own_copy(i).start()
    send_own(0)
    middle = jnp.logical_not(is_end)

    def send_far_first(kind):
        for distance in (2, 1):
            for sign in (-1, 1):
                send_z(kind, distance, sign)

    def send_near_first(kind):
        for distance, sign in steps:
            send_z(kind, distance, sign)

    def send_toks():
        for sign in (-1, 1):
            for i in (1, 0) if sign > 0 else (0, 1):
                pl.when(can(sign))(lambda sign=sign, i=i: tok_copy(z, sign, 0, i, own_tok[i]).start())

    pl.when(middle)(lambda: send_far_first(0))

    @pl.when(is_end)
    def _():
        send_near_first(0)
        send_toks()


    for i, (src, dst) in enumerate(small):
        pltpu.make_async_copy(src, dst, ssem.at[i]).start()

    def relay_tok(distance, sign, i):
        zs = z + sign * distance

        @pl.when(within(zs))
        def _():
            half = half_at(-sign, i)
            tok_copy(zs, -sign, distance - 1, half).wait_recv()
            if distance < n - 1:
                pl.when(can(-sign))(lambda: tok_copy(zs, -sign, distance, half).start())
            partner_copy(zs, c, half).start()

    def relay_toks(distance, sides=sides):
        for sign in sides:
            for i in range(2):
                relay_tok(distance, sign, i)

    def each_zs(fn):
        def body(i, carry):
            fn(lax.rem(z + i, n))
            return carry

        lax.fori_loop(0, n, body, 0)

    def at_distance(distance, fn):
        for sign in sides:
            zs = z + sign * distance
            pl.when(within(zs))(lambda zs=zs: fn(zs))

    lane = lax.broadcasted_iota(jnp.int32, (tr, rot_w), 1)
    quarter = lane % (ROPE // 2)
    first_half = (lane % ROPE) < ROPE // 2
    frequency = jnp.exp(quarter.astype(jnp.float32) * (-2.0 / ROPE * math.log(rope_theta)))

    def tables(i, carry):
        at = pl.ds(pl.multiple_of(i * tr, tr), tr)
        position = (i * tr + lax.broadcasted_iota(jnp.int32, (tr, rot_w), 0)).astype(jnp.float32)
        angle = position * frequency
        cosine[at, :] = jnp.cos(angle)
        turned = jnp.sin(angle)
        sine[at, :] = jnp.where(first_half, -turned, turned)
        return carry

    lax.fori_loop(0, n, tables, 0)
    prod[0:head_rows, :] = jnp.zeros((head_rows, channels), prod.dtype)

    def rotated(x, at):
        low_half = (lax.broadcasted_iota(jnp.int32, x.shape, 1) % ROPE) < ROPE // 2
        swapped = jnp.where(low_half, pltpu.roll(x, rot_w - ROPE // 2, 1), pltpu.roll(x, ROPE // 2, 1))
        return (x * cosine[at, :] + swapped * sine[at, :]).astype(jnp.bfloat16)

    for i, (src, dst) in enumerate(small):
        pltpu.make_async_copy(src, dst, ssem.at[i]).wait()
    wide = tok.shape[2]

    def half_rows(zs, i):
        return pl.ds(pl.multiple_of(zs * tr + i * hr, hr), hr)

    def norm_half(zs, i):
        partner_copy(zs, other, i).wait_recv()
        at = half_rows(zs, i)
        first = tok[0, at, :].astype(jnp.float32)
        second = tok[1, at, :].astype(jnp.float32)
        mean = (
            jnp.sum(first * first, axis=-1, keepdims=True) + jnp.sum(second * second, axis=-1, keepdims=True)
        ) / (2 * wide)
        scale = lax.rsqrt(mean + norm_epsilon)
        normed[at, 0:wide] = (first * scale * gain[0:1, 0:wide]).astype(jnp.bfloat16)
        normed[at, wide : 2 * wide] = (second * scale * gain[0:1, wide : 2 * wide]).astype(jnp.bfloat16)

    def norm_block(zs):
        def body(i, carry):
            norm_half(zs, i)
            return carry

        lax.fori_loop(0, 2, body, 0)

    def rows_of(zs):
        return pl.ds(pl.multiple_of(zs * tr, tr), tr)

    def lat_block(zs, owner):
        return lat.at[owner, rows_of(zs), :]

    def rot_block(zs, owner):
        return krot.at[pl.ds(pl.multiple_of(zs * tr + owner * hr, hr), hr), :]

    shared = (lat_block, rot_block)

    def lat_copy(k, dest):
        block = shared[k](z, c)
        return remote(block, block, gone.at[5 + k], latsem.at[k, 0, z], here.to(z=dest))

    def lat_arrival(k, zs):
        block = shared[k](zs, c)
        return remote(block, block, gone.at[5 + k], latsem.at[k, 0, zs], here.to(z=zs))

    def lat_forward(k, zs, sign):
        block = shared[k](zs, c)
        return remote(block, block, gone.at[5 + k], latsem.at[k, 0, zs], here.to(z=z + sign))

    def lat_partner(k, zs, owner):
        block = shared[k](zs, owner)
        return remote(block, block, gone.at[5 + k], latsem.at[k, 1, zs], here.to(c=other))

    def relay_lat(distance, sides=sides):
        for sign in sides:
            zs = z + sign * distance

            @pl.when(within(zs))
            def _(zs=zs, sign=sign):
                for k in range(2):
                    lat_arrival(k, zs).wait_recv()
                    pl.when(serves(-sign))(lambda k=k: lat_forward(k, zs, -sign).start())
                    lat_partner(k, zs, c).start()

    def own_latents():
        at = rows_of(z)
        block = normed[at, :]
        lat[c, at, :] = jnp.dot(block, wlat[...], preferred_element_type=jnp.float32).astype(jnp.bfloat16)
        key_raw = lax.dot_general(
            block, krw[...], (((1,), (1,)), ((), ())), preferred_element_type=jnp.float32
        )
        krot[at, :] = rotated(key_raw, at)

    def relay_weights_z(distance):
        for sign in (-1, 1):
            for kind in (0, 1):
                relay_z(kind, distance, sign)

    def relay_weights_plane(zs):
        for kind in (0, 1):
            relay_plane(kind, zs)

    def relay_all_z(kind, distance):
        for sign in sides:
            relay_z(kind, distance, sign)

    def diagonals(kind, distance):
        at_distance(distance, lambda zs: relay_plane(kind, zs))

    def share_latents():
        pltpu.make_async_copy(low_block(z, f), low_block(z, f), lsem.at[2]).wait()
        each_zs(lambda zs: relay_done(2, zs))
        own_latents()
        for distance, sign in steps:
            dest = z + sign * distance

            @pl.when(reached(distance, sign))
            def _(dest=dest):
                for k in range(2):
                    lat_copy(k, dest).start()

        lat_partner(0, z, c).start()

    relay_all_z(2, 1)
    relay_plane(2, z)
    for i in range(2):
        own_copy(i).wait()
    norm_block(z)

    @pl.when(is_end)
    def _():
        relay_plane(0, z)
        send_own(1)
        for distance in range(2, n):
            relay_all_z(2, distance)
        relay_all_z(0, 1)
        for distance in range(1, n):
            diagonals(2, distance)
        relay_all_z(0, 2)
        relay_all_z(0, 3)
        share_latents()
        diagonals(0, 1)
        send_near_first(1)
        diagonals(0, 2)
        diagonals(0, 3)
        relay_lat(1)
        relay_toks(1)

    @pl.when(middle)
    def _():
        relay_all_z(2, 2)
        relay_plane(0, z)
        diagonals(2, 1)
        diagonals(2, 2)
        relay_z(0, 1, near)
        relay_all_z(0, 2)
        share_latents()
        send_toks()
        send_far_first(1)
        relay_plane(0, z + near)
        relay_z(0, 1, -near)
        diagonals(0, 2)
        relay_lat(1, sides[1:])
        relay_toks(1, sides[:1])
        send_own(1)
        relay_plane(0, z - near)
        relay_lat(1, sides[:1])
        relay_lat(2)
        relay_toks(1, sides[1:])

    pltpu.make_async_copy(in_block(z, f), in_block(z, f), lsem.at[0]).wait()
    each_zs(lambda zs: relay_done(0, zs))

    @pl.when(is_end)
    def _():
        pl.when(z == 0)(lambda: relay_all_z(1, 1))
        relay_all_z(1, 2)
        pl.when(z != 0)(lambda: relay_all_z(1, 1))

    pl.when(middle)(lambda: relay_z(1, 1, -near))
    norm_block(arrive_at(1))

    def project_rows(first_row, count):
        at = pl.ds(pl.multiple_of(first_row, hr), count)
        joined = jnp.dot(normed[at, :], win[...], preferred_element_type=jnp.float32)
        gates = joined[:, channels : 3 * channels].astype(jnp.bfloat16).astype(jnp.float32)
        gate[at, :] = joined[:, 0:channels].astype(jnp.bfloat16)
        below = pl.ds(pl.multiple_of(first_row + head_rows, head_rows), count)
        prod[below, :] = (gates[:, 0:channels] * gates[:, channels : 2 * channels]).astype(jnp.bfloat16)
        start = 3 * channels
        q_nope[at, :] = joined[:, start : start + heads * NOPE].astype(jnp.bfloat16)
        q_rot[at, :] = rotated(joined[:, start + heads * NOPE :], at)

    def project_half(zs, i):
        project_rows(zs * tr + i * hr, hr)

    def project_arrived(t, carry):
        project_rows(arrive_at(t) * tr, tr)
        return carry

    lax.fori_loop(0, 2, project_arrived, 0)

    @pl.when(is_end)
    def _():
        relay_lat(2)
        relay_lat(3)
        relay_all_z(1, 3)

    @pl.when(middle)
    def _():
        relay_z(1, 1, near)
        relay_all_z(1, 2)


    def lat_waits(zs):
        lat_partner(0, zs, other).wait_recv()
        pl.when(zs != z)(lambda: lat_partner(1, zs, other).wait_recv())

    def expand(i, carry):
        lat_waits(i)
        at = rows_of(i)
        raw = jnp.concatenate([lat[0, at, :], lat[1, at, :]], axis=1).astype(jnp.float32)
        mean = jnp.mean(raw * raw, axis=-1, keepdims=True)
        low = (raw * lax.rsqrt(mean + norm_epsilon) * lat_gain[0:1, :]).astype(jnp.bfloat16)
        wide_keys = jnp.dot(low, key_up[...], preferred_element_type=jnp.float32).astype(jnp.bfloat16)
        key_rot = krot[at, :]
        for h in range(heads):
            keys[h, at, 0:NOPE] = wide_keys[:, h * NOPE : (h + 1) * NOPE]
            keys[h, at, NOPE:] = key_rot
        values[at, :] = jnp.dot(low, value_up[...], preferred_element_type=jnp.float32).astype(jnp.bfloat16)
        return carry

    lax.fori_loop(0, n, expand, 0)
    relay_plane(1, order[1][0])
    pl.when(middle)(lambda: relay_toks(2))

    shift = SEG.bit_length() - 1
    row_index = lax.broadcasted_iota(jnp.int32, (tr, length), 0)
    key_segment = jnp.right_shift(lax.broadcasted_iota(jnp.int32, (tr, length), 1), shift)
    own_lanes = lane // ROPE
    own_channels = pl.ds(pl.multiple_of(z * channels, channels), channels)

    def features(dest):
        at = rows_of(dest)
        allowed = key_segment <= jnp.right_shift(row_index + dest * tr, shift)
        padded = prod[pl.ds(pl.multiple_of(dest * tr, head_rows), tr + head_rows), :].astype(jnp.float32)
        convolved = (
            taps[0:1, own_channels] * pltpu.roll(padded, 2, 0)[head_rows:]
            + taps[1:2, own_channels] * pltpu.roll(padded, 1, 0)[head_rows:]
            + taps[2:3, own_channels] * padded[head_rows:]
        )
        outputs = [(gate[at, :].astype(jnp.float32) * convolved).astype(jnp.bfloat16)]
        rot = q_rot[at, :]
        for h in range(heads):
            query = jnp.concatenate(
                [
                    q_nope[at, h * NOPE : (h + 1) * NOPE],
                    jnp.where(own_lanes == h, rot, jnp.zeros_like(rot)),
                ],
                axis=1,
            )
            scores = lax.dot_general(
                query, keys[h], (((1,), (1,)), ((), ())), preferred_element_type=jnp.float32
            ) * (NOPE + ROPE) ** (-0.5)
            scores = jnp.where(allowed, scores, -1e30)
            weights = jnp.exp(scores - jnp.max(scores, axis=-1, keepdims=True))
            denom = jnp.sum(weights, axis=-1, keepdims=True)
            head_out = (
                jnp.dot(
                    weights.astype(jnp.bfloat16),
                    values[:, h * VD : (h + 1) * VD],
                    preferred_element_type=jnp.float32,
                )
                / denom
            )
            mean = jnp.mean(head_out * head_out, axis=-1, keepdims=True)
            gained = head_out * lax.rsqrt(mean + norm_epsilon) * head_gain[0:1, h * VD : (h + 1) * VD]
            outputs.append(gained.astype(jnp.bfloat16))
        mix[dest] = jnp.concatenate(outputs, axis=1)

    piece_w = wout.shape[1] // n

    def cut(g):
        return pl.ds(pl.multiple_of(g * piece_w, piece_w), piece_w)

    def own_rows():
        return pl.ds(pl.multiple_of(c * share, share), share)

    def pair_copy(dest, g):
        theirs = pl.ds(pl.multiple_of(other * share, share), share)
        return remote(
            part.at[dest, theirs, cut(g)],
            pair.at[dest, :, cut(g)],
            gone.at[7],
            pairsem.at[dest, g],
            here.to(c=other),
        )

    def line_copy(d, dest, g, target):
        row = jnp.where((dest == target) & (d == 1), n, dest)
        return remote(
            moving.at[dest, :, cut(g)],
            fetched.at[d, dest, :, cut(g)],
            gone.at[8],
            zsem.at[row, g],
            here.to(z=z + 2 * d - 1),
        )

    def line_send(d, dest, g):
        line_copy(d, dest, g, z + 2 * d - 1).start()

    def summed(dest, g):
        kept = part[dest, own_rows(), cut(g)]
        return kept.astype(jnp.float32) + pair[dest, :, cut(g)].astype(jnp.float32)

    def toward(dest):
        return jnp.where(dest > z, 1, 0)

    def pass_first(dest, g):
        pair_copy(dest, g).wait_recv()
        moving[dest, :, cut(g)] = summed(dest, g).astype(jnp.bfloat16)
        line_send(toward(dest), dest, g)

    def pass_on(dest, g):
        d = toward(dest)
        pair_copy(dest, g).wait_recv()
        line_copy(d, dest, g, z).wait_recv()
        moving[dest, :, cut(g)] = (
            summed(dest, g) + fetched[d, dest, :, cut(g)].astype(jnp.float32)
        ).astype(jnp.bfloat16)
        line_send(d, dest, g)

    def process_half(zs, i):
        norm_half(zs, i)
        project_half(zs, i)

    @pl.when(middle)
    def _():
        def rest(t, carry):
            norm_block(arrive_at(t))
            return project_arrived(t, carry)

        lax.fori_loop(2, n, rest, 0)

    half_first = half_at(-sides[1], 0)
    half_last = 1 - half_first

    @pl.when(is_end)
    def _():
        relay_tok(2, sides[1], 0)
        process_half(arrive_at(2), half_first)

    relay_plane(1, order[1][1])


    second_block, third_block = [i for i, opens in enumerate(order[5][0]) if opens][1:3]

    def step(i, carry):
        dest, g = step_block(i), step_column(i)
        before = jnp.maximum(i - 1, 0)

        def pass_before():
            pass_first(step_block(before), step_column(before))

        pl.when(block_opens(i) == 1)(lambda: features(dest))

        @pl.when(column_opens(i) == 1)
        def _():
            pl.when(g == z)(lambda: pltpu.make_async_copy(out_block(z, f), out_block(z, f), lsem.at[1]).wait())
            relay_done(1, g)

        part[dest, :, cut(g)] = jnp.dot(
            mix[dest], wout[:, cut(g)], preferred_element_type=jnp.float32
        ).astype(jnp.bfloat16)
        pair_copy(dest, g).start()
        pl.when(is_end & (i >= 1) & (i <= n * (n - 1)))(pass_before)
        for k in range(2, n):
            pl.when(i == k - 2)(lambda k=k: relay_plane(1, order[1][k]))

        @pl.when(is_end)
        def _():
            @pl.when(i == 0)
            def _():
                relay_tok(2, sides[1], 1)
                relay_tok(3, sides[1], 0)

            pl.when(i == third_block - 3)(lambda: relay_tok(3, sides[1], 1))

            @pl.when((i == 1) | (i == third_block - 2))
            def _():
                first = jnp.where(i == 1, 0, 2)

                def late(t, carry):
                    process_half(jnp.where(t == 0, arrive_at(2), arrive_at(3)), jnp.where(t == 1, half_first, half_last))
                    return carry

                lax.fori_loop(first, jnp.where(i == 1, 2, 3), late, 0)

        return carry

    lax.fori_loop(0, n * n, step, 0)

    @pl.when(middle)
    def _():
        def passing(i, carry):
            pass_on(pass_block(i), pass_column(i))
            return carry

        lax.fori_loop(0, n * (n - 1), passing, 0)

    low, high = z > 0, z < n - 1

    def out_copy(g):
        return pltpu.make_async_copy(summed_out.at[:, cut(g)], out.at[:, cut(g)], gone.at[9])

    def finish(turn, carry):
        g = column_at(turn)
        pair_copy(z, g).wait_recv()
        pl.when(low)(lambda: line_copy(1, z, g, z).wait_recv())
        pl.when(high)(lambda: line_copy(0, z, g, z).wait_recv())

        @pl.when(middle)
        def _():
            summed_out[:, cut(g)] = (
                summed(z, g)
                + fetched[1, z, :, cut(g)].astype(jnp.float32)
                + fetched[0, z, :, cut(g)].astype(jnp.float32)
            ).astype(jnp.bfloat16)

        @pl.when(is_end)
        def _():
            d = jnp.where(low, 1, 0)
            summed_out[:, cut(g)] = (
                summed(z, g) + fetched[d, z, :, cut(g)].astype(jnp.float32)
            ).astype(jnp.bfloat16)

        out_copy(g).start()
        return carry

    lax.fori_loop(0, n, finish, 0)

    def sent(sem, ref):
        pltpu.make_async_copy(ref, ref, gone.at[sem]).wait()

    def by_place(sem, at_ends, at_middle):
        pl.when(is_end)(lambda: sent(sem, at_ends))
        pl.when(middle)(lambda: sent(sem, at_middle))

    whole = 4 * n - 1
    sent(0, win.at[0 : whole * rows, :])
    sent(1, wout.at[:, 0 : whole * out_cols])
    by_place(2, wlat.at[0 : (3 * n + 2) * rows, :], wlat.at[0 : 4 * n * rows, :])
    by_place(3, tok.at[:, 0:hr, :], tok.at[:, 0 : (n + 1) * hr, :])
    sent(4, tok.at[0])
    by_place(5, lat.at[:, 0 : 3 * tr, :], lat)
    by_place(6, krot.at[0 : 5 * hr, :], krot.at[0 : 7 * hr, :])
    sent(7, pair)
    sent(8, moving.at[0 : n - 1])
    sent(9, summed_out)


def split_shards(
    tokens,
    mix_gain,
    conv_b_weight,
    conv_c_weight,
    conv_v_weight,
    conv_taps,
    query_weight,
    query_rope_weight,
    latent_weight,
    key_rope_weight,
    latent_gain,
    key_up_weight,
    value_up_weight,
    head_gain,
    conv_out_weight,
    attn_out_weight,
):
    n = lax.axis_size("sp")
    tr = tokens.shape[1]
    wide = tokens.shape[2]
    length = n * tr
    features = 2 * wide
    heads = query_weight.shape[1] // NOPE // n
    channels = conv_b_weight.shape[1] // n
    low_rank = latent_weight.shape[1]
    proj_w = 3 * channels + heads * (NOPE + ROPE)
    out_rows = (conv_out_weight.shape[0] + attn_out_weight.shape[0]) // n
    columns = attn_out_weight.shape[1] * n * 4
    share = tr // 2
    head_rows = 16
    bf16, f32 = jnp.bfloat16, jnp.float32
    dma = pltpu.SemaphoreType.DMA
    result = pl.pallas_call(
        functools.partial(layer_kernel, n, orders(n)),
        out_shape=jax.ShapeDtypeStruct((share, columns), bf16),
        in_specs=[pl.BlockSpec(memory_space=pltpu.HBM)] * 16,
        out_specs=pl.BlockSpec(memory_space=pltpu.HBM),
        scratch_shapes=[
            pltpu.VMEM((2, length, wide), bf16),
            pltpu.VMEM((length, features), bf16),
            pltpu.VMEM((features, proj_w), bf16),
            pltpu.VMEM((out_rows, columns), bf16),
            pltpu.VMEM((features, low_rank // 2), bf16),
            pltpu.VMEM((2, length, low_rank // 2), bf16),
            pltpu.VMEM((length, 2 * ROPE), bf16),
            pltpu.VMEM((8, features), f32),
            pltpu.VMEM((2 * ROPE, features), bf16),
            pltpu.VMEM(conv_taps.shape, f32),
            pltpu.VMEM((8, low_rank), f32),
            pltpu.VMEM((low_rank, heads * NOPE), bf16),
            pltpu.VMEM((low_rank, heads * VD), bf16),
            pltpu.VMEM((8, heads * VD), f32),
            pltpu.VMEM((length, channels), bf16),
            pltpu.VMEM((length + head_rows, channels), bf16),
            pltpu.VMEM((length, heads * NOPE), bf16),
            pltpu.VMEM((length, heads * ROPE), bf16),
            pltpu.VMEM((heads, length, NOPE + 2 * ROPE), bf16),
            pltpu.VMEM((length, heads * VD), bf16),
            pltpu.VMEM((length, heads * ROPE), f32),
            pltpu.VMEM((length, heads * ROPE), f32),
            pltpu.VMEM((n, tr, columns), bf16),
            pltpu.VMEM((n, share, columns), bf16),
            pltpu.VMEM((n, share, columns), bf16),
            pltpu.VMEM((2, n, share, columns), bf16),
            dma((3, 4, n)),
            dma((5,)),
            dma((n, 2)),
            dma((n, 2)),
            dma((2, 2, n)),
            dma((8,)),
            dma((n, n)),
            dma((n + 1, n)),
            dma((10,)),
            pltpu.VMEM((n, tr, out_rows), bf16),
            pltpu.VMEM((share, columns), bf16),
        ],
        compiler_params=pltpu.CompilerParams(
            collective_id=0, has_side_effects=True, vmem_limit_bytes=60 * 1024 * 1024
        ),
        name="whole_layer",
    )(
        tokens,
        mix_gain[None],
        latent_gain[None],
        head_gain[None],
        conv_taps,
        conv_b_weight,
        conv_c_weight,
        conv_v_weight,
        query_weight,
        query_rope_weight,
        latent_weight,
        key_rope_weight.T,
        key_up_weight,
        value_up_weight,
        conv_out_weight,
        attn_out_weight,
    )
    return result[None]


def splits_well(mesh):
    n = mesh.shape["sp"]
    return n == 4 and mesh.shape["fs"] == 4 and mesh.shape["tp"] == 2


def shards(*arrays):
    n = lax.axis_size("sp")
    conv, query, rope, low_rank = (arrays[i].shape[1] for i in (2, 6, 7, 8))
    heads = query // NOPE
    even = heads == n * 128 // ROPE and all(w % (128 * n) == 0 for w in (conv, query, rope, low_rank))
    if even and arrays[0].shape[1] % 32 == 0 and arrays[15].shape[1] % 128 == 0:
        return split_shards(*arrays)
    return general_shards(*arrays)


def solution(mesh):
    return jax.shard_map(
        shards if splits_well(mesh) else general_shards,
        mesh=mesh,
        in_specs=(
            P("fs", "sp", "tp"),
            P(),
            P(("sp", "fs"), "tp"),
            P(("sp", "fs"), "tp"),
            P(("sp", "fs"), "tp"),
            P(None, "tp"),
            P(("sp", "fs"), "tp"),
            P(("sp", "fs"), "tp"),
            P(("sp", "fs"), None),
            P(),
            P(),
            P(None, "tp"),
            P(None, "tp"),
            P("tp"),
            P("tp", ("sp", "fs")),
            P("tp", ("sp", "fs")),
        ),
        out_specs=P("fs", ("sp", "tp"), None),
        check_vma=False,
    )
```

```python
import functools
import math

import jax
import jax.numpy as jnp
from jax import lax
from jax.experimental import pallas as pl
from jax.experimental.pallas import tpu as pltpu
from jax.sharding import PartitionSpec as P

NOPE = 128
ROPE = 64
VD = 128
KVL = 512
SEG = 64


norm_epsilon = 1e-06
rope_theta = 10000.0


def passed_along(block, axis, distance):
    devices = range(lax.axis_size(axis))
    route = [(i - distance, i) for i in devices if i - distance in devices]
    return lax.ppermute(block, axis, route)


def rms_scale(values, gain):
    return (
        values * lax.rsqrt(jnp.mean(values * values, axis=-1, keepdims=True) + norm_epsilon) * gain
    )


def rope_tables(positions):
    half_width = ROPE // 2
    frequency = rope_theta ** (-jnp.arange(half_width, dtype=jnp.float32) * 2.0 / ROPE)
    angles = positions[:, None] * frequency[None, :]
    return (jnp.cos(angles), jnp.sin(angles))


def rotate(values, cosine, sine):
    half_width = ROPE // 2
    first = values[..., :half_width]
    second = values[..., half_width:]
    return jnp.concatenate(
        [first * cosine - second * sine, second * cosine + first * sine], axis=-1
    )


def general_shards(
    tokens,
    mix_gain,
    conv_b_weight,
    conv_c_weight,
    conv_v_weight,
    conv_taps,
    query_weight,
    query_rope_weight,
    latent_weight,
    key_rope_weight,
    latent_gain,
    key_up_weight,
    value_up_weight,
    head_gain,
    conv_out_weight,
    attn_out_weight,
):
    full_rows = lax.all_gather(tokens[0], "tp", axis=1, tiled=True)
    tok_rows = full_rows.shape[0]
    normed = rms_scale(full_rows.astype(jnp.float32), mix_gain).astype(jnp.bfloat16)
    offset = lax.axis_index("sp") * tok_rows
    token_index = offset + jnp.arange(tok_rows, dtype=jnp.int32)
    cosine, sine = rope_tables(token_index.astype(jnp.float32))
    local_heads = query_weight.shape[1] // NOPE
    count_sp = lax.axis_size("sp")
    count_fs = lax.axis_size("fs")
    count_tp = lax.axis_size("tp")
    fs_index = lax.axis_index("fs")
    row_piece = normed.shape[1] // (count_sp * count_fs)
    all_normed = lax.all_gather(normed, "fs", axis=0, tiled=True)
    picked = lax.dynamic_index_in_dim(
        all_normed.reshape(-1, count_sp, count_fs, row_piece), fs_index, 2, keepdims=False
    ).reshape(-1, count_sp * row_piece)
    gathered = (
        lax.all_gather(conv_b_weight, "sp", axis=0, tiled=True),
        lax.all_gather(conv_c_weight, "sp", axis=0, tiled=True),
        lax.all_gather(conv_v_weight, "sp", axis=0, tiled=True),
        lax.all_gather(query_weight, "sp", axis=0, tiled=True),
        lax.all_gather(query_rope_weight, "sp", axis=0, tiled=True),
        lax.all_gather(latent_weight, "sp", axis=0, tiled=True),
    )

    def project_in():
        return jnp.concatenate(
            [jnp.dot(picked, member, preferred_element_type=jnp.float32) for member in gathered],
            axis=1,
        )

    joined = lax.psum_scatter(
        project_in().astype(jnp.bfloat16), "fs", scatter_dimension=0, tiled=True
    ).astype(jnp.float32)
    bounds = []
    running_total = 0
    for member in gathered[:-1]:
        running_total = running_total + member.shape[1]
        bounds.append(running_total)
    sums = tuple(jnp.split(joined, bounds, axis=1))
    latent_raw = sums[5].astype(jnp.bfloat16)
    gate_b = sums[0].astype(jnp.bfloat16)
    gate_c = sums[1].astype(jnp.bfloat16)
    values_v = sums[2].astype(jnp.bfloat16)
    query_nope = sums[3].astype(jnp.bfloat16).reshape(tok_rows, local_heads, NOPE)
    query_rot = rotate(
        sums[4].reshape(tok_rows, local_heads, ROPE), cosine[:, None, :], sine[:, None, :]
    ).astype(jnp.bfloat16)
    latent = rms_scale(latent_raw.astype(jnp.float32), latent_gain).astype(jnp.bfloat16)
    key_rot = rotate(
        jnp.dot(normed, key_rope_weight, preferred_element_type=jnp.float32), cosine, sine
    ).astype(jnp.bfloat16)
    query_latent = jnp.einsum(
        "thn,khn->thk",
        query_nope,
        key_up_weight.reshape(KVL, local_heads, NOPE),
        preferred_element_type=jnp.float32,
    ).astype(jnp.bfloat16)
    attn_scale = (NOPE + ROPE) ** (-0.5)
    product = (gate_c.astype(jnp.float32) * values_v.astype(jnp.float32)).astype(jnp.bfloat16)
    previous = passed_along(product[tok_rows - 2 :], "sp", 1)
    padded = jnp.concatenate([previous, product], axis=0).astype(jnp.float32)
    convolved = (
        conv_taps[0] * padded[0:tok_rows]
        + conv_taps[1] * padded[1 : tok_rows + 1]
        + conv_taps[2] * padded[2 : tok_rows + 2]
    )
    conv_y = (gate_b.astype(jnp.float32) * convolved).astype(jnp.bfloat16)
    query_segment = token_index // SEG
    last_segment = (offset + tok_rows - 1) // SEG

    def key_block(running, latent_block, rot_block, first_key):
        peak_old, denom_old, accum_old = running
        block_rows = latent_block.shape[0]
        scores = (
            jnp.einsum(
                "thk,jk->thj", query_latent, latent_block, preferred_element_type=jnp.float32
            )
            + jnp.einsum("thr,jr->thj", query_rot, rot_block, preferred_element_type=jnp.float32)
        ) * attn_scale
        key_segment = (first_key + jnp.arange(block_rows, dtype=jnp.int32)) // SEG
        allowed = key_segment[None, None, :] <= query_segment[:, None, None]
        peak_new = jnp.maximum(peak_old, jnp.max(jnp.where(allowed, scores, -1e30), axis=-1))
        weights = jnp.where(allowed, jnp.exp(scores - peak_new[..., None]), 0.0)
        rescale = jnp.exp(peak_old - peak_new)
        denom_new = denom_old * rescale + jnp.sum(weights, axis=-1)
        accum_new = accum_old * rescale[..., None] + jnp.einsum(
            "thj,jk->thk",
            weights.astype(jnp.bfloat16),
            latent_block,
            preferred_element_type=jnp.float32,
        )
        return (peak_new, denom_new, accum_new)

    starting = (
        jnp.full((tok_rows, local_heads), -1e30, jnp.float32),
        jnp.zeros((tok_rows, local_heads), jnp.float32),
        jnp.zeros((tok_rows, local_heads, KVL), jnp.float32),
    )
    latent_piece = lax.all_gather(latent, "sp", axis=0, tiled=True)
    rot_piece = lax.all_gather(key_rot, "sp", axis=0, tiled=True)
    piece_rows = latent_piece.shape[0]
    splits = max(1, piece_rows // 512)
    while piece_rows % splits:
        splits = splits - 1
    block_rows = piece_rows // splits

    def visit(state, block_index):
        block_begin = block_index * block_rows
        latent_block = lax.dynamic_slice_in_dim(latent_piece, block_begin, block_rows, 0)
        rot_block = lax.dynamic_slice_in_dim(rot_piece, block_begin, block_rows, 0)
        updated = lax.cond(
            block_begin // SEG <= last_segment,
            lambda inner: key_block(inner, latent_block, rot_block, block_begin),
            lambda inner: inner,
            state,
        )
        return (updated, None)

    peak, denom, accum = lax.scan(visit, starting, jnp.arange(splits, dtype=jnp.int32))[0]
    attended = (accum / denom[..., None]).astype(jnp.bfloat16)
    head_out = jnp.einsum(
        "thk,khv->thv",
        attended,
        value_up_weight.reshape(KVL, local_heads, VD),
        preferred_element_type=jnp.float32,
    )
    normed_heads = rms_scale(head_out, head_gain.reshape(local_heads, VD))
    attn_y = normed_heads.astype(jnp.bfloat16).reshape(tok_rows, local_heads * VD)
    share_rows = tok_rows // count_tp
    conv_all, attn_all = (
        lax.all_gather(conv_y, "fs", axis=0, tiled=True),
        lax.all_gather(attn_y, "fs", axis=0, tiled=True),
    )
    conv_sorted = (
        conv_all.reshape(count_fs, count_tp, share_rows, -1)
        .transpose(1, 0, 2, 3)
        .reshape(count_fs * tok_rows, -1)
    )
    attn_sorted = (
        attn_all.reshape(count_fs, count_tp, share_rows, -1)
        .transpose(1, 0, 2, 3)
        .reshape(count_fs * tok_rows, -1)
    )
    conv_cols_sp, attn_cols_sp = (
        lax.all_gather(conv_out_weight, "sp", axis=1, tiled=True),
        lax.all_gather(attn_out_weight, "sp", axis=1, tiled=True),
    )
    col_sums = lax.psum_scatter(
        (
            jnp.dot(conv_sorted, conv_cols_sp, preferred_element_type=jnp.float32)
            + jnp.dot(attn_sorted, attn_cols_sp, preferred_element_type=jnp.float32)
        ).astype(jnp.bfloat16),
        "tp",
        scatter_dimension=0,
        tiled=True,
    )
    col_piece = conv_cols_sp.shape[1] // count_sp
    outgoing = col_sums.reshape(count_fs, share_rows, count_sp * col_piece)
    arrived = lax.all_to_all(outgoing, "fs", split_axis=0, concat_axis=2, tiled=True)
    result = (
        arrived.reshape(share_rows, count_fs, count_sp, col_piece)
        .transpose(0, 2, 1, 3)
        .reshape(share_rows, count_fs * count_sp * col_piece)
    )
    return result[None]


MESH = pl.DeviceIdType.MESH


class Place:
    def __init__(self):
        self.z = lax.axis_index("sp")
        self.f = lax.axis_index("fs")
        self.c = lax.axis_index("tp")

    def to(self, z=None, f=None, c=None):
        return {
            "sp": self.z if z is None else z,
            "fs": self.f if f is None else f,
            "tp": self.c if c is None else c,
        }


def flip(index, bit):
    digit = (index // bit) % 2
    return index + bit * (1 - 2 * digit)


def remote(src, dst, send, recv, device):
    return pltpu.make_async_remote_copy(
        src_ref=src, dst_ref=dst, send_sem=send, recv_sem=recv, device_id=device, device_id_type=MESH
    )


def greet(devices):
    barrier = pltpu.get_barrier_semaphore()
    for device in devices:
        pl.semaphore_signal(barrier, inc=1, device_id=device, device_id_type=MESH)
    pl.semaphore_wait(barrier, len(devices))


def orders(n):
    columns = sorted(range(n), key=lambda g: (max(g, n - 1 - g), g))
    arrival, steps, passes = [], [], []
    slots = {}
    for z in (0, n - 1):
        by = [abs(z - d) for d in range(n)]
        g = columns
        sent = [(by[d], g[k]) for d, k in ((1, 0), (1, 1), (2, 0), (2, 1), (1, 2), (3, 0), (3, 1), (3, 2), (3, 3), (2, 2), (2, 3), (1, 3))]
        slots[z] = sent
    for z in range(n):
        end = 0 if 2 * z < n else n - 1
        near = sorted((d for d in range(n) if d != z), key=lambda d: (abs(d - z), abs(d - end)))
        arrival.append([z] + near)
        if z == end:
            steps.append(slots[z] + [(z, g) for g in columns])
            passes.append([(z, 0)])
            continue
        opposite = n - 1 - end
        seen = [(i, step) for i, step in enumerate(slots[end]) if step[0] not in (z, end)]
        seen += [(i + 2.2, step) for i, step in enumerate(slots[opposite]) if step[0] == end]
        passes.append([step for _, step in sorted(seen)])
        steps.append([(d, g) for g in columns for d in near + [z]])
    first_column, first_block = [], []
    for listed in steps:
        blocks_seen, columns_seen, at_column, at_block = set(), set(), [], []
        for d, g in listed:
            at_column.append(n if g in columns_seen else columns.index(g))
            at_block.append(0 if d in blocks_seen else 1)
            columns_seen.add(g)
            blocks_seen.add(d)
        first_column.append(at_column)
        first_block.append(at_block)
    split = lambda table, i: [[pair[i] for pair in row] for row in table]
    return arrival, columns, split(steps, 0), split(steps, 1), first_column, first_block, split(passes, 0), split(passes, 1)


def layer_kernel(
    n,
    order,
    tok_in,
    mix_gain_in,
    lat_gain_in,
    head_gain_in,
    taps_in,
    cb,
    cc,
    cv,
    qw,
    qr,
    lw,
    krw_in,
    key_up_in,
    value_up_in,
    co,
    ao,
    out,
    tok,
    normed,
    win,
    wout,
    wlat,
    lat,
    krot,
    gain,
    krw,
    taps,
    lat_gain,
    key_up,
    value_up,
    head_gain,
    gate,
    prod,
    q_nope,
    q_rot,
    keys,
    values,
    cosine,
    sine,
    part,
    pair,
    moving,
    fetched,
    wsem,
    lsem,
    tsem,
    psem,
    latsem,
    ssem,
    pairsem,
    zsem,
    gone,
    mix,
):
    here = Place()
    z, f, c = here.z, here.f, here.c
    fx, fy = flip(f, 1), flip(f, 2)
    other = 1 - c
    is_end = (z == 0) | (z == n - 1)
    near = jnp.where(2 * z < n, -1, 1)
    sides = (near, -near)
    rows = cb.shape[0]
    members = (cb, cc, cv, qw, qr)
    widths = [m.shape[1] // n for m in members]
    starts = [sum(widths[:i]) for i in range(len(widths))]
    lat_half = lw.shape[1] // 2
    tr = tok_in.shape[1]
    hr = tr // 2
    length = n * tr
    outs = (co, ao)
    heights = [m.shape[0] // n for m in outs]
    tops = [sum(heights[:i]) for i in range(len(heights))]
    out_cols = co.shape[1]
    head_rows = prod.shape[0] - length

    steps = [(1 + j, s) for j in range(n - 1) for s in (-1, 1)]

    def chosen(table, t):
        found = jnp.int32(0)
        for zz in range(n):
            for tt in range(len(table[zz])):
                found = jnp.where((z == zz) & (t == tt), table[zz][tt], found)
        return found

    def arrive_at(t):
        return chosen(order[0], t)

    def packed(table, bits):
        words = []
        for row in table:
            word = sum(v << (bits * t) for t, v in enumerate(row))
            words.append(word - (1 << 32) if word >= 1 << 31 else word)
        mine = jnp.int32(words[0])
        for zz in range(1, n):
            mine = jnp.where(z == zz, jnp.int32(words[zz]), mine)
        return lambda t: jnp.right_shift(mine, bits * t) & ((1 << bits) - 1)

    step_block, step_column = packed(order[2], 2), packed(order[3], 2)
    column_opens = packed([[int(k < n) for k in row] for row in order[4]], 1)
    block_opens = packed(order[5], 1)
    pass_block, pass_column = packed(order[6], 2), packed(order[7], 2)
    column_at = packed([order[1]] * n, 2)

    greet(
        [here.to(z=lax.rem(z + j, n)) for j in range(1, n)]
        + [here.to(f=fx), here.to(f=fy), here.to(c=other)]
    )

    def in_block(zs, fs):
        return win.at[pl.ds(pl.multiple_of((zs * 4 + fs) * rows, rows), rows), :]

    def out_block(zs, fs):
        return wout.at[:, pl.ds(pl.multiple_of((zs * 4 + fs) * out_cols, out_cols), out_cols)]

    def low_block(zs, fs):
        return wlat.at[pl.ds(pl.multiple_of((zs * 4 + fs) * rows, rows), rows), :]

    blocks = (in_block, out_block, low_block)

    def pieces(kind, dest):
        found = []
        if kind == 0:
            dst = (z * 4 + f) * rows
            for m, w, s in zip(members, widths, starts):
                src = m.at[:, pl.ds(pl.multiple_of(dest * w, w), w)]
                found.append((src, win.at[pl.ds(pl.multiple_of(dst, rows), rows), pl.ds(s, w)]))
        elif kind == 1:
            dst = (z * 4 + f) * out_cols
            for m, h, s in zip(outs, heights, tops):
                src = m.at[pl.ds(pl.multiple_of(dest * h, h), h), :]
                found.append((src, wout.at[pl.ds(s, h), pl.ds(pl.multiple_of(dst, out_cols), out_cols)]))
        else:
            found.append((lw.at[:, pl.ds(pl.multiple_of(c * lat_half, lat_half), lat_half)], low_block(z, f)))
        return found

    def send_own(kind):
        for src, dst in pieces(kind, z):
            remote(src, dst, gone.at[kind], wsem.at[kind, 1, z], here.to(f=fx)).start()
            remote(src, dst, gone.at[kind], wsem.at[kind, 2, z], here.to(f=fy)).start()
            pltpu.make_async_copy(src, dst, lsem.at[kind]).start()

    def can(sign):
        return (z + sign >= 0) & (z + sign < n)

    def within(zs):
        return (zs >= 0) & (zs < n)

    def reached(distance, sign):
        dest = z + sign * distance
        if distance == 1:
            return within(dest)
        return (dest > 0) & (dest < n - 1)

    def serves(sign):
        return z + sign == jnp.where(sign > 0, n - 1, 0)

    def send_z(kind, distance, sign):
        dest = z + sign * distance

        @pl.when(reached(distance, sign) if kind == 2 else within(dest))
        def _():
            for src, dst in pieces(kind, dest):
                remote(src, dst, gone.at[kind], wsem.at[kind, 0, z], here.to(z=dest)).start()

    def plane_copy(kind, zs, role, fs, to):
        block = blocks[kind](zs, fs)
        return remote(block, block, gone.at[kind], wsem.at[kind, role, zs], here.to(f=to))

    def end_copy(zs, sign):
        block = low_block(zs, f)
        return remote(block, block, gone.at[2], wsem.at[2, 0, zs], here.to(z=z + sign))

    def relay_z(kind, distance, sign):
        zs = z + sign * distance

        @pl.when(within(zs))
        def _():
            block = blocks[kind](zs, f)
            remote(block, block, gone.at[kind], wsem.at[kind, 0, zs], here.to(z=zs)).wait_recv()
            if kind == 2:
                pl.when(serves(-sign))(lambda: end_copy(zs, -sign).start())
            plane_copy(kind, zs, 1, f, fx).start()
            plane_copy(kind, zs, 2, f, fy).start()

    def relay_plane(kind, zs):
        plane_copy(kind, zs, 1, fx, fx).wait_recv()

        @pl.when(zs % 2 == 0)
        def _():
            plane_copy(kind, zs, 3, fx, fy).start()

        plane_copy(kind, zs, 2, fy, fy).wait_recv()

        @pl.when(zs % 2 == 1)
        def _():
            plane_copy(kind, zs, 3, fy, fx).start()

    def relay_done(kind, zs):
        plane_copy(kind, zs, 3, flip(fx, 2), fx).wait_recv()

    def tok_block(owner, zs, i):
        return tok.at[owner, pl.ds(pl.multiple_of(zs * tr + i * hr, hr), hr), :]

    def half_at(sign, i):
        return jnp.where(sign > 0, 1 - i, i)

    own_tok = [tok_in.at[0, i * hr : (i + 1) * hr, :] for i in range(2)]

    def tok_copy(zs, sign, hop, i, src=None):
        block = tok_block(c, zs, i)
        return remote(
            block if src is None else src, block, gone.at[3], tsem.at[zs, i], here.to(z=z + sign)
        )

    def partner_copy(zs, owner, i, src=None):
        block = tok_block(owner, zs, i)
        return remote(
            block if src is None else src, block, gone.at[4], psem.at[zs, i], here.to(c=other)
        )

    def own_copy(i):
        return pltpu.make_async_copy(own_tok[i], tok_block(c, z, i), lsem.at[3 + i])

    channels = widths[0]
    heads = widths[3] // NOPE
    rot_w = widths[4]
    share = tr // 2

    def columns_of(array, width):
        return array.at[:, pl.ds(pl.multiple_of(z * width, width), width)]

    small = [
        (mix_gain_in, gain.at[0:1, :]),
        (krw_in, krw.at[0:ROPE, :]),
        (krw_in, krw.at[ROPE : 2 * ROPE, :]),
        (taps_in, taps),
        (lat_gain_in, lat_gain.at[0:1, :]),
        (columns_of(key_up_in, heads * NOPE), key_up),
        (columns_of(value_up_in, heads * VD), value_up),
        (columns_of(head_gain_in, heads * VD), head_gain.at[0:1, :]),
    ]

    send_own(2)
    for distance, sign in steps:
        send_z(2, distance, sign)
    for i in range(2):
        partner_copy(z, c, i, own_tok[i]).start()
        own_copy(i).start()
    send_own(0)
    middle = jnp.logical_not(is_end)

    def send_far_first(kind):
        for distance in (2, 1):
            for sign in (-1, 1):
                send_z(kind, distance, sign)

    def send_near_first(kind):
        for distance, sign in steps:
            send_z(kind, distance, sign)

    def send_toks():
        for sign in (-1, 1):
            for i in (1, 0) if sign > 0 else (0, 1):
                pl.when(can(sign))(lambda sign=sign, i=i: tok_copy(z, sign, 0, i, own_tok[i]).start())

    pl.when(middle)(lambda: send_far_first(0))

    @pl.when(is_end)
    def _():
        send_near_first(0)
        send_toks()


    for i, (src, dst) in enumerate(small):
        pltpu.make_async_copy(src, dst, ssem.at[i]).start()

    def relay_tok(distance, sign, i):
        zs = z + sign * distance

        @pl.when(within(zs))
        def _():
            half = half_at(-sign, i)
            tok_copy(zs, -sign, distance - 1, half).wait_recv()
            if distance < n - 1:
                pl.when(can(-sign))(lambda: tok_copy(zs, -sign, distance, half).start())
            partner_copy(zs, c, half).start()

    def relay_toks(distance, sides=sides):
        for sign in sides:
            for i in range(2):
                relay_tok(distance, sign, i)

    def each_zs(fn):
        def body(i, carry):
            fn(lax.rem(z + i, n))
            return carry

        lax.fori_loop(0, n, body, 0)

    def at_distance(distance, fn):
        for sign in sides:
            zs = z + sign * distance
            pl.when(within(zs))(lambda zs=zs: fn(zs))

    lane = lax.broadcasted_iota(jnp.int32, (tr, rot_w), 1)
    quarter = lane % (ROPE // 2)
    first_half = (lane % ROPE) < ROPE // 2
    frequency = jnp.exp(quarter.astype(jnp.float32) * (-2.0 / ROPE * math.log(rope_theta)))

    def tables(i, carry):
        at = pl.ds(pl.multiple_of(i * tr, tr), tr)
        position = (i * tr + lax.broadcasted_iota(jnp.int32, (tr, rot_w), 0)).astype(jnp.float32)
        angle = position * frequency
        cosine[at, :] = jnp.cos(angle)
        turned = jnp.sin(angle)
        sine[at, :] = jnp.where(first_half, -turned, turned)
        return carry

    lax.fori_loop(0, n, tables, 0)
    prod[0:head_rows, :] = jnp.zeros((head_rows, channels), prod.dtype)

    def rotated(x, at):
        low_half = (lax.broadcasted_iota(jnp.int32, x.shape, 1) % ROPE) < ROPE // 2
        swapped = jnp.where(low_half, pltpu.roll(x, rot_w - ROPE // 2, 1), pltpu.roll(x, ROPE // 2, 1))
        return (x * cosine[at, :] + swapped * sine[at, :]).astype(jnp.bfloat16)

    for i, (src, dst) in enumerate(small):
        pltpu.make_async_copy(src, dst, ssem.at[i]).wait()
    wide = tok.shape[2]

    def half_rows(zs, i):
        return pl.ds(pl.multiple_of(zs * tr + i * hr, hr), hr)

    def norm_half(zs, i):
        partner_copy(zs, other, i).wait_recv()
        at = half_rows(zs, i)
        first = tok[0, at, :].astype(jnp.float32)
        second = tok[1, at, :].astype(jnp.float32)
        mean = (
            jnp.sum(first * first, axis=-1, keepdims=True) + jnp.sum(second * second, axis=-1, keepdims=True)
        ) / (2 * wide)
        scale = lax.rsqrt(mean + norm_epsilon)
        normed[at, 0:wide] = (first * scale * gain[0:1, 0:wide]).astype(jnp.bfloat16)
        normed[at, wide : 2 * wide] = (second * scale * gain[0:1, wide : 2 * wide]).astype(jnp.bfloat16)

    def norm_block(zs):
        def body(i, carry):
            norm_half(zs, i)
            return carry

        lax.fori_loop(0, 2, body, 0)

    def rows_of(zs):
        return pl.ds(pl.multiple_of(zs * tr, tr), tr)

    def lat_block(zs, owner):
        return lat.at[owner, rows_of(zs), :]

    def rot_block(zs, owner):
        return krot.at[pl.ds(pl.multiple_of(zs * tr + owner * hr, hr), hr), :]

    shared = (lat_block, rot_block)

    def lat_copy(k, dest):
        block = shared[k](z, c)
        return remote(block, block, gone.at[5 + k], latsem.at[k, 0, z], here.to(z=dest))

    def lat_arrival(k, zs):
        block = shared[k](zs, c)
        return remote(block, block, gone.at[5 + k], latsem.at[k, 0, zs], here.to(z=zs))

    def lat_forward(k, zs, sign):
        block = shared[k](zs, c)
        return remote(block, block, gone.at[5 + k], latsem.at[k, 0, zs], here.to(z=z + sign))

    def lat_partner(k, zs, owner):
        block = shared[k](zs, owner)
        return remote(block, block, gone.at[5 + k], latsem.at[k, 1, zs], here.to(c=other))

    def relay_lat(distance, sides=sides):
        for sign in sides:
            zs = z + sign * distance

            @pl.when(within(zs))
            def _(zs=zs, sign=sign):
                for k in range(2):
                    lat_arrival(k, zs).wait_recv()
                    pl.when(serves(-sign))(lambda k=k: lat_forward(k, zs, -sign).start())
                    lat_partner(k, zs, c).start()

    def own_latents():
        at = rows_of(z)
        block = normed[at, :]
        lat[c, at, :] = jnp.dot(block, wlat[...], preferred_element_type=jnp.float32).astype(jnp.bfloat16)
        key_raw = lax.dot_general(
            block, krw[...], (((1,), (1,)), ((), ())), preferred_element_type=jnp.float32
        )
        krot[at, :] = rotated(key_raw, at)

    def relay_weights_z(distance):
        for sign in (-1, 1):
            for kind in (0, 1):
                relay_z(kind, distance, sign)

    def relay_weights_plane(zs):
        for kind in (0, 1):
            relay_plane(kind, zs)

    def relay_all_z(kind, distance):
        for sign in sides:
            relay_z(kind, distance, sign)

    def diagonals(kind, distance):
        at_distance(distance, lambda zs: relay_plane(kind, zs))

    def share_latents():
        pltpu.make_async_copy(low_block(z, f), low_block(z, f), lsem.at[2]).wait()
        each_zs(lambda zs: relay_done(2, zs))
        own_latents()
        for distance, sign in steps:
            dest = z + sign * distance

            @pl.when(reached(distance, sign))
            def _(dest=dest):
                for k in range(2):
                    lat_copy(k, dest).start()

        lat_partner(0, z, c).start()

    relay_all_z(2, 1)
    relay_plane(2, z)
    for i in range(2):
        own_copy(i).wait()
    norm_block(z)

    @pl.when(is_end)
    def _():
        relay_plane(0, z)
        send_own(1)
        for distance in range(2, n):
            relay_all_z(2, distance)
        relay_all_z(0, 1)
        for distance in range(1, n):
            diagonals(2, distance)
        relay_all_z(0, 2)
        relay_all_z(0, 3)
        share_latents()
        diagonals(0, 1)
        send_near_first(1)
        diagonals(0, 2)
        diagonals(0, 3)
        relay_lat(1)
        relay_toks(1)

    @pl.when(middle)
    def _():
        relay_all_z(2, 2)
        relay_plane(0, z)
        diagonals(2, 1)
        diagonals(2, 2)
        relay_z(0, 1, near)
        relay_all_z(0, 2)
        share_latents()
        send_toks()
        send_far_first(1)
        relay_plane(0, z + near)
        relay_z(0, 1, -near)
        diagonals(0, 2)
        relay_lat(1, sides[1:])
        relay_toks(1, sides[:1])
        send_own(1)
        relay_plane(0, z - near)
        relay_lat(1, sides[:1])
        relay_lat(2)
        relay_toks(1, sides[1:])

    pltpu.make_async_copy(in_block(z, f), in_block(z, f), lsem.at[0]).wait()
    each_zs(lambda zs: relay_done(0, zs))

    @pl.when(is_end)
    def _():
        pl.when(z == 0)(lambda: relay_all_z(1, 1))
        relay_all_z(1, 2)
        pl.when(z != 0)(lambda: relay_all_z(1, 1))

    pl.when(middle)(lambda: relay_z(1, 1, -near))
    norm_block(arrive_at(1))

    def project_rows(first_row, count):
        at = pl.ds(pl.multiple_of(first_row, hr), count)
        joined = jnp.dot(normed[at, :], win[...], preferred_element_type=jnp.float32)
        gates = joined[:, channels : 3 * channels].astype(jnp.bfloat16).astype(jnp.float32)
        gate[at, :] = joined[:, 0:channels].astype(jnp.bfloat16)
        below = pl.ds(pl.multiple_of(first_row + head_rows, head_rows), count)
        prod[below, :] = (gates[:, 0:channels] * gates[:, channels : 2 * channels]).astype(jnp.bfloat16)
        start = 3 * channels
        q_nope[at, :] = joined[:, start : start + heads * NOPE].astype(jnp.bfloat16)
        q_rot[at, :] = rotated(joined[:, start + heads * NOPE :], at)

    def project_half(zs, i):
        project_rows(zs * tr + i * hr, hr)

    def project_arrived(t, carry):
        project_rows(arrive_at(t) * tr, tr)
        return carry

    lax.fori_loop(0, 2, project_arrived, 0)

    @pl.when(is_end)
    def _():
        relay_lat(2)
        relay_lat(3)


    def lat_waits(zs):
        lat_partner(0, zs, other).wait_recv()
        pl.when(zs != z)(lambda: lat_partner(1, zs, other).wait_recv())

    def expand(i, carry):
        lat_waits(i)
        at = rows_of(i)
        raw = jnp.concatenate([lat[0, at, :], lat[1, at, :]], axis=1).astype(jnp.float32)
        mean = jnp.mean(raw * raw, axis=-1, keepdims=True)
        low = (raw * lax.rsqrt(mean + norm_epsilon) * lat_gain[0:1, :]).astype(jnp.bfloat16)
        wide_keys = jnp.dot(low, key_up[...], preferred_element_type=jnp.float32).astype(jnp.bfloat16)
        key_rot = krot[at, :]
        for h in range(heads):
            keys[h, at, 0:NOPE] = wide_keys[:, h * NOPE : (h + 1) * NOPE]
            keys[h, at, NOPE:] = key_rot
        values[at, :] = jnp.dot(low, value_up[...], preferred_element_type=jnp.float32).astype(jnp.bfloat16)
        return carry

    lax.fori_loop(0, n, expand, 0)
    relay_plane(1, order[1][0])
    pl.when(is_end)(lambda: relay_all_z(1, 3))

    @pl.when(middle)
    def _():
        relay_z(1, 1, near)
        relay_all_z(1, 2)
        relay_toks(2)


    shift = SEG.bit_length() - 1
    row_index = lax.broadcasted_iota(jnp.int32, (tr, length), 0)
    key_segment = jnp.right_shift(lax.broadcasted_iota(jnp.int32, (tr, length), 1), shift)
    own_lanes = lane // ROPE
    own_channels = pl.ds(pl.multiple_of(z * channels, channels), channels)

    def features(dest):
        at = rows_of(dest)
        allowed = key_segment <= jnp.right_shift(row_index + dest * tr, shift)
        padded = prod[pl.ds(pl.multiple_of(dest * tr, head_rows), tr + head_rows), :].astype(jnp.float32)
        convolved = (
            taps[0:1, own_channels] * pltpu.roll(padded, 2, 0)[head_rows:]
            + taps[1:2, own_channels] * pltpu.roll(padded, 1, 0)[head_rows:]
            + taps[2:3, own_channels] * padded[head_rows:]
        )
        outputs = [(gate[at, :].astype(jnp.float32) * convolved).astype(jnp.bfloat16)]
        rot = q_rot[at, :]
        for h in range(heads):
            query = jnp.concatenate(
                [
                    q_nope[at, h * NOPE : (h + 1) * NOPE],
                    jnp.where(own_lanes == h, rot, jnp.zeros_like(rot)),
                ],
                axis=1,
            )
            scores = lax.dot_general(
                query, keys[h], (((1,), (1,)), ((), ())), preferred_element_type=jnp.float32
            ) * (NOPE + ROPE) ** (-0.5)
            scores = jnp.where(allowed, scores, -1e30)
            weights = jnp.exp(scores - jnp.max(scores, axis=-1, keepdims=True))
            denom = jnp.sum(weights, axis=-1, keepdims=True)
            head_out = (
                jnp.dot(
                    weights.astype(jnp.bfloat16),
                    values[:, h * VD : (h + 1) * VD],
                    preferred_element_type=jnp.float32,
                )
                / denom
            )
            mean = jnp.mean(head_out * head_out, axis=-1, keepdims=True)
            gained = head_out * lax.rsqrt(mean + norm_epsilon) * head_gain[0:1, h * VD : (h + 1) * VD]
            outputs.append(gained.astype(jnp.bfloat16))
        mix[dest] = jnp.concatenate(outputs, axis=1)

    piece_w = wout.shape[1] // n

    def cut(g):
        return pl.ds(pl.multiple_of(g * piece_w, piece_w), piece_w)

    def own_rows():
        return pl.ds(pl.multiple_of(c * share, share), share)

    def pair_copy(dest, g):
        theirs = pl.ds(pl.multiple_of(other * share, share), share)
        return remote(
            part.at[dest, theirs, cut(g)],
            pair.at[dest, :, cut(g)],
            gone.at[7],
            pairsem.at[dest, g],
            here.to(c=other),
        )

    def line_copy(d, dest, g, target):
        row = jnp.where((dest == target) & (d == 1), n, dest)
        return remote(
            moving.at[dest, :, cut(g)],
            fetched.at[d, dest, :, cut(g)],
            gone.at[8],
            zsem.at[row, g],
            here.to(z=z + 2 * d - 1),
        )

    def line_send(d, dest, g):
        line_copy(d, dest, g, z + 2 * d - 1).start()

    def summed(dest, g):
        kept = part[dest, own_rows(), cut(g)]
        return kept.astype(jnp.float32) + pair[dest, :, cut(g)].astype(jnp.float32)

    def toward(dest):
        return jnp.where(dest > z, 1, 0)

    def pass_first(dest, g):
        pair_copy(dest, g).wait_recv()
        moving[dest, :, cut(g)] = summed(dest, g).astype(jnp.bfloat16)
        line_send(toward(dest), dest, g)

    def pass_on(dest, g):
        d = toward(dest)
        pair_copy(dest, g).wait_recv()
        line_copy(d, dest, g, z).wait_recv()
        moving[dest, :, cut(g)] = (
            summed(dest, g) + fetched[d, dest, :, cut(g)].astype(jnp.float32)
        ).astype(jnp.bfloat16)
        line_send(d, dest, g)

    def process_half(zs, i):
        norm_half(zs, i)
        project_half(zs, i)

    @pl.when(middle)
    def _():
        def rest(t, carry):
            norm_block(arrive_at(t))
            return project_arrived(t, carry)

        lax.fori_loop(2, n, rest, 0)

    half_first = half_at(-sides[1], 0)
    half_last = 1 - half_first

    @pl.when(is_end)
    def _():
        relay_tok(2, sides[1], 0)
        relay_tok(2, sides[1], 1)
        process_half(arrive_at(2), half_first)

    relay_plane(1, order[1][1])


    second_block, third_block = [i for i, opens in enumerate(order[5][0]) if opens][1:3]

    def step(i, carry):
        dest, g = step_block(i), step_column(i)
        before = jnp.maximum(i - 1, 0)

        def pass_before():
            pass_first(step_block(before), step_column(before))

        opens = (block_opens(i) == 1) | (column_opens(i) == 1)
        passes = is_end & (i >= 1) & (i <= n * (n - 1))
        pl.when(passes & opens)(pass_before)
        pl.when(block_opens(i) == 1)(lambda: features(dest))
        pl.when(is_end & (i == 0))(lambda: process_half(arrive_at(2), half_last))

        @pl.when(column_opens(i) == 1)
        def _():
            pl.when(g == z)(lambda: pltpu.make_async_copy(out_block(z, f), out_block(z, f), lsem.at[1]).wait())
            relay_done(1, g)

        part[dest, :, cut(g)] = jnp.dot(
            mix[dest], wout[:, cut(g)], preferred_element_type=jnp.float32
        ).astype(jnp.bfloat16)
        pair_copy(dest, g).start()
        pl.when(passes & jnp.logical_not(opens))(pass_before)
        for k in range(2, n):
            pl.when(i == k - 2)(lambda k=k: relay_plane(1, order[1][k]))

        @pl.when(is_end)
        def _():
            pl.when(i == 0)(lambda: relay_tok(3, sides[1], 0))
            pl.when(i == third_block - 3)(lambda: relay_tok(3, sides[1], 1))

            @pl.when((i == 1) | (i == third_block - 2))
            def _():
                process_half(arrive_at(3), jnp.where(i == 1, half_first, half_last))

        return carry

    lax.fori_loop(0, n * n, step, 0)

    @pl.when(middle)
    def _():
        def passing(i, carry):
            pass_on(pass_block(i), pass_column(i))
            return carry

        lax.fori_loop(0, n * (n - 1), passing, 0)

    low, high = z > 0, z < n - 1

    def finish(turn, carry):
        g = column_at(turn)
        pair_copy(z, g).wait_recv()
        pl.when(low)(lambda: line_copy(1, z, g, z).wait_recv())
        pl.when(high)(lambda: line_copy(0, z, g, z).wait_recv())

        @pl.when(middle)
        def _():
            out[:, cut(g)] = (
                summed(z, g)
                + fetched[1, z, :, cut(g)].astype(jnp.float32)
                + fetched[0, z, :, cut(g)].astype(jnp.float32)
            ).astype(jnp.bfloat16)

        @pl.when(is_end)
        def _():
            d = jnp.where(low, 1, 0)
            out[:, cut(g)] = (
                summed(z, g) + fetched[d, z, :, cut(g)].astype(jnp.float32)
            ).astype(jnp.bfloat16)

        return carry

    lax.fori_loop(0, n, finish, 0)

    def sent(sem, ref):
        pltpu.make_async_copy(ref, ref, gone.at[sem]).wait()

    def by_place(sem, at_ends, at_middle):
        pl.when(is_end)(lambda: sent(sem, at_ends))
        pl.when(middle)(lambda: sent(sem, at_middle))

    whole = 4 * n - 1
    sent(0, win.at[0 : whole * rows, :])
    sent(1, wout.at[:, 0 : whole * out_cols])
    by_place(2, wlat.at[0 : (3 * n + 2) * rows, :], wlat.at[0 : 4 * n * rows, :])
    by_place(3, tok.at[:, 0:hr, :], tok.at[:, 0 : (n + 1) * hr, :])
    sent(4, tok.at[0])
    by_place(5, lat.at[:, 0 : 3 * tr, :], lat)
    by_place(6, krot.at[0 : 5 * hr, :], krot.at[0 : 7 * hr, :])
    sent(7, pair)
    sent(8, moving.at[0 : n - 1])


def split_shards(
    tokens,
    mix_gain,
    conv_b_weight,
    conv_c_weight,
    conv_v_weight,
    conv_taps,
    query_weight,
    query_rope_weight,
    latent_weight,
    key_rope_weight,
    latent_gain,
    key_up_weight,
    value_up_weight,
    head_gain,
    conv_out_weight,
    attn_out_weight,
):
    n = lax.axis_size("sp")
    tr = tokens.shape[1]
    wide = tokens.shape[2]
    length = n * tr
    features = 2 * wide
    heads = query_weight.shape[1] // NOPE // n
    channels = conv_b_weight.shape[1] // n
    low_rank = latent_weight.shape[1]
    proj_w = 3 * channels + heads * (NOPE + ROPE)
    out_rows = (conv_out_weight.shape[0] + attn_out_weight.shape[0]) // n
    columns = attn_out_weight.shape[1] * n * 4
    share = tr // 2
    head_rows = 16
    bf16, f32 = jnp.bfloat16, jnp.float32
    dma = pltpu.SemaphoreType.DMA
    operands = (
        tokens,
        mix_gain[None],
        latent_gain[None],
        head_gain[None],
        conv_taps,
        conv_b_weight,
        conv_c_weight,
        conv_v_weight,
        query_weight,
        query_rope_weight,
        latent_weight,
        key_rope_weight.T,
        key_up_weight,
        value_up_weight,
        conv_out_weight,
        attn_out_weight,
    )
    result = pl.pallas_call(
        functools.partial(layer_kernel, n, orders(n)),
        out_shape=jax.ShapeDtypeStruct((share, columns), bf16),
        in_specs=[pl.BlockSpec(memory_space=pltpu.HBM)] * 16,
        out_specs=pl.BlockSpec(memory_space=pltpu.VMEM),
        scratch_shapes=[
            pltpu.VMEM((2, length, wide), bf16),
            pltpu.VMEM((length, features), bf16),
            pltpu.VMEM((features, proj_w), bf16),
            pltpu.VMEM((out_rows, columns), bf16),
            pltpu.VMEM((features, low_rank // 2), bf16),
            pltpu.VMEM((2, length, low_rank // 2), bf16),
            pltpu.VMEM((length, 2 * ROPE), bf16),
            pltpu.VMEM((8, features), f32),
            pltpu.VMEM((2 * ROPE, features), bf16),
            pltpu.VMEM(conv_taps.shape, f32),
            pltpu.VMEM((8, low_rank), f32),
            pltpu.VMEM((low_rank, heads * NOPE), bf16),
            pltpu.VMEM((low_rank, heads * VD), bf16),
            pltpu.VMEM((8, heads * VD), f32),
            pltpu.VMEM((length, channels), bf16),
            pltpu.VMEM((length + head_rows, channels), bf16),
            pltpu.VMEM((length, heads * NOPE), bf16),
            pltpu.VMEM((length, heads * ROPE), bf16),
            pltpu.VMEM((heads, length, NOPE + 2 * ROPE), bf16),
            pltpu.VMEM((length, heads * VD), bf16),
            pltpu.VMEM((length, heads * ROPE), f32),
            pltpu.VMEM((length, heads * ROPE), f32),
            pltpu.VMEM((n, tr, columns), bf16),
            pltpu.VMEM((n, share, columns), bf16),
            pltpu.VMEM((n, share, columns), bf16),
            pltpu.VMEM((2, n, share, columns), bf16),
            dma((3, 4, n)),
            dma((5,)),
            dma((n, 2)),
            dma((n, 2)),
            dma((2, 2, n)),
            dma((8,)),
            dma((n, n)),
            dma((n + 1, n)),
            dma((9,)),
            pltpu.VMEM((n, tr, out_rows), bf16),
        ],
        compiler_params=pltpu.CompilerParams(
            collective_id=0, has_side_effects=True, vmem_limit_bytes=40 * 1024 * 1024
        ),
        name="whole_layer",
    )(*(pltpu.with_memory_space_constraint(operand, pltpu.HBM) for operand in operands))
    return result[None]


def splits_well(mesh):
    n = mesh.shape["sp"]
    return n == 4 and mesh.shape["fs"] == 4 and mesh.shape["tp"] == 2


def shards(*arrays):
    n = lax.axis_size("sp")
    conv, query, rope, low_rank = (arrays[i].shape[1] for i in (2, 6, 7, 8))
    heads = query // NOPE
    even = heads == n * 128 // ROPE and all(w % (128 * n) == 0 for w in (conv, query, rope, low_rank))
    if even and arrays[0].shape[1] % 32 == 0 and arrays[15].shape[1] % 128 == 0:
        return split_shards(*arrays)
    return general_shards(*arrays)


def solution(mesh):
    return jax.shard_map(
        shards if splits_well(mesh) else general_shards,
        mesh=mesh,
        in_specs=(
            P("fs", "sp", "tp"),
            P(),
            P(("sp", "fs"), "tp"),
            P(("sp", "fs"), "tp"),
            P(("sp", "fs"), "tp"),
            P(None, "tp"),
            P(("sp", "fs"), "tp"),
            P(("sp", "fs"), "tp"),
            P(("sp", "fs"), None),
            P(),
            P(),
            P(None, "tp"),
            P(None, "tp"),
            P("tp"),
            P("tp", ("sp", "fs")),
            P("tp", ("sp", "fs")),
        ),
        out_specs=P("fs", ("sp", "tp"), None),
        check_vma=False,
    )
```

```python
import functools
import math

import jax
import jax.numpy as jnp
from jax import lax
from jax.experimental import pallas as pl
from jax.experimental.pallas import tpu as pltpu
from jax.sharding import PartitionSpec as P

NOPE = 128
ROPE = 64
VD = 128
KVL = 512
SEG = 64


norm_epsilon = 1e-06
rope_theta = 10000.0


def passed_along(block, axis, distance):
    devices = range(lax.axis_size(axis))
    route = [(i - distance, i) for i in devices if i - distance in devices]
    return lax.ppermute(block, axis, route)


def rms_scale(values, gain):
    return (
        values * lax.rsqrt(jnp.mean(values * values, axis=-1, keepdims=True) + norm_epsilon) * gain
    )


def rope_tables(positions):
    half_width = ROPE // 2
    frequency = rope_theta ** (-jnp.arange(half_width, dtype=jnp.float32) * 2.0 / ROPE)
    angles = positions[:, None] * frequency[None, :]
    return (jnp.cos(angles), jnp.sin(angles))


def rotate(values, cosine, sine):
    half_width = ROPE // 2
    first = values[..., :half_width]
    second = values[..., half_width:]
    return jnp.concatenate(
        [first * cosine - second * sine, second * cosine + first * sine], axis=-1
    )


def general_shards(
    tokens,
    mix_gain,
    conv_b_weight,
    conv_c_weight,
    conv_v_weight,
    conv_taps,
    query_weight,
    query_rope_weight,
    latent_weight,
    key_rope_weight,
    latent_gain,
    key_up_weight,
    value_up_weight,
    head_gain,
    conv_out_weight,
    attn_out_weight,
):
    full_rows = lax.all_gather(tokens[0], "tp", axis=1, tiled=True)
    tok_rows = full_rows.shape[0]
    normed = rms_scale(full_rows.astype(jnp.float32), mix_gain).astype(jnp.bfloat16)
    offset = lax.axis_index("sp") * tok_rows
    token_index = offset + jnp.arange(tok_rows, dtype=jnp.int32)
    cosine, sine = rope_tables(token_index.astype(jnp.float32))
    local_heads = query_weight.shape[1] // NOPE
    count_sp = lax.axis_size("sp")
    count_fs = lax.axis_size("fs")
    count_tp = lax.axis_size("tp")
    fs_index = lax.axis_index("fs")
    row_piece = normed.shape[1] // (count_sp * count_fs)
    all_normed = lax.all_gather(normed, "fs", axis=0, tiled=True)
    picked = lax.dynamic_index_in_dim(
        all_normed.reshape(-1, count_sp, count_fs, row_piece), fs_index, 2, keepdims=False
    ).reshape(-1, count_sp * row_piece)
    gathered = (
        lax.all_gather(conv_b_weight, "sp", axis=0, tiled=True),
        lax.all_gather(conv_c_weight, "sp", axis=0, tiled=True),
        lax.all_gather(conv_v_weight, "sp", axis=0, tiled=True),
        lax.all_gather(query_weight, "sp", axis=0, tiled=True),
        lax.all_gather(query_rope_weight, "sp", axis=0, tiled=True),
        lax.all_gather(latent_weight, "sp", axis=0, tiled=True),
    )

    def project_in():
        return jnp.concatenate(
            [jnp.dot(picked, member, preferred_element_type=jnp.float32) for member in gathered],
            axis=1,
        )

    joined = lax.psum_scatter(
        project_in().astype(jnp.bfloat16), "fs", scatter_dimension=0, tiled=True
    ).astype(jnp.float32)
    bounds = []
    running_total = 0
    for member in gathered[:-1]:
        running_total = running_total + member.shape[1]
        bounds.append(running_total)
    sums = tuple(jnp.split(joined, bounds, axis=1))
    latent_raw = sums[5].astype(jnp.bfloat16)
    gate_b = sums[0].astype(jnp.bfloat16)
    gate_c = sums[1].astype(jnp.bfloat16)
    values_v = sums[2].astype(jnp.bfloat16)
    query_nope = sums[3].astype(jnp.bfloat16).reshape(tok_rows, local_heads, NOPE)
    query_rot = rotate(
        sums[4].reshape(tok_rows, local_heads, ROPE), cosine[:, None, :], sine[:, None, :]
    ).astype(jnp.bfloat16)
    latent = rms_scale(latent_raw.astype(jnp.float32), latent_gain).astype(jnp.bfloat16)
    key_rot = rotate(
        jnp.dot(normed, key_rope_weight, preferred_element_type=jnp.float32), cosine, sine
    ).astype(jnp.bfloat16)
    query_latent = jnp.einsum(
        "thn,khn->thk",
        query_nope,
        key_up_weight.reshape(KVL, local_heads, NOPE),
        preferred_element_type=jnp.float32,
    ).astype(jnp.bfloat16)
    attn_scale = (NOPE + ROPE) ** (-0.5)
    product = (gate_c.astype(jnp.float32) * values_v.astype(jnp.float32)).astype(jnp.bfloat16)
    previous = passed_along(product[tok_rows - 2 :], "sp", 1)
    padded = jnp.concatenate([previous, product], axis=0).astype(jnp.float32)
    convolved = (
        conv_taps[0] * padded[0:tok_rows]
        + conv_taps[1] * padded[1 : tok_rows + 1]
        + conv_taps[2] * padded[2 : tok_rows + 2]
    )
    conv_y = (gate_b.astype(jnp.float32) * convolved).astype(jnp.bfloat16)
    query_segment = token_index // SEG
    last_segment = (offset + tok_rows - 1) // SEG

    def key_block(running, latent_block, rot_block, first_key):
        peak_old, denom_old, accum_old = running
        block_rows = latent_block.shape[0]
        scores = (
            jnp.einsum(
                "thk,jk->thj", query_latent, latent_block, preferred_element_type=jnp.float32
            )
            + jnp.einsum("thr,jr->thj", query_rot, rot_block, preferred_element_type=jnp.float32)
        ) * attn_scale
        key_segment = (first_key + jnp.arange(block_rows, dtype=jnp.int32)) // SEG
        allowed = key_segment[None, None, :] <= query_segment[:, None, None]
        peak_new = jnp.maximum(peak_old, jnp.max(jnp.where(allowed, scores, -1e30), axis=-1))
        weights = jnp.where(allowed, jnp.exp(scores - peak_new[..., None]), 0.0)
        rescale = jnp.exp(peak_old - peak_new)
        denom_new = denom_old * rescale + jnp.sum(weights, axis=-1)
        accum_new = accum_old * rescale[..., None] + jnp.einsum(
            "thj,jk->thk",
            weights.astype(jnp.bfloat16),
            latent_block,
            preferred_element_type=jnp.float32,
        )
        return (peak_new, denom_new, accum_new)

    starting = (
        jnp.full((tok_rows, local_heads), -1e30, jnp.float32),
        jnp.zeros((tok_rows, local_heads), jnp.float32),
        jnp.zeros((tok_rows, local_heads, KVL), jnp.float32),
    )
    latent_piece = lax.all_gather(latent, "sp", axis=0, tiled=True)
    rot_piece = lax.all_gather(key_rot, "sp", axis=0, tiled=True)
    piece_rows = latent_piece.shape[0]
    splits = max(1, piece_rows // 512)
    while piece_rows % splits:
        splits = splits - 1
    block_rows = piece_rows // splits

    def visit(state, block_index):
        block_begin = block_index * block_rows
        latent_block = lax.dynamic_slice_in_dim(latent_piece, block_begin, block_rows, 0)
        rot_block = lax.dynamic_slice_in_dim(rot_piece, block_begin, block_rows, 0)
        updated = lax.cond(
            block_begin // SEG <= last_segment,
            lambda inner: key_block(inner, latent_block, rot_block, block_begin),
            lambda inner: inner,
            state,
        )
        return (updated, None)

    peak, denom, accum = lax.scan(visit, starting, jnp.arange(splits, dtype=jnp.int32))[0]
    attended = (accum / denom[..., None]).astype(jnp.bfloat16)
    head_out = jnp.einsum(
        "thk,khv->thv",
        attended,
        value_up_weight.reshape(KVL, local_heads, VD),
        preferred_element_type=jnp.float32,
    )
    normed_heads = rms_scale(head_out, head_gain.reshape(local_heads, VD))
    attn_y = normed_heads.astype(jnp.bfloat16).reshape(tok_rows, local_heads * VD)
    share_rows = tok_rows // count_tp
    conv_all, attn_all = (
        lax.all_gather(conv_y, "fs", axis=0, tiled=True),
        lax.all_gather(attn_y, "fs", axis=0, tiled=True),
    )
    conv_sorted = (
        conv_all.reshape(count_fs, count_tp, share_rows, -1)
        .transpose(1, 0, 2, 3)
        .reshape(count_fs * tok_rows, -1)
    )
    attn_sorted = (
        attn_all.reshape(count_fs, count_tp, share_rows, -1)
        .transpose(1, 0, 2, 3)
        .reshape(count_fs * tok_rows, -1)
    )
    conv_cols_sp, attn_cols_sp = (
        lax.all_gather(conv_out_weight, "sp", axis=1, tiled=True),
        lax.all_gather(attn_out_weight, "sp", axis=1, tiled=True),
    )
    col_sums = lax.psum_scatter(
        (
            jnp.dot(conv_sorted, conv_cols_sp, preferred_element_type=jnp.float32)
            + jnp.dot(attn_sorted, attn_cols_sp, preferred_element_type=jnp.float32)
        ).astype(jnp.bfloat16),
        "tp",
        scatter_dimension=0,
        tiled=True,
    )
    col_piece = conv_cols_sp.shape[1] // count_sp
    outgoing = col_sums.reshape(count_fs, share_rows, count_sp * col_piece)
    arrived = lax.all_to_all(outgoing, "fs", split_axis=0, concat_axis=2, tiled=True)
    result = (
        arrived.reshape(share_rows, count_fs, count_sp, col_piece)
        .transpose(0, 2, 1, 3)
        .reshape(share_rows, count_fs * count_sp * col_piece)
    )
    return result[None]


MESH = pl.DeviceIdType.MESH


class Place:
    def __init__(self):
        self.z = lax.axis_index("sp")
        self.f = lax.axis_index("fs")
        self.c = lax.axis_index("tp")

    def to(self, z=None, f=None, c=None):
        return {
            "sp": self.z if z is None else z,
            "fs": self.f if f is None else f,
            "tp": self.c if c is None else c,
        }


def flip(index, bit):
    digit = (index // bit) % 2
    return index + bit * (1 - 2 * digit)


def remote(src, dst, send, recv, device):
    return pltpu.make_async_remote_copy(
        src_ref=src, dst_ref=dst, send_sem=send, recv_sem=recv, device_id=device, device_id_type=MESH
    )


def greet(devices):
    barrier = pltpu.get_barrier_semaphore()
    for device in devices:
        pl.semaphore_signal(barrier, inc=1, device_id=device, device_id_type=MESH)
    pl.semaphore_wait(barrier, len(devices))


def orders(n):
    columns = sorted(range(n), key=lambda g: (max(g, n - 1 - g), g))
    arrival, steps, passes = [], [], []
    slots = {}
    for z in (0, n - 1):
        by = [abs(z - d) for d in range(n)]
        g = columns
        sent = [(by[d], g[k]) for d, k in ((1, 0), (1, 1), (2, 0), (2, 1), (3, 0), (3, 1), (3, 2), (3, 3), (1, 2), (2, 2), (2, 3), (1, 3))]
        slots[z] = sent
    for z in range(n):
        end = 0 if 2 * z < n else n - 1
        near = sorted((d for d in range(n) if d != z), key=lambda d: (abs(d - z), abs(d - end)))
        arrival.append([z] + near)
        if z == end:
            steps.append(slots[z] + [(z, g) for g in columns])
            passes.append([(z, 0)])
            continue
        opposite = n - 1 - end
        seen = [(i, step) for i, step in enumerate(slots[end]) if step[0] not in (z, end)]
        seen += [(i + 2.2, step) for i, step in enumerate(slots[opposite]) if step[0] == end]
        passes.append([step for _, step in sorted(seen)])
        steps.append([(d, g) for g in columns for d in near + [z]])
    first_column, first_block = [], []
    for listed in steps:
        blocks_seen, columns_seen, at_column, at_block = set(), set(), [], []
        for d, g in listed:
            at_column.append(n if g in columns_seen else columns.index(g))
            at_block.append(0 if d in blocks_seen else 1)
            columns_seen.add(g)
            blocks_seen.add(d)
        first_column.append(at_column)
        first_block.append(at_block)
    split = lambda table, i: [[pair[i] for pair in row] for row in table]
    return arrival, columns, split(steps, 0), split(steps, 1), first_column, first_block, split(passes, 0), split(passes, 1)


def layer_kernel(
    n,
    order,
    tok_in,
    mix_gain_in,
    lat_gain_in,
    head_gain_in,
    taps_in,
    cb,
    cc,
    cv,
    qw,
    qr,
    lw,
    krw_in,
    key_up_in,
    value_up_in,
    co,
    ao,
    out,
    tok,
    normed,
    win,
    wout,
    wlat,
    lat,
    krot,
    gain,
    krw,
    taps,
    lat_gain,
    key_up,
    value_up,
    head_gain,
    gate,
    prod,
    q_nope,
    q_rot,
    keys,
    values,
    cosine,
    sine,
    part,
    pair,
    moving,
    fetched,
    wsem,
    lsem,
    tsem,
    psem,
    latsem,
    ssem,
    pairsem,
    zsem,
    gone,
    mix,
):
    here = Place()
    z, f, c = here.z, here.f, here.c
    fx, fy = flip(f, 1), flip(f, 2)
    other = 1 - c
    is_end = (z == 0) | (z == n - 1)
    near = jnp.where(2 * z < n, -1, 1)
    sides = (near, -near)
    rows = cb.shape[0]
    members = (cb, cc, cv, qw, qr)
    widths = [m.shape[1] // n for m in members]
    starts = [sum(widths[:i]) for i in range(len(widths))]
    lat_half = lw.shape[1] // 2
    tr = tok_in.shape[1]
    hr = tr // 2
    length = n * tr
    outs = (co, ao)
    heights = [m.shape[0] // n for m in outs]
    tops = [sum(heights[:i]) for i in range(len(heights))]
    out_cols = co.shape[1]
    head_rows = prod.shape[0] - length

    steps = [(1 + j, s) for j in range(n - 1) for s in (-1, 1)]

    def chosen(table, t):
        found = jnp.int32(0)
        for zz in range(n):
            for tt in range(len(table[zz])):
                found = jnp.where((z == zz) & (t == tt), table[zz][tt], found)
        return found

    def arrive_at(t):
        return chosen(order[0], t)

    def packed(table, bits):
        words = []
        for row in table:
            word = sum(v << (bits * t) for t, v in enumerate(row))
            words.append(word - (1 << 32) if word >= 1 << 31 else word)
        mine = jnp.int32(words[0])
        for zz in range(1, n):
            mine = jnp.where(z == zz, jnp.int32(words[zz]), mine)
        return lambda t: jnp.right_shift(mine, bits * t) & ((1 << bits) - 1)

    step_block, step_column = packed(order[2], 2), packed(order[3], 2)
    column_opens = packed([[int(k < n) for k in row] for row in order[4]], 1)
    block_opens = packed(order[5], 1)
    pass_block, pass_column = packed(order[6], 2), packed(order[7], 2)
    column_at = packed([order[1]] * n, 2)

    greet(
        [here.to(z=lax.rem(z + j, n)) for j in range(1, n)]
        + [here.to(f=fx), here.to(f=fy), here.to(c=other)]
    )

    def in_block(zs, fs):
        return win.at[pl.ds(pl.multiple_of((zs * 4 + fs) * rows, rows), rows), :]

    def out_block(zs, fs):
        return wout.at[:, pl.ds(pl.multiple_of((zs * 4 + fs) * out_cols, out_cols), out_cols)]

    def low_block(zs, fs):
        return wlat.at[pl.ds(pl.multiple_of((zs * 4 + fs) * rows, rows), rows), :]

    blocks = (in_block, out_block, low_block)

    def pieces(kind, dest):
        found = []
        if kind == 0:
            dst = (z * 4 + f) * rows
            for m, w, s in zip(members, widths, starts):
                src = m.at[:, pl.ds(pl.multiple_of(dest * w, w), w)]
                found.append((src, win.at[pl.ds(pl.multiple_of(dst, rows), rows), pl.ds(s, w)]))
        elif kind == 1:
            dst = (z * 4 + f) * out_cols
            for m, h, s in zip(outs, heights, tops):
                src = m.at[pl.ds(pl.multiple_of(dest * h, h), h), :]
                found.append((src, wout.at[pl.ds(s, h), pl.ds(pl.multiple_of(dst, out_cols), out_cols)]))
        else:
            found.append((lw.at[:, pl.ds(pl.multiple_of(c * lat_half, lat_half), lat_half)], low_block(z, f)))
        return found

    def send_own(kind):
        for src, dst in pieces(kind, z):
            remote(src, dst, gone.at[kind], wsem.at[kind, 1, z], here.to(f=fx)).start()
            remote(src, dst, gone.at[kind], wsem.at[kind, 2, z], here.to(f=fy)).start()
            pltpu.make_async_copy(src, dst, lsem.at[kind]).start()

    def can(sign):
        return (z + sign >= 0) & (z + sign < n)

    def within(zs):
        return (zs >= 0) & (zs < n)

    def reached(distance, sign):
        dest = z + sign * distance
        if distance == 1:
            return within(dest)
        return (dest > 0) & (dest < n - 1)

    def serves(sign):
        return z + sign == jnp.where(sign > 0, n - 1, 0)

    def send_z(kind, distance, sign):
        dest = z + sign * distance

        @pl.when(reached(distance, sign) if kind == 2 else within(dest))
        def _():
            for src, dst in pieces(kind, dest):
                remote(src, dst, gone.at[kind], wsem.at[kind, 0, z], here.to(z=dest)).start()

    def plane_copy(kind, zs, role, fs, to):
        block = blocks[kind](zs, fs)
        return remote(block, block, gone.at[kind], wsem.at[kind, role, zs], here.to(f=to))

    def end_copy(zs, sign):
        block = low_block(zs, f)
        return remote(block, block, gone.at[2], wsem.at[2, 0, zs], here.to(z=z + sign))

    def relay_z(kind, distance, sign):
        zs = z + sign * distance

        @pl.when(within(zs))
        def _():
            block = blocks[kind](zs, f)
            remote(block, block, gone.at[kind], wsem.at[kind, 0, zs], here.to(z=zs)).wait_recv()
            if kind == 2:
                pl.when(serves(-sign))(lambda: end_copy(zs, -sign).start())
            plane_copy(kind, zs, 1, f, fx).start()
            plane_copy(kind, zs, 2, f, fy).start()

    def relay_plane(kind, zs):
        plane_copy(kind, zs, 1, fx, fx).wait_recv()

        @pl.when(zs % 2 == 0)
        def _():
            plane_copy(kind, zs, 3, fx, fy).start()

        plane_copy(kind, zs, 2, fy, fy).wait_recv()

        @pl.when(zs % 2 == 1)
        def _():
            plane_copy(kind, zs, 3, fy, fx).start()

    def relay_done(kind, zs):
        plane_copy(kind, zs, 3, flip(fx, 2), fx).wait_recv()

    def tok_block(owner, zs, i):
        return tok.at[owner, pl.ds(pl.multiple_of(zs * tr + i * hr, hr), hr), :]

    def half_at(sign, i):
        return jnp.where(sign > 0, 1 - i, i)

    own_tok = [tok_in.at[0, i * hr : (i + 1) * hr, :] for i in range(2)]

    def tok_copy(zs, sign, hop, i, src=None):
        block = tok_block(c, zs, i)
        return remote(
            block if src is None else src, block, gone.at[3], tsem.at[zs, i], here.to(z=z + sign)
        )

    def partner_copy(zs, owner, i, src=None):
        block = tok_block(owner, zs, i)
        return remote(
            block if src is None else src, block, gone.at[4], psem.at[zs, i], here.to(c=other)
        )

    def own_copy(i):
        return pltpu.make_async_copy(own_tok[i], tok_block(c, z, i), lsem.at[3 + i])

    channels = widths[0]
    heads = widths[3] // NOPE
    rot_w = widths[4]
    share = tr // 2

    def columns_of(array, width):
        return array.at[:, pl.ds(pl.multiple_of(z * width, width), width)]

    small = [
        (mix_gain_in, gain.at[0:1, :]),
        (krw_in, krw.at[0:ROPE, :]),
        (krw_in, krw.at[ROPE : 2 * ROPE, :]),
        (taps_in, taps),
        (lat_gain_in, lat_gain.at[0:1, :]),
        (columns_of(key_up_in, heads * NOPE), key_up),
        (columns_of(value_up_in, heads * VD), value_up),
        (columns_of(head_gain_in, heads * VD), head_gain.at[0:1, :]),
    ]

    send_own(2)
    for distance, sign in steps:
        send_z(2, distance, sign)
    for i in range(2):
        partner_copy(z, c, i, own_tok[i]).start()
        own_copy(i).start()
    send_own(0)
    middle = jnp.logical_not(is_end)

    def send_far_first(kind):
        for distance in (2, 1):
            for sign in (-1, 1):
                send_z(kind, distance, sign)

    def send_near_first(kind):
        for distance, sign in steps:
            send_z(kind, distance, sign)

    def send_toks():
        for sign in (-1, 1):
            for i in (1, 0) if sign > 0 else (0, 1):
                pl.when(can(sign))(lambda sign=sign, i=i: tok_copy(z, sign, 0, i, own_tok[i]).start())

    pl.when(middle)(lambda: send_far_first(0))

    @pl.when(is_end)
    def _():
        send_near_first(0)
        send_toks()


    for i, (src, dst) in enumerate(small):
        pltpu.make_async_copy(src, dst, ssem.at[i]).start()

    def relay_tok(distance, sign, i):
        zs = z + sign * distance

        @pl.when(within(zs))
        def _():
            half = half_at(-sign, i)
            tok_copy(zs, -sign, distance - 1, half).wait_recv()
            if distance < n - 1:
                pl.when(can(-sign))(lambda: tok_copy(zs, -sign, distance, half).start())
            partner_copy(zs, c, half).start()

    def relay_toks(distance, sides=sides):
        for sign in sides:
            for i in range(2):
                relay_tok(distance, sign, i)

    def each_zs(fn):
        def body(i, carry):
            fn(lax.rem(z + i, n))
            return carry

        lax.fori_loop(0, n, body, 0)

    def at_distance(distance, fn):
        for sign in sides:
            zs = z + sign * distance
            pl.when(within(zs))(lambda zs=zs: fn(zs))

    lane = lax.broadcasted_iota(jnp.int32, (tr, rot_w), 1)
    quarter = lane % (ROPE // 2)
    first_half = (lane % ROPE) < ROPE // 2
    frequency = jnp.exp(quarter.astype(jnp.float32) * (-2.0 / ROPE * math.log(rope_theta)))

    def tables(i, carry):
        at = pl.ds(pl.multiple_of(i * tr, tr), tr)
        position = (i * tr + lax.broadcasted_iota(jnp.int32, (tr, rot_w), 0)).astype(jnp.float32)
        angle = position * frequency
        cosine[at, :] = jnp.cos(angle)
        turned = jnp.sin(angle)
        sine[at, :] = jnp.where(first_half, -turned, turned)
        return carry

    lax.fori_loop(0, n, tables, 0)
    prod[0:head_rows, :] = jnp.zeros((head_rows, channels), prod.dtype)

    def rotated(x, at):
        low_half = (lax.broadcasted_iota(jnp.int32, x.shape, 1) % ROPE) < ROPE // 2
        swapped = jnp.where(low_half, pltpu.roll(x, rot_w - ROPE // 2, 1), pltpu.roll(x, ROPE // 2, 1))
        return (x * cosine[at, :] + swapped * sine[at, :]).astype(jnp.bfloat16)

    for i, (src, dst) in enumerate(small):
        pltpu.make_async_copy(src, dst, ssem.at[i]).wait()
    wide = tok.shape[2]

    def half_rows(zs, i):
        return pl.ds(pl.multiple_of(zs * tr + i * hr, hr), hr)

    def norm_half(zs, i):
        partner_copy(zs, other, i).wait_recv()
        at = half_rows(zs, i)
        first = tok[0, at, :].astype(jnp.float32)
        second = tok[1, at, :].astype(jnp.float32)
        mean = (
            jnp.sum(first * first, axis=-1, keepdims=True) + jnp.sum(second * second, axis=-1, keepdims=True)
        ) / (2 * wide)
        scale = lax.rsqrt(mean + norm_epsilon)
        normed[at, 0:wide] = (first * scale * gain[0:1, 0:wide]).astype(jnp.bfloat16)
        normed[at, wide : 2 * wide] = (second * scale * gain[0:1, wide : 2 * wide]).astype(jnp.bfloat16)

    def norm_block(zs):
        def body(i, carry):
            norm_half(zs, i)
            return carry

        lax.fori_loop(0, 2, body, 0)

    def rows_of(zs):
        return pl.ds(pl.multiple_of(zs * tr, tr), tr)

    def lat_block(zs, owner):
        return lat.at[owner, rows_of(zs), :]

    def rot_block(zs, owner):
        return krot.at[pl.ds(pl.multiple_of(zs * tr + owner * hr, hr), hr), :]

    shared = (lat_block, rot_block)

    def lat_copy(k, dest):
        block = shared[k](z, c)
        return remote(block, block, gone.at[5 + k], latsem.at[k, 0, z], here.to(z=dest))

    def lat_arrival(k, zs):
        block = shared[k](zs, c)
        return remote(block, block, gone.at[5 + k], latsem.at[k, 0, zs], here.to(z=zs))

    def lat_forward(k, zs, sign):
        block = shared[k](zs, c)
        return remote(block, block, gone.at[5 + k], latsem.at[k, 0, zs], here.to(z=z + sign))

    def lat_partner(k, zs, owner):
        block = shared[k](zs, owner)
        return remote(block, block, gone.at[5 + k], latsem.at[k, 1, zs], here.to(c=other))

    def relay_lat(distance, sides=sides):
        for sign in sides:
            zs = z + sign * distance

            @pl.when(within(zs))
            def _(zs=zs, sign=sign):
                for k in range(2):
                    lat_arrival(k, zs).wait_recv()
                    pl.when(serves(-sign))(lambda k=k: lat_forward(k, zs, -sign).start())
                    lat_partner(k, zs, c).start()

    def own_latents():
        at = rows_of(z)
        block = normed[at, :]
        lat[c, at, :] = jnp.dot(block, wlat[...], preferred_element_type=jnp.float32).astype(jnp.bfloat16)
        key_raw = lax.dot_general(
            block, krw[...], (((1,), (1,)), ((), ())), preferred_element_type=jnp.float32
        )
        krot[at, :] = rotated(key_raw, at)

    def relay_weights_z(distance):
        for sign in (-1, 1):
            for kind in (0, 1):
                relay_z(kind, distance, sign)

    def relay_weights_plane(zs):
        for kind in (0, 1):
            relay_plane(kind, zs)

    def relay_all_z(kind, distance):
        for sign in sides:
            relay_z(kind, distance, sign)

    def diagonals(kind, distance):
        at_distance(distance, lambda zs: relay_plane(kind, zs))

    def share_latents():
        pltpu.make_async_copy(low_block(z, f), low_block(z, f), lsem.at[2]).wait()
        each_zs(lambda zs: relay_done(2, zs))
        own_latents()
        for distance, sign in steps:
            dest = z + sign * distance

            @pl.when(reached(distance, sign))
            def _(dest=dest):
                for k in range(2):
                    lat_copy(k, dest).start()

        lat_partner(0, z, c).start()

    relay_all_z(2, 1)
    relay_plane(2, z)
    for i in range(2):
        own_copy(i).wait()
    norm_block(z)

    @pl.when(is_end)
    def _():
        relay_plane(0, z)
        send_own(1)
        for distance in range(2, n):
            relay_all_z(2, distance)
        relay_all_z(0, 1)
        for distance in range(1, n):
            diagonals(2, distance)
        relay_all_z(0, 2)
        relay_all_z(0, 3)
        share_latents()
        diagonals(0, 1)
        send_near_first(1)
        diagonals(0, 2)
        diagonals(0, 3)
        relay_lat(1)
        relay_toks(1)

    @pl.when(middle)
    def _():
        relay_all_z(2, 2)
        relay_plane(0, z)
        diagonals(2, 1)
        diagonals(2, 2)
        relay_z(0, 1, near)
        relay_all_z(0, 2)
        share_latents()
        send_toks()
        send_far_first(1)
        relay_plane(0, z + near)
        relay_z(0, 1, -near)
        diagonals(0, 2)
        relay_lat(1, sides[1:])
        relay_toks(1, sides[:1])
        send_own(1)
        relay_plane(0, z - near)
        relay_lat(1, sides[:1])
        relay_lat(2)
        relay_toks(1, sides[1:])

    pltpu.make_async_copy(in_block(z, f), in_block(z, f), lsem.at[0]).wait()
    each_zs(lambda zs: relay_done(0, zs))

    @pl.when(is_end)
    def _():
        pl.when(z == 0)(lambda: relay_all_z(1, 1))
        relay_all_z(1, 2)
        pl.when(z != 0)(lambda: relay_all_z(1, 1))

    pl.when(middle)(lambda: relay_z(1, 1, -near))
    norm_block(arrive_at(1))

    def project_rows(first_row, count):
        at = pl.ds(pl.multiple_of(first_row, hr), count)
        joined = jnp.dot(normed[at, :], win[...], preferred_element_type=jnp.float32)
        gates = joined[:, channels : 3 * channels].astype(jnp.bfloat16).astype(jnp.float32)
        gate[at, :] = joined[:, 0:channels].astype(jnp.bfloat16)
        below = pl.ds(pl.multiple_of(first_row + head_rows, head_rows), count)
        prod[below, :] = (gates[:, 0:channels] * gates[:, channels : 2 * channels]).astype(jnp.bfloat16)
        start = 3 * channels
        q_nope[at, :] = joined[:, start : start + heads * NOPE].astype(jnp.bfloat16)
        q_rot[at, :] = rotated(joined[:, start + heads * NOPE :], at)

    def project_half(zs, i):
        project_rows(zs * tr + i * hr, hr)

    def project_arrived(t, carry):
        project_rows(arrive_at(t) * tr, tr)
        return carry

    lax.fori_loop(0, 2, project_arrived, 0)

    @pl.when(is_end)
    def _():
        relay_lat(2)
        relay_lat(3)


    def lat_waits(zs):
        lat_partner(0, zs, other).wait_recv()
        pl.when(zs != z)(lambda: lat_partner(1, zs, other).wait_recv())

    def expand(i, carry):
        lat_waits(i)
        at = rows_of(i)
        raw = jnp.concatenate([lat[0, at, :], lat[1, at, :]], axis=1).astype(jnp.float32)
        mean = jnp.mean(raw * raw, axis=-1, keepdims=True)
        low = (raw * lax.rsqrt(mean + norm_epsilon) * lat_gain[0:1, :]).astype(jnp.bfloat16)
        wide_keys = jnp.dot(low, key_up[...], preferred_element_type=jnp.float32).astype(jnp.bfloat16)
        key_rot = krot[at, :]
        for h in range(heads):
            keys[h, at, 0:NOPE] = wide_keys[:, h * NOPE : (h + 1) * NOPE]
            keys[h, at, NOPE:] = key_rot
        values[at, :] = jnp.dot(low, value_up[...], preferred_element_type=jnp.float32).astype(jnp.bfloat16)
        return carry

    lax.fori_loop(0, n, expand, 0)
    relay_plane(1, order[1][0])
    pl.when(is_end)(lambda: relay_all_z(1, 3))

    @pl.when(middle)
    def _():
        relay_z(1, 1, near)
        relay_all_z(1, 2)
        relay_toks(2)


    shift = SEG.bit_length() - 1
    row_index = lax.broadcasted_iota(jnp.int32, (tr, length), 0)
    key_segment = jnp.right_shift(lax.broadcasted_iota(jnp.int32, (tr, length), 1), shift)
    own_lanes = lane // ROPE
    own_channels = pl.ds(pl.multiple_of(z * channels, channels), channels)

    def features(dest):
        at = rows_of(dest)
        allowed = key_segment <= jnp.right_shift(row_index + dest * tr, shift)
        padded = prod[pl.ds(pl.multiple_of(dest * tr, head_rows), tr + head_rows), :].astype(jnp.float32)
        convolved = (
            taps[0:1, own_channels] * pltpu.roll(padded, 2, 0)[head_rows:]
            + taps[1:2, own_channels] * pltpu.roll(padded, 1, 0)[head_rows:]
            + taps[2:3, own_channels] * padded[head_rows:]
        )
        outputs = [(gate[at, :].astype(jnp.float32) * convolved).astype(jnp.bfloat16)]
        rot = q_rot[at, :]
        for h in range(heads):
            query = jnp.concatenate(
                [
                    q_nope[at, h * NOPE : (h + 1) * NOPE],
                    jnp.where(own_lanes == h, rot, jnp.zeros_like(rot)),
                ],
                axis=1,
            )
            scores = lax.dot_general(
                query, keys[h], (((1,), (1,)), ((), ())), preferred_element_type=jnp.float32
            ) * (NOPE + ROPE) ** (-0.5)
            scores = jnp.where(allowed, scores, -1e30)
            weights = jnp.exp(scores - jnp.max(scores, axis=-1, keepdims=True))
            denom = jnp.sum(weights, axis=-1, keepdims=True)
            head_out = (
                jnp.dot(
                    weights.astype(jnp.bfloat16),
                    values[:, h * VD : (h + 1) * VD],
                    preferred_element_type=jnp.float32,
                )
                / denom
            )
            mean = jnp.mean(head_out * head_out, axis=-1, keepdims=True)
            gained = head_out * lax.rsqrt(mean + norm_epsilon) * head_gain[0:1, h * VD : (h + 1) * VD]
            outputs.append(gained.astype(jnp.bfloat16))
        mix[dest] = jnp.concatenate(outputs, axis=1)

    piece_w = wout.shape[1] // n

    def cut(g):
        return pl.ds(pl.multiple_of(g * piece_w, piece_w), piece_w)

    def own_rows():
        return pl.ds(pl.multiple_of(c * share, share), share)

    def pair_copy(dest, g):
        theirs = pl.ds(pl.multiple_of(other * share, share), share)
        return remote(
            part.at[dest, theirs, cut(g)],
            pair.at[dest, :, cut(g)],
            gone.at[7],
            pairsem.at[dest, g],
            here.to(c=other),
        )

    def line_copy(d, dest, g, target):
        row = jnp.where((dest == target) & (d == 1), n, dest)
        return remote(
            moving.at[dest, :, cut(g)],
            fetched.at[d, dest, :, cut(g)],
            gone.at[8],
            zsem.at[row, g],
            here.to(z=z + 2 * d - 1),
        )

    def line_send(d, dest, g):
        line_copy(d, dest, g, z + 2 * d - 1).start()

    def summed(dest, g):
        kept = part[dest, own_rows(), cut(g)]
        return kept.astype(jnp.float32) + pair[dest, :, cut(g)].astype(jnp.float32)

    def toward(dest):
        return jnp.where(dest > z, 1, 0)

    def pass_first(dest, g):
        pair_copy(dest, g).wait_recv()
        moving[dest, :, cut(g)] = summed(dest, g).astype(jnp.bfloat16)
        line_send(toward(dest), dest, g)

    def pass_on(dest, g):
        d = toward(dest)
        pair_copy(dest, g).wait_recv()
        line_copy(d, dest, g, z).wait_recv()
        moving[dest, :, cut(g)] = (
            summed(dest, g) + fetched[d, dest, :, cut(g)].astype(jnp.float32)
        ).astype(jnp.bfloat16)
        line_send(d, dest, g)

    def process_half(zs, i):
        norm_half(zs, i)
        project_half(zs, i)

    @pl.when(middle)
    def _():
        def rest(t, carry):
            norm_block(arrive_at(t))
            return project_arrived(t, carry)

        lax.fori_loop(2, n, rest, 0)

    half_first = half_at(-sides[1], 0)
    half_last = 1 - half_first

    @pl.when(is_end)
    def _():
        relay_tok(2, sides[1], 0)
        relay_tok(2, sides[1], 1)
        process_half(arrive_at(2), half_first)

    relay_plane(1, order[1][1])


    second_block, third_block = [i for i, opens in enumerate(order[5][0]) if opens][1:3]

    def step(i, carry):
        dest, g = step_block(i), step_column(i)
        before = jnp.maximum(i - 1, 0)

        def pass_before():
            pass_first(step_block(before), step_column(before))

        early = (i == 1) | (i == 2)
        passes = is_end & (i >= 1) & (i <= n * (n - 1))
        pl.when(passes & early)(pass_before)
        pl.when(block_opens(i) == 1)(lambda: features(dest))
        pl.when(passes & (i == third_block))(pass_before)

        @pl.when(column_opens(i) == 1)
        def _():
            pl.when(g == z)(lambda: pltpu.make_async_copy(out_block(z, f), out_block(z, f), lsem.at[1]).wait())
            relay_done(1, g)

        part[dest, :, cut(g)] = jnp.dot(
            mix[dest], wout[:, cut(g)], preferred_element_type=jnp.float32
        ).astype(jnp.bfloat16)
        pair_copy(dest, g).start()
        pl.when(passes & jnp.logical_not(early | (i == third_block)))(pass_before)
        pl.when(is_end & (i == 0))(lambda: process_half(arrive_at(2), half_last))
        for k in range(2, n):
            pl.when(i == k - 2)(lambda k=k: relay_plane(1, order[1][k]))

        @pl.when(is_end)
        def _():
            pl.when(i == 0)(lambda: relay_tok(3, sides[1], 0))
            pl.when(i == third_block - 3)(lambda: relay_tok(3, sides[1], 1))

            @pl.when((i == 1) | (i == third_block - 2))
            def _():
                process_half(arrive_at(3), jnp.where(i == 1, half_first, half_last))

        return carry

    lax.fori_loop(0, n * n, step, 0)

    @pl.when(middle)
    def _():
        def passing(i, carry):
            pass_on(pass_block(i), pass_column(i))
            return carry

        lax.fori_loop(0, n * (n - 1), passing, 0)

    low, high = z > 0, z < n - 1

    def finish(turn, carry):
        g = column_at(turn)
        pair_copy(z, g).wait_recv()
        pl.when(low)(lambda: line_copy(1, z, g, z).wait_recv())
        pl.when(high)(lambda: line_copy(0, z, g, z).wait_recv())

        @pl.when(middle)
        def _():
            out[:, cut(g)] = (
                summed(z, g)
                + fetched[1, z, :, cut(g)].astype(jnp.float32)
                + fetched[0, z, :, cut(g)].astype(jnp.float32)
            ).astype(jnp.bfloat16)

        @pl.when(is_end)
        def _():
            d = jnp.where(low, 1, 0)
            out[:, cut(g)] = (
                summed(z, g) + fetched[d, z, :, cut(g)].astype(jnp.float32)
            ).astype(jnp.bfloat16)

        return carry

    lax.fori_loop(0, n, finish, 0)

    def sent(sem, ref):
        pltpu.make_async_copy(ref, ref, gone.at[sem]).wait()

    def by_place(sem, at_ends, at_middle):
        pl.when(is_end)(lambda: sent(sem, at_ends))
        pl.when(middle)(lambda: sent(sem, at_middle))

    whole = 4 * n - 1
    sent(0, win.at[0 : whole * rows, :])
    sent(1, wout.at[:, 0 : whole * out_cols])
    by_place(2, wlat.at[0 : (3 * n + 2) * rows, :], wlat.at[0 : 4 * n * rows, :])
    by_place(3, tok.at[:, 0:hr, :], tok.at[:, 0 : (n + 1) * hr, :])
    sent(4, tok.at[0])
    by_place(5, lat.at[:, 0 : 3 * tr, :], lat)
    by_place(6, krot.at[0 : 5 * hr, :], krot.at[0 : 7 * hr, :])
    sent(7, pair)
    sent(8, moving.at[0 : n - 1])


def split_shards(
    tokens,
    mix_gain,
    conv_b_weight,
    conv_c_weight,
    conv_v_weight,
    conv_taps,
    query_weight,
    query_rope_weight,
    latent_weight,
    key_rope_weight,
    latent_gain,
    key_up_weight,
    value_up_weight,
    head_gain,
    conv_out_weight,
    attn_out_weight,
):
    n = lax.axis_size("sp")
    tr = tokens.shape[1]
    wide = tokens.shape[2]
    length = n * tr
    features = 2 * wide
    heads = query_weight.shape[1] // NOPE // n
    channels = conv_b_weight.shape[1] // n
    low_rank = latent_weight.shape[1]
    proj_w = 3 * channels + heads * (NOPE + ROPE)
    out_rows = (conv_out_weight.shape[0] + attn_out_weight.shape[0]) // n
    columns = attn_out_weight.shape[1] * n * 4
    share = tr // 2
    head_rows = 16
    bf16, f32 = jnp.bfloat16, jnp.float32
    dma = pltpu.SemaphoreType.DMA
    operands = (
        tokens,
        mix_gain[None],
        latent_gain[None],
        head_gain[None],
        conv_taps,
        conv_b_weight,
        conv_c_weight,
        conv_v_weight,
        query_weight,
        query_rope_weight,
        latent_weight,
        key_rope_weight.T,
        key_up_weight,
        value_up_weight,
        conv_out_weight,
        attn_out_weight,
    )
    result = pl.pallas_call(
        functools.partial(layer_kernel, n, orders(n)),
        out_shape=jax.ShapeDtypeStruct((share, columns), bf16),
        in_specs=[pl.BlockSpec(memory_space=pltpu.HBM)] * 16,
        out_specs=pl.BlockSpec(memory_space=pltpu.VMEM),
        scratch_shapes=[
            pltpu.VMEM((2, length, wide), bf16),
            pltpu.VMEM((length, features), bf16),
            pltpu.VMEM((features, proj_w), bf16),
            pltpu.VMEM((out_rows, columns), bf16),
            pltpu.VMEM((features, low_rank // 2), bf16),
            pltpu.VMEM((2, length, low_rank // 2), bf16),
            pltpu.VMEM((length, 2 * ROPE), bf16),
            pltpu.VMEM((8, features), f32),
            pltpu.VMEM((2 * ROPE, features), bf16),
            pltpu.VMEM(conv_taps.shape, f32),
            pltpu.VMEM((8, low_rank), f32),
            pltpu.VMEM((low_rank, heads * NOPE), bf16),
            pltpu.VMEM((low_rank, heads * VD), bf16),
            pltpu.VMEM((8, heads * VD), f32),
            pltpu.VMEM((length, channels), bf16),
            pltpu.VMEM((length + head_rows, channels), bf16),
            pltpu.VMEM((length, heads * NOPE), bf16),
            pltpu.VMEM((length, heads * ROPE), bf16),
            pltpu.VMEM((heads, length, NOPE + 2 * ROPE), bf16),
            pltpu.VMEM((length, heads * VD), bf16),
            pltpu.VMEM((length, heads * ROPE), f32),
            pltpu.VMEM((length, heads * ROPE), f32),
            pltpu.VMEM((n, tr, columns), bf16),
            pltpu.VMEM((n, share, columns), bf16),
            pltpu.VMEM((n, share, columns), bf16),
            pltpu.VMEM((2, n, share, columns), bf16),
            dma((3, 4, n)),
            dma((5,)),
            dma((n, 2)),
            dma((n, 2)),
            dma((2, 2, n)),
            dma((8,)),
            dma((n, n)),
            dma((n + 1, n)),
            dma((9,)),
            pltpu.VMEM((n, tr, out_rows), bf16),
        ],
        compiler_params=pltpu.CompilerParams(
            collective_id=0, has_side_effects=True, vmem_limit_bytes=40 * 1024 * 1024
        ),
        name="whole_layer",
    )(*(pltpu.with_memory_space_constraint(operand, pltpu.HBM) for operand in operands))
    return result[None]


def splits_well(mesh):
    n = mesh.shape["sp"]
    return n == 4 and mesh.shape["fs"] == 4 and mesh.shape["tp"] == 2


def shards(*arrays):
    n = lax.axis_size("sp")
    conv, query, rope, low_rank = (arrays[i].shape[1] for i in (2, 6, 7, 8))
    heads = query // NOPE
    even = heads == n * 128 // ROPE and all(w % (128 * n) == 0 for w in (conv, query, rope, low_rank))
    if even and arrays[0].shape[1] % 32 == 0 and arrays[15].shape[1] % 128 == 0:
        return split_shards(*arrays)
    return general_shards(*arrays)


def solution(mesh):
    return jax.shard_map(
        shards if splits_well(mesh) else general_shards,
        mesh=mesh,
        in_specs=(
            P("fs", "sp", "tp"),
            P(),
            P(("sp", "fs"), "tp"),
            P(("sp", "fs"), "tp"),
            P(("sp", "fs"), "tp"),
            P(None, "tp"),
            P(("sp", "fs"), "tp"),
            P(("sp", "fs"), "tp"),
            P(("sp", "fs"), None),
            P(),
            P(),
            P(None, "tp"),
            P(None, "tp"),
            P("tp"),
            P("tp", ("sp", "fs")),
            P("tp", ("sp", "fs")),
        ),
        out_specs=P("fs", ("sp", "tp"), None),
        check_vma=False,
    )
```

```python
import functools
import math

import jax
import jax.numpy as jnp
from jax import lax
from jax.experimental import pallas as pl
from jax.experimental.pallas import tpu as pltpu
from jax.sharding import PartitionSpec as P

NOPE = 128
ROPE = 64
VD = 128
KVL = 512
SEG = 64


norm_epsilon = 1e-06
rope_theta = 10000.0


def passed_along(block, axis, distance):
    devices = range(lax.axis_size(axis))
    route = [(i - distance, i) for i in devices if i - distance in devices]
    return lax.ppermute(block, axis, route)


def rms_scale(values, gain):
    return (
        values * lax.rsqrt(jnp.mean(values * values, axis=-1, keepdims=True) + norm_epsilon) * gain
    )


def rope_tables(positions):
    half_width = ROPE // 2
    frequency = rope_theta ** (-jnp.arange(half_width, dtype=jnp.float32) * 2.0 / ROPE)
    angles = positions[:, None] * frequency[None, :]
    return (jnp.cos(angles), jnp.sin(angles))


def rotate(values, cosine, sine):
    half_width = ROPE // 2
    first = values[..., :half_width]
    second = values[..., half_width:]
    return jnp.concatenate(
        [first * cosine - second * sine, second * cosine + first * sine], axis=-1
    )


def general_shards(
    tokens,
    mix_gain,
    conv_b_weight,
    conv_c_weight,
    conv_v_weight,
    conv_taps,
    query_weight,
    query_rope_weight,
    latent_weight,
    key_rope_weight,
    latent_gain,
    key_up_weight,
    value_up_weight,
    head_gain,
    conv_out_weight,
    attn_out_weight,
):
    full_rows = lax.all_gather(tokens[0], "tp", axis=1, tiled=True)
    tok_rows = full_rows.shape[0]
    normed = rms_scale(full_rows.astype(jnp.float32), mix_gain).astype(jnp.bfloat16)
    offset = lax.axis_index("sp") * tok_rows
    token_index = offset + jnp.arange(tok_rows, dtype=jnp.int32)
    cosine, sine = rope_tables(token_index.astype(jnp.float32))
    local_heads = query_weight.shape[1] // NOPE
    count_sp = lax.axis_size("sp")
    count_fs = lax.axis_size("fs")
    count_tp = lax.axis_size("tp")
    fs_index = lax.axis_index("fs")
    row_piece = normed.shape[1] // (count_sp * count_fs)
    all_normed = lax.all_gather(normed, "fs", axis=0, tiled=True)
    picked = lax.dynamic_index_in_dim(
        all_normed.reshape(-1, count_sp, count_fs, row_piece), fs_index, 2, keepdims=False
    ).reshape(-1, count_sp * row_piece)
    gathered = (
        lax.all_gather(conv_b_weight, "sp", axis=0, tiled=True),
        lax.all_gather(conv_c_weight, "sp", axis=0, tiled=True),
        lax.all_gather(conv_v_weight, "sp", axis=0, tiled=True),
        lax.all_gather(query_weight, "sp", axis=0, tiled=True),
        lax.all_gather(query_rope_weight, "sp", axis=0, tiled=True),
        lax.all_gather(latent_weight, "sp", axis=0, tiled=True),
    )

    def project_in():
        return jnp.concatenate(
            [jnp.dot(picked, member, preferred_element_type=jnp.float32) for member in gathered],
            axis=1,
        )

    joined = lax.psum_scatter(
        project_in().astype(jnp.bfloat16), "fs", scatter_dimension=0, tiled=True
    ).astype(jnp.float32)
    bounds = []
    running_total = 0
    for member in gathered[:-1]:
        running_total = running_total + member.shape[1]
        bounds.append(running_total)
    sums = tuple(jnp.split(joined, bounds, axis=1))
    latent_raw = sums[5].astype(jnp.bfloat16)
    gate_b = sums[0].astype(jnp.bfloat16)
    gate_c = sums[1].astype(jnp.bfloat16)
    values_v = sums[2].astype(jnp.bfloat16)
    query_nope = sums[3].astype(jnp.bfloat16).reshape(tok_rows, local_heads, NOPE)
    query_rot = rotate(
        sums[4].reshape(tok_rows, local_heads, ROPE), cosine[:, None, :], sine[:, None, :]
    ).astype(jnp.bfloat16)
    latent = rms_scale(latent_raw.astype(jnp.float32), latent_gain).astype(jnp.bfloat16)
    key_rot = rotate(
        jnp.dot(normed, key_rope_weight, preferred_element_type=jnp.float32), cosine, sine
    ).astype(jnp.bfloat16)
    query_latent = jnp.einsum(
        "thn,khn->thk",
        query_nope,
        key_up_weight.reshape(KVL, local_heads, NOPE),
        preferred_element_type=jnp.float32,
    ).astype(jnp.bfloat16)
    attn_scale = (NOPE + ROPE) ** (-0.5)
    product = (gate_c.astype(jnp.float32) * values_v.astype(jnp.float32)).astype(jnp.bfloat16)
    previous = passed_along(product[tok_rows - 2 :], "sp", 1)
    padded = jnp.concatenate([previous, product], axis=0).astype(jnp.float32)
    convolved = (
        conv_taps[0] * padded[0:tok_rows]
        + conv_taps[1] * padded[1 : tok_rows + 1]
        + conv_taps[2] * padded[2 : tok_rows + 2]
    )
    conv_y = (gate_b.astype(jnp.float32) * convolved).astype(jnp.bfloat16)
    query_segment = token_index // SEG
    last_segment = (offset + tok_rows - 1) // SEG

    def key_block(running, latent_block, rot_block, first_key):
        peak_old, denom_old, accum_old = running
        block_rows = latent_block.shape[0]
        scores = (
            jnp.einsum(
                "thk,jk->thj", query_latent, latent_block, preferred_element_type=jnp.float32
            )
            + jnp.einsum("thr,jr->thj", query_rot, rot_block, preferred_element_type=jnp.float32)
        ) * attn_scale
        key_segment = (first_key + jnp.arange(block_rows, dtype=jnp.int32)) // SEG
        allowed = key_segment[None, None, :] <= query_segment[:, None, None]
        peak_new = jnp.maximum(peak_old, jnp.max(jnp.where(allowed, scores, -1e30), axis=-1))
        weights = jnp.where(allowed, jnp.exp(scores - peak_new[..., None]), 0.0)
        rescale = jnp.exp(peak_old - peak_new)
        denom_new = denom_old * rescale + jnp.sum(weights, axis=-1)
        accum_new = accum_old * rescale[..., None] + jnp.einsum(
            "thj,jk->thk",
            weights.astype(jnp.bfloat16),
            latent_block,
            preferred_element_type=jnp.float32,
        )
        return (peak_new, denom_new, accum_new)

    starting = (
        jnp.full((tok_rows, local_heads), -1e30, jnp.float32),
        jnp.zeros((tok_rows, local_heads), jnp.float32),
        jnp.zeros((tok_rows, local_heads, KVL), jnp.float32),
    )
    latent_piece = lax.all_gather(latent, "sp", axis=0, tiled=True)
    rot_piece = lax.all_gather(key_rot, "sp", axis=0, tiled=True)
    piece_rows = latent_piece.shape[0]
    splits = max(1, piece_rows // 512)
    while piece_rows % splits:
        splits = splits - 1
    block_rows = piece_rows // splits

    def visit(state, block_index):
        block_begin = block_index * block_rows
        latent_block = lax.dynamic_slice_in_dim(latent_piece, block_begin, block_rows, 0)
        rot_block = lax.dynamic_slice_in_dim(rot_piece, block_begin, block_rows, 0)
        updated = lax.cond(
            block_begin // SEG <= last_segment,
            lambda inner: key_block(inner, latent_block, rot_block, block_begin),
            lambda inner: inner,
            state,
        )
        return (updated, None)

    peak, denom, accum = lax.scan(visit, starting, jnp.arange(splits, dtype=jnp.int32))[0]
    attended = (accum / denom[..., None]).astype(jnp.bfloat16)
    head_out = jnp.einsum(
        "thk,khv->thv",
        attended,
        value_up_weight.reshape(KVL, local_heads, VD),
        preferred_element_type=jnp.float32,
    )
    normed_heads = rms_scale(head_out, head_gain.reshape(local_heads, VD))
    attn_y = normed_heads.astype(jnp.bfloat16).reshape(tok_rows, local_heads * VD)
    share_rows = tok_rows // count_tp
    conv_all, attn_all = (
        lax.all_gather(conv_y, "fs", axis=0, tiled=True),
        lax.all_gather(attn_y, "fs", axis=0, tiled=True),
    )
    conv_sorted = (
        conv_all.reshape(count_fs, count_tp, share_rows, -1)
        .transpose(1, 0, 2, 3)
        .reshape(count_fs * tok_rows, -1)
    )
    attn_sorted = (
        attn_all.reshape(count_fs, count_tp, share_rows, -1)
        .transpose(1, 0, 2, 3)
        .reshape(count_fs * tok_rows, -1)
    )
    conv_cols_sp, attn_cols_sp = (
        lax.all_gather(conv_out_weight, "sp", axis=1, tiled=True),
        lax.all_gather(attn_out_weight, "sp", axis=1, tiled=True),
    )
    col_sums = lax.psum_scatter(
        (
            jnp.dot(conv_sorted, conv_cols_sp, preferred_element_type=jnp.float32)
            + jnp.dot(attn_sorted, attn_cols_sp, preferred_element_type=jnp.float32)
        ).astype(jnp.bfloat16),
        "tp",
        scatter_dimension=0,
        tiled=True,
    )
    col_piece = conv_cols_sp.shape[1] // count_sp
    outgoing = col_sums.reshape(count_fs, share_rows, count_sp * col_piece)
    arrived = lax.all_to_all(outgoing, "fs", split_axis=0, concat_axis=2, tiled=True)
    result = (
        arrived.reshape(share_rows, count_fs, count_sp, col_piece)
        .transpose(0, 2, 1, 3)
        .reshape(share_rows, count_fs * count_sp * col_piece)
    )
    return result[None]


MESH = pl.DeviceIdType.MESH


class Place:
    def __init__(self):
        self.z = lax.axis_index("sp")
        self.f = lax.axis_index("fs")
        self.c = lax.axis_index("tp")

    def to(self, z=None, f=None, c=None):
        return {
            "sp": self.z if z is None else z,
            "fs": self.f if f is None else f,
            "tp": self.c if c is None else c,
        }


def flip(index, bit):
    digit = (index // bit) % 2
    return index + bit * (1 - 2 * digit)


def remote(src, dst, send, recv, device):
    return pltpu.make_async_remote_copy(
        src_ref=src, dst_ref=dst, send_sem=send, recv_sem=recv, device_id=device, device_id_type=MESH
    )


def greet(devices):
    barrier = pltpu.get_barrier_semaphore()
    for device in devices:
        pl.semaphore_signal(barrier, inc=1, device_id=device, device_id_type=MESH)
    pl.semaphore_wait(barrier, len(devices))


def orders(n):
    columns = sorted(range(n), key=lambda g: (max(g, n - 1 - g), g))
    arrival, steps, passes = [], [], []
    slots = {}
    for z in (0, n - 1):
        by = [abs(z - d) for d in range(n)]
        g = columns
        sent = [(by[d], g[k]) for d, k in ((1, 0), (1, 1), (2, 0), (2, 1), (3, 0), (3, 1), (3, 2), (3, 3), (2, 2), (2, 3), (1, 2), (1, 3))]
        slots[z] = sent
    for z in range(n):
        end = 0 if 2 * z < n else n - 1
        near = sorted((d for d in range(n) if d != z), key=lambda d: (abs(d - z), abs(d - end)))
        arrival.append([z] + near)
        if z == end:
            steps.append(slots[z] + [(z, g) for g in columns])
            passes.append([(z, 0)])
            continue
        opposite = n - 1 - end
        seen = [(i, step) for i, step in enumerate(slots[end]) if step[0] not in (z, end)]
        seen += [(i + 2.2, step) for i, step in enumerate(slots[opposite]) if step[0] == end]
        passes.append([step for _, step in sorted(seen)])
        steps.append([(d, g) for g in columns for d in near + [z]])
    first_column, first_block = [], []
    for listed in steps:
        blocks_seen, columns_seen, at_column, at_block = set(), set(), [], []
        for d, g in listed:
            at_column.append(n if g in columns_seen else columns.index(g))
            at_block.append(0 if d in blocks_seen else 1)
            columns_seen.add(g)
            blocks_seen.add(d)
        first_column.append(at_column)
        first_block.append(at_block)
    split = lambda table, i: [[pair[i] for pair in row] for row in table]
    return arrival, columns, split(steps, 0), split(steps, 1), first_column, first_block, split(passes, 0), split(passes, 1)


def layer_kernel(
    n,
    order,
    tok_in,
    mix_gain_in,
    lat_gain_in,
    head_gain_in,
    taps_in,
    cb,
    cc,
    cv,
    qw,
    qr,
    lw,
    krw_in,
    key_up_in,
    value_up_in,
    co,
    ao,
    out,
    tok,
    normed,
    win,
    wout,
    wlat,
    lat,
    krot,
    gain,
    krw,
    taps,
    lat_gain,
    key_up,
    value_up,
    head_gain,
    gate,
    prod,
    q_nope,
    q_rot,
    keys,
    values,
    cosine,
    sine,
    part,
    pair,
    moving,
    fetched,
    wsem,
    lsem,
    tsem,
    psem,
    latsem,
    ssem,
    pairsem,
    zsem,
    gone,
    mix,
):
    here = Place()
    z, f, c = here.z, here.f, here.c
    fx, fy = flip(f, 1), flip(f, 2)
    other = 1 - c
    is_end = (z == 0) | (z == n - 1)
    near = jnp.where(2 * z < n, -1, 1)
    sides = (near, -near)
    rows = cb.shape[0]
    members = (cb, cc, cv, qw, qr)
    widths = [m.shape[1] // n for m in members]
    starts = [sum(widths[:i]) for i in range(len(widths))]
    lat_half = lw.shape[1] // 2
    tr = tok_in.shape[1]
    hr = tr // 2
    length = n * tr
    outs = (co, ao)
    heights = [m.shape[0] // n for m in outs]
    tops = [sum(heights[:i]) for i in range(len(heights))]
    out_cols = co.shape[1]
    head_rows = prod.shape[0] - length

    steps = [(1 + j, s) for j in range(n - 1) for s in (-1, 1)]

    def chosen(table, t):
        found = jnp.int32(0)
        for zz in range(n):
            for tt in range(len(table[zz])):
                found = jnp.where((z == zz) & (t == tt), table[zz][tt], found)
        return found

    def arrive_at(t):
        return chosen(order[0], t)

    def packed(table, bits):
        words = []
        for row in table:
            word = sum(v << (bits * t) for t, v in enumerate(row))
            words.append(word - (1 << 32) if word >= 1 << 31 else word)
        mine = jnp.int32(words[0])
        for zz in range(1, n):
            mine = jnp.where(z == zz, jnp.int32(words[zz]), mine)
        return lambda t: jnp.right_shift(mine, bits * t) & ((1 << bits) - 1)

    step_block, step_column = packed(order[2], 2), packed(order[3], 2)
    column_opens = packed([[int(k < n) for k in row] for row in order[4]], 1)
    block_opens = packed(order[5], 1)
    pass_block, pass_column = packed(order[6], 2), packed(order[7], 2)
    column_at = packed([order[1]] * n, 2)

    greet(
        [here.to(z=lax.rem(z + j, n)) for j in range(1, n)]
        + [here.to(f=fx), here.to(f=fy), here.to(c=other)]
    )

    def in_block(zs, fs):
        return win.at[pl.ds(pl.multiple_of((zs * 4 + fs) * rows, rows), rows), :]

    def out_block(zs, fs):
        return wout.at[:, pl.ds(pl.multiple_of((zs * 4 + fs) * out_cols, out_cols), out_cols)]

    def low_block(zs, fs):
        return wlat.at[pl.ds(pl.multiple_of((zs * 4 + fs) * rows, rows), rows), :]

    blocks = (in_block, out_block, low_block)

    def pieces(kind, dest):
        found = []
        if kind == 0:
            dst = (z * 4 + f) * rows
            for m, w, s in zip(members, widths, starts):
                src = m.at[:, pl.ds(pl.multiple_of(dest * w, w), w)]
                found.append((src, win.at[pl.ds(pl.multiple_of(dst, rows), rows), pl.ds(s, w)]))
        elif kind == 1:
            dst = (z * 4 + f) * out_cols
            for m, h, s in zip(outs, heights, tops):
                src = m.at[pl.ds(pl.multiple_of(dest * h, h), h), :]
                found.append((src, wout.at[pl.ds(s, h), pl.ds(pl.multiple_of(dst, out_cols), out_cols)]))
        else:
            found.append((lw.at[:, pl.ds(pl.multiple_of(c * lat_half, lat_half), lat_half)], low_block(z, f)))
        return found

    def send_own(kind):
        for src, dst in pieces(kind, z):
            remote(src, dst, gone.at[kind], wsem.at[kind, 1, z], here.to(f=fx)).start()
            remote(src, dst, gone.at[kind], wsem.at[kind, 2, z], here.to(f=fy)).start()
            pltpu.make_async_copy(src, dst, lsem.at[kind]).start()

    def can(sign):
        return (z + sign >= 0) & (z + sign < n)

    def within(zs):
        return (zs >= 0) & (zs < n)

    def reached(distance, sign):
        dest = z + sign * distance
        if distance == 1:
            return within(dest)
        return (dest > 0) & (dest < n - 1)

    def serves(sign):
        return z + sign == jnp.where(sign > 0, n - 1, 0)

    def send_z(kind, distance, sign):
        dest = z + sign * distance

        @pl.when(reached(distance, sign) if kind == 2 else within(dest))
        def _():
            for src, dst in pieces(kind, dest):
                remote(src, dst, gone.at[kind], wsem.at[kind, 0, z], here.to(z=dest)).start()

    def plane_copy(kind, zs, role, fs, to):
        block = blocks[kind](zs, fs)
        return remote(block, block, gone.at[kind], wsem.at[kind, role, zs], here.to(f=to))

    def end_copy(zs, sign):
        block = low_block(zs, f)
        return remote(block, block, gone.at[2], wsem.at[2, 0, zs], here.to(z=z + sign))

    def relay_z(kind, distance, sign):
        zs = z + sign * distance

        @pl.when(within(zs))
        def _():
            block = blocks[kind](zs, f)
            remote(block, block, gone.at[kind], wsem.at[kind, 0, zs], here.to(z=zs)).wait_recv()
            if kind == 2:
                pl.when(serves(-sign))(lambda: end_copy(zs, -sign).start())
            plane_copy(kind, zs, 1, f, fx).start()
            plane_copy(kind, zs, 2, f, fy).start()

    def relay_plane(kind, zs):
        plane_copy(kind, zs, 1, fx, fx).wait_recv()

        @pl.when(zs % 2 == 0)
        def _():
            plane_copy(kind, zs, 3, fx, fy).start()

        plane_copy(kind, zs, 2, fy, fy).wait_recv()

        @pl.when(zs % 2 == 1)
        def _():
            plane_copy(kind, zs, 3, fy, fx).start()

    def relay_done(kind, zs):
        plane_copy(kind, zs, 3, flip(fx, 2), fx).wait_recv()

    def tok_block(owner, zs, i):
        return tok.at[owner, pl.ds(pl.multiple_of(zs * tr + i * hr, hr), hr), :]

    def half_at(sign, i):
        return jnp.where(sign > 0, 1 - i, i)

    own_tok = [tok_in.at[0, i * hr : (i + 1) * hr, :] for i in range(2)]

    def tok_copy(zs, sign, hop, i, src=None):
        block = tok_block(c, zs, i)
        return remote(
            block if src is None else src, block, gone.at[3], tsem.at[zs, i], here.to(z=z + sign)
        )

    def partner_copy(zs, owner, i, src=None):
        block = tok_block(owner, zs, i)
        return remote(
            block if src is None else src, block, gone.at[4], psem.at[zs, i], here.to(c=other)
        )

    def own_copy(i):
        return pltpu.make_async_copy(own_tok[i], tok_block(c, z, i), lsem.at[3 + i])

    channels = widths[0]
    heads = widths[3] // NOPE
    rot_w = widths[4]
    share = tr // 2

    def columns_of(array, width):
        return array.at[:, pl.ds(pl.multiple_of(z * width, width), width)]

    small = [
        (mix_gain_in, gain.at[0:1, :]),
        (krw_in, krw.at[0:ROPE, :]),
        (krw_in, krw.at[ROPE : 2 * ROPE, :]),
        (taps_in, taps),
        (lat_gain_in, lat_gain.at[0:1, :]),
        (columns_of(key_up_in, heads * NOPE), key_up),
        (columns_of(value_up_in, heads * VD), value_up),
        (columns_of(head_gain_in, heads * VD), head_gain.at[0:1, :]),
    ]

    send_own(2)
    for distance, sign in steps:
        send_z(2, distance, sign)
    for i in range(2):
        partner_copy(z, c, i, own_tok[i]).start()
        own_copy(i).start()
    send_own(0)
    middle = jnp.logical_not(is_end)

    def send_far_first(kind):
        for distance in (2, 1):
            for sign in (-1, 1):
                send_z(kind, distance, sign)

    def send_near_first(kind):
        for distance, sign in steps:
            send_z(kind, distance, sign)

    def send_toks():
        for sign in (-1, 1):
            for i in (1, 0) if sign > 0 else (0, 1):
                pl.when(can(sign))(lambda sign=sign, i=i: tok_copy(z, sign, 0, i, own_tok[i]).start())

    pl.when(middle)(lambda: send_far_first(0))

    @pl.when(is_end)
    def _():
        send_near_first(0)
        send_toks()


    for i, (src, dst) in enumerate(small):
        pltpu.make_async_copy(src, dst, ssem.at[i]).start()

    def relay_tok(distance, sign, i):
        zs = z + sign * distance

        @pl.when(within(zs))
        def _():
            half = half_at(-sign, i)
            tok_copy(zs, -sign, distance - 1, half).wait_recv()
            if distance < n - 1:
                pl.when(can(-sign))(lambda: tok_copy(zs, -sign, distance, half).start())
            partner_copy(zs, c, half).start()

    def relay_toks(distance, sides=sides):
        for sign in sides:
            for i in range(2):
                relay_tok(distance, sign, i)

    def each_zs(fn):
        def body(i, carry):
            fn(lax.rem(z + i, n))
            return carry

        lax.fori_loop(0, n, body, 0)

    def at_distance(distance, fn):
        for sign in sides:
            zs = z + sign * distance
            pl.when(within(zs))(lambda zs=zs: fn(zs))

    lane = lax.broadcasted_iota(jnp.int32, (tr, rot_w), 1)
    quarter = lane % (ROPE // 2)
    first_half = (lane % ROPE) < ROPE // 2
    frequency = jnp.exp(quarter.astype(jnp.float32) * (-2.0 / ROPE * math.log(rope_theta)))

    def tables(i, carry):
        at = pl.ds(pl.multiple_of(i * tr, tr), tr)
        position = (i * tr + lax.broadcasted_iota(jnp.int32, (tr, rot_w), 0)).astype(jnp.float32)
        angle = position * frequency
        cosine[at, :] = jnp.cos(angle)
        turned = jnp.sin(angle)
        sine[at, :] = jnp.where(first_half, -turned, turned)
        return carry

    lax.fori_loop(0, n, tables, 0)
    prod[0:head_rows, :] = jnp.zeros((head_rows, channels), prod.dtype)

    def rotated(x, at):
        low_half = (lax.broadcasted_iota(jnp.int32, x.shape, 1) % ROPE) < ROPE // 2
        swapped = jnp.where(low_half, pltpu.roll(x, rot_w - ROPE // 2, 1), pltpu.roll(x, ROPE // 2, 1))
        return (x * cosine[at, :] + swapped * sine[at, :]).astype(jnp.bfloat16)

    for i, (src, dst) in enumerate(small):
        pltpu.make_async_copy(src, dst, ssem.at[i]).wait()
    wide = tok.shape[2]

    def half_rows(zs, i):
        return pl.ds(pl.multiple_of(zs * tr + i * hr, hr), hr)

    def norm_half(zs, i):
        partner_copy(zs, other, i).wait_recv()
        at = half_rows(zs, i)
        first = tok[0, at, :].astype(jnp.float32)
        second = tok[1, at, :].astype(jnp.float32)
        mean = (
            jnp.sum(first * first, axis=-1, keepdims=True) + jnp.sum(second * second, axis=-1, keepdims=True)
        ) / (2 * wide)
        scale = lax.rsqrt(mean + norm_epsilon)
        normed[at, 0:wide] = (first * scale * gain[0:1, 0:wide]).astype(jnp.bfloat16)
        normed[at, wide : 2 * wide] = (second * scale * gain[0:1, wide : 2 * wide]).astype(jnp.bfloat16)

    def norm_block(zs):
        def body(i, carry):
            norm_half(zs, i)
            return carry

        lax.fori_loop(0, 2, body, 0)

    def rows_of(zs):
        return pl.ds(pl.multiple_of(zs * tr, tr), tr)

    def lat_block(zs, owner):
        return lat.at[owner, rows_of(zs), :]

    def rot_block(zs, owner):
        return krot.at[pl.ds(pl.multiple_of(zs * tr + owner * hr, hr), hr), :]

    shared = (lat_block, rot_block)

    def lat_copy(k, dest):
        block = shared[k](z, c)
        return remote(block, block, gone.at[5 + k], latsem.at[k, 0, z], here.to(z=dest))

    def lat_arrival(k, zs):
        block = shared[k](zs, c)
        return remote(block, block, gone.at[5 + k], latsem.at[k, 0, zs], here.to(z=zs))

    def lat_forward(k, zs, sign):
        block = shared[k](zs, c)
        return remote(block, block, gone.at[5 + k], latsem.at[k, 0, zs], here.to(z=z + sign))

    def lat_partner(k, zs, owner):
        block = shared[k](zs, owner)
        return remote(block, block, gone.at[5 + k], latsem.at[k, 1, zs], here.to(c=other))

    def relay_lat(distance, sides=sides):
        for sign in sides:
            zs = z + sign * distance

            @pl.when(within(zs))
            def _(zs=zs, sign=sign):
                for k in range(2):
                    lat_arrival(k, zs).wait_recv()
                    pl.when(serves(-sign))(lambda k=k: lat_forward(k, zs, -sign).start())
                    lat_partner(k, zs, c).start()

    def own_latents():
        at = rows_of(z)
        block = normed[at, :]
        lat[c, at, :] = jnp.dot(block, wlat[...], preferred_element_type=jnp.float32).astype(jnp.bfloat16)
        key_raw = lax.dot_general(
            block, krw[...], (((1,), (1,)), ((), ())), preferred_element_type=jnp.float32
        )
        krot[at, :] = rotated(key_raw, at)

    def relay_weights_z(distance):
        for sign in (-1, 1):
            for kind in (0, 1):
                relay_z(kind, distance, sign)

    def relay_weights_plane(zs):
        for kind in (0, 1):
            relay_plane(kind, zs)

    def relay_all_z(kind, distance):
        for sign in sides:
            relay_z(kind, distance, sign)

    def diagonals(kind, distance):
        at_distance(distance, lambda zs: relay_plane(kind, zs))

    def share_latents():
        pltpu.make_async_copy(low_block(z, f), low_block(z, f), lsem.at[2]).wait()
        each_zs(lambda zs: relay_done(2, zs))
        own_latents()
        for distance, sign in steps:
            dest = z + sign * distance

            @pl.when(reached(distance, sign))
            def _(dest=dest):
                for k in range(2):
                    lat_copy(k, dest).start()

        lat_partner(0, z, c).start()

    relay_all_z(2, 1)
    relay_plane(2, z)
    for i in range(2):
        own_copy(i).wait()
    norm_block(z)

    @pl.when(is_end)
    def _():
        relay_plane(0, z)
        send_own(1)
        for distance in range(2, n):
            relay_all_z(2, distance)
        relay_all_z(0, 1)
        for distance in range(1, n):
            diagonals(2, distance)
        relay_all_z(0, 2)
        relay_all_z(0, 3)
        share_latents()
        diagonals(0, 1)
        send_near_first(1)
        diagonals(0, 2)
        diagonals(0, 3)
        relay_lat(1)
        relay_toks(1)

    @pl.when(middle)
    def _():
        relay_all_z(2, 2)
        relay_plane(0, z)
        diagonals(2, 1)
        diagonals(2, 2)
        relay_z(0, 1, near)
        relay_all_z(0, 2)
        share_latents()
        send_toks()
        send_far_first(1)
        relay_plane(0, z + near)
        relay_z(0, 1, -near)
        diagonals(0, 2)
        relay_lat(1, sides[1:])
        relay_toks(1, sides[:1])
        send_own(1)
        relay_plane(0, z - near)
        relay_lat(1, sides[:1])
        relay_lat(2)
        relay_toks(1, sides[1:])

    pltpu.make_async_copy(in_block(z, f), in_block(z, f), lsem.at[0]).wait()
    each_zs(lambda zs: relay_done(0, zs))

    @pl.when(is_end)
    def _():
        pl.when(z == 0)(lambda: relay_all_z(1, 1))
        relay_all_z(1, 2)
        pl.when(z != 0)(lambda: relay_all_z(1, 1))

    pl.when(middle)(lambda: relay_z(1, 1, -near))
    norm_block(arrive_at(1))

    def project_rows(first_row, count):
        at = pl.ds(pl.multiple_of(first_row, hr), count)
        joined = jnp.dot(normed[at, :], win[...], preferred_element_type=jnp.float32)
        gates = joined[:, channels : 3 * channels].astype(jnp.bfloat16).astype(jnp.float32)
        gate[at, :] = joined[:, 0:channels].astype(jnp.bfloat16)
        below = pl.ds(pl.multiple_of(first_row + head_rows, head_rows), count)
        prod[below, :] = (gates[:, 0:channels] * gates[:, channels : 2 * channels]).astype(jnp.bfloat16)
        start = 3 * channels
        q_nope[at, :] = joined[:, start : start + heads * NOPE].astype(jnp.bfloat16)
        q_rot[at, :] = rotated(joined[:, start + heads * NOPE :], at)

    def project_half(zs, i):
        project_rows(zs * tr + i * hr, hr)

    def project_arrived(t, carry):
        project_rows(arrive_at(t) * tr, tr)
        return carry

    lax.fori_loop(0, 2, project_arrived, 0)

    @pl.when(is_end)
    def _():
        relay_lat(2)
        relay_lat(3)


    def lat_waits(zs):
        lat_partner(0, zs, other).wait_recv()
        pl.when(zs != z)(lambda: lat_partner(1, zs, other).wait_recv())

    def expand(i, carry):
        lat_waits(i)
        at = rows_of(i)
        raw = jnp.concatenate([lat[0, at, :], lat[1, at, :]], axis=1).astype(jnp.float32)
        mean = jnp.mean(raw * raw, axis=-1, keepdims=True)
        low = (raw * lax.rsqrt(mean + norm_epsilon) * lat_gain[0:1, :]).astype(jnp.bfloat16)
        wide_keys = jnp.dot(low, key_up[...], preferred_element_type=jnp.float32).astype(jnp.bfloat16)
        key_rot = krot[at, :]
        for h in range(heads):
            keys[h, at, 0:NOPE] = wide_keys[:, h * NOPE : (h + 1) * NOPE]
            keys[h, at, NOPE:] = key_rot
        values[at, :] = jnp.dot(low, value_up[...], preferred_element_type=jnp.float32).astype(jnp.bfloat16)
        return carry

    lax.fori_loop(0, n, expand, 0)
    relay_plane(1, order[1][0])
    pl.when(is_end)(lambda: relay_all_z(1, 3))

    @pl.when(middle)
    def _():
        relay_z(1, 1, near)
        relay_all_z(1, 2)
        relay_toks(2)


    shift = SEG.bit_length() - 1
    row_index = lax.broadcasted_iota(jnp.int32, (tr, length), 0)
    key_segment = jnp.right_shift(lax.broadcasted_iota(jnp.int32, (tr, length), 1), shift)
    own_lanes = lane // ROPE
    own_channels = pl.ds(pl.multiple_of(z * channels, channels), channels)

    def features(dest):
        at = rows_of(dest)
        allowed = key_segment <= jnp.right_shift(row_index + dest * tr, shift)
        padded = prod[pl.ds(pl.multiple_of(dest * tr, head_rows), tr + head_rows), :].astype(jnp.float32)
        convolved = (
            taps[0:1, own_channels] * pltpu.roll(padded, 2, 0)[head_rows:]
            + taps[1:2, own_channels] * pltpu.roll(padded, 1, 0)[head_rows:]
            + taps[2:3, own_channels] * padded[head_rows:]
        )
        outputs = [(gate[at, :].astype(jnp.float32) * convolved).astype(jnp.bfloat16)]
        rot = q_rot[at, :]
        for h in range(heads):
            query = jnp.concatenate(
                [
                    q_nope[at, h * NOPE : (h + 1) * NOPE],
                    jnp.where(own_lanes == h, rot, jnp.zeros_like(rot)),
                ],
                axis=1,
            )
            scores = lax.dot_general(
                query, keys[h], (((1,), (1,)), ((), ())), preferred_element_type=jnp.float32
            ) * (NOPE + ROPE) ** (-0.5)
            scores = jnp.where(allowed, scores, -1e30)
            weights = jnp.exp(scores - jnp.max(scores, axis=-1, keepdims=True))
            denom = jnp.sum(weights, axis=-1, keepdims=True)
            head_out = (
                jnp.dot(
                    weights.astype(jnp.bfloat16),
                    values[:, h * VD : (h + 1) * VD],
                    preferred_element_type=jnp.float32,
                )
                / denom
            )
            mean = jnp.mean(head_out * head_out, axis=-1, keepdims=True)
            gained = head_out * lax.rsqrt(mean + norm_epsilon) * head_gain[0:1, h * VD : (h + 1) * VD]
            outputs.append(gained.astype(jnp.bfloat16))
        mix[dest] = jnp.concatenate(outputs, axis=1)

    piece_w = wout.shape[1] // n

    def cut(g):
        return pl.ds(pl.multiple_of(g * piece_w, piece_w), piece_w)

    def own_rows():
        return pl.ds(pl.multiple_of(c * share, share), share)

    def pair_copy(dest, g):
        theirs = pl.ds(pl.multiple_of(other * share, share), share)
        return remote(
            part.at[dest, theirs, cut(g)],
            pair.at[dest, :, cut(g)],
            gone.at[7],
            pairsem.at[dest, g],
            here.to(c=other),
        )

    def line_copy(d, dest, g, target):
        row = jnp.where((dest == target) & (d == 1), n, dest)
        return remote(
            moving.at[dest, :, cut(g)],
            fetched.at[d, dest, :, cut(g)],
            gone.at[8],
            zsem.at[row, g],
            here.to(z=z + 2 * d - 1),
        )

    def line_send(d, dest, g):
        line_copy(d, dest, g, z + 2 * d - 1).start()

    def summed(dest, g):
        kept = part[dest, own_rows(), cut(g)]
        return kept.astype(jnp.float32) + pair[dest, :, cut(g)].astype(jnp.float32)

    def toward(dest):
        return jnp.where(dest > z, 1, 0)

    def pass_first(dest, g):
        pair_copy(dest, g).wait_recv()
        moving[dest, :, cut(g)] = summed(dest, g).astype(jnp.bfloat16)
        line_send(toward(dest), dest, g)

    def pass_on(dest, g):
        d = toward(dest)
        pair_copy(dest, g).wait_recv()
        line_copy(d, dest, g, z).wait_recv()
        moving[dest, :, cut(g)] = (
            summed(dest, g) + fetched[d, dest, :, cut(g)].astype(jnp.float32)
        ).astype(jnp.bfloat16)
        line_send(d, dest, g)

    def process_half(zs, i):
        norm_half(zs, i)
        project_half(zs, i)

    @pl.when(middle)
    def _():
        def rest(t, carry):
            norm_block(arrive_at(t))
            return project_arrived(t, carry)

        lax.fori_loop(2, n, rest, 0)

    half_first = half_at(-sides[1], 0)
    half_last = 1 - half_first

    @pl.when(is_end)
    def _():
        relay_tok(2, sides[1], 0)
        relay_tok(2, sides[1], 1)
        process_half(arrive_at(2), half_first)

    relay_plane(1, order[1][1])


    second_block, third_block = [i for i, opens in enumerate(order[5][0]) if opens][1:3]

    def step(i, carry):
        dest, g = step_block(i), step_column(i)
        before = jnp.maximum(i - 1, 0)

        def pass_before():
            pass_first(step_block(before), step_column(before))

        early = (i == 1) | (i == 2)
        passes = is_end & (i >= 1) & (i <= n * (n - 1))
        pl.when(passes & early)(pass_before)
        pl.when(block_opens(i) == 1)(lambda: features(dest))
        pl.when(passes & (i == third_block))(pass_before)

        @pl.when(column_opens(i) == 1)
        def _():
            pl.when(g == z)(lambda: pltpu.make_async_copy(out_block(z, f), out_block(z, f), lsem.at[1]).wait())
            relay_done(1, g)

        part[dest, :, cut(g)] = jnp.dot(
            mix[dest], wout[:, cut(g)], preferred_element_type=jnp.float32
        ).astype(jnp.bfloat16)
        pair_copy(dest, g).start()
        pl.when(passes & jnp.logical_not(early | (i == third_block)))(pass_before)
        pl.when(is_end & (i == 0))(lambda: process_half(arrive_at(2), half_last))
        for k in range(2, n):
            pl.when(i == k - 2)(lambda k=k: relay_plane(1, order[1][k]))

        @pl.when(is_end)
        def _():
            pl.when(i == 0)(lambda: relay_tok(3, sides[1], 0))
            pl.when(i == third_block - 3)(lambda: relay_tok(3, sides[1], 1))

            @pl.when((i == 1) | (i == third_block - 2))
            def _():
                process_half(arrive_at(3), jnp.where(i == 1, half_first, half_last))

        return carry

    lax.fori_loop(0, n * n, step, 0)

    @pl.when(middle)
    def _():
        def passing(i, carry):
            pass_on(pass_block(i), pass_column(i))
            return carry

        lax.fori_loop(0, n * (n - 1), passing, 0)

    low, high = z > 0, z < n - 1

    def finish(turn, carry):
        g = column_at(turn)
        pair_copy(z, g).wait_recv()
        pl.when(low)(lambda: line_copy(1, z, g, z).wait_recv())
        pl.when(high)(lambda: line_copy(0, z, g, z).wait_recv())

        @pl.when(middle)
        def _():
            out[:, cut(g)] = (
                summed(z, g)
                + fetched[1, z, :, cut(g)].astype(jnp.float32)
                + fetched[0, z, :, cut(g)].astype(jnp.float32)
            ).astype(jnp.bfloat16)

        @pl.when(is_end)
        def _():
            d = jnp.where(low, 1, 0)
            out[:, cut(g)] = (
                summed(z, g) + fetched[d, z, :, cut(g)].astype(jnp.float32)
            ).astype(jnp.bfloat16)

        return carry

    lax.fori_loop(0, n, finish, 0)

    def sent(sem, ref):
        pltpu.make_async_copy(ref, ref, gone.at[sem]).wait()

    def by_place(sem, at_ends, at_middle):
        pl.when(is_end)(lambda: sent(sem, at_ends))
        pl.when(middle)(lambda: sent(sem, at_middle))

    whole = 4 * n - 1
    sent(0, win.at[0 : whole * rows, :])
    sent(1, wout.at[:, 0 : whole * out_cols])
    by_place(2, wlat.at[0 : (3 * n + 2) * rows, :], wlat.at[0 : 4 * n * rows, :])
    by_place(3, tok.at[:, 0:hr, :], tok.at[:, 0 : (n + 1) * hr, :])
    sent(4, tok.at[0])
    by_place(5, lat.at[:, 0 : 3 * tr, :], lat)
    by_place(6, krot.at[0 : 5 * hr, :], krot.at[0 : 7 * hr, :])
    sent(7, pair)
    sent(8, moving.at[0 : n - 1])


def split_shards(
    tokens,
    mix_gain,
    conv_b_weight,
    conv_c_weight,
    conv_v_weight,
    conv_taps,
    query_weight,
    query_rope_weight,
    latent_weight,
    key_rope_weight,
    latent_gain,
    key_up_weight,
    value_up_weight,
    head_gain,
    conv_out_weight,
    attn_out_weight,
):
    n = lax.axis_size("sp")
    tr = tokens.shape[1]
    wide = tokens.shape[2]
    length = n * tr
    features = 2 * wide
    heads = query_weight.shape[1] // NOPE // n
    channels = conv_b_weight.shape[1] // n
    low_rank = latent_weight.shape[1]
    proj_w = 3 * channels + heads * (NOPE + ROPE)
    out_rows = (conv_out_weight.shape[0] + attn_out_weight.shape[0]) // n
    columns = attn_out_weight.shape[1] * n * 4
    share = tr // 2
    head_rows = 16
    bf16, f32 = jnp.bfloat16, jnp.float32
    dma = pltpu.SemaphoreType.DMA
    operands = (
        tokens,
        mix_gain[None],
        latent_gain[None],
        head_gain[None],
        conv_taps,
        conv_b_weight,
        conv_c_weight,
        conv_v_weight,
        query_weight,
        query_rope_weight,
        latent_weight,
        key_rope_weight.T,
        key_up_weight,
        value_up_weight,
        conv_out_weight,
        attn_out_weight,
    )
    result = pl.pallas_call(
        functools.partial(layer_kernel, n, orders(n)),
        out_shape=jax.ShapeDtypeStruct((share, columns), bf16),
        in_specs=[pl.BlockSpec(memory_space=pltpu.HBM)] * 16,
        out_specs=pl.BlockSpec(memory_space=pltpu.VMEM),
        scratch_shapes=[
            pltpu.VMEM((2, length, wide), bf16),
            pltpu.VMEM((length, features), bf16),
            pltpu.VMEM((features, proj_w), bf16),
            pltpu.VMEM((out_rows, columns), bf16),
            pltpu.VMEM((features, low_rank // 2), bf16),
            pltpu.VMEM((2, length, low_rank // 2), bf16),
            pltpu.VMEM((length, 2 * ROPE), bf16),
            pltpu.VMEM((8, features), f32),
            pltpu.VMEM((2 * ROPE, features), bf16),
            pltpu.VMEM(conv_taps.shape, f32),
            pltpu.VMEM((8, low_rank), f32),
            pltpu.VMEM((low_rank, heads * NOPE), bf16),
            pltpu.VMEM((low_rank, heads * VD), bf16),
            pltpu.VMEM((8, heads * VD), f32),
            pltpu.VMEM((length, channels), bf16),
            pltpu.VMEM((length + head_rows, channels), bf16),
            pltpu.VMEM((length, heads * NOPE), bf16),
            pltpu.VMEM((length, heads * ROPE), bf16),
            pltpu.VMEM((heads, length, NOPE + 2 * ROPE), bf16),
            pltpu.VMEM((length, heads * VD), bf16),
            pltpu.VMEM((length, heads * ROPE), f32),
            pltpu.VMEM((length, heads * ROPE), f32),
            pltpu.VMEM((n, tr, columns), bf16),
            pltpu.VMEM((n, share, columns), bf16),
            pltpu.VMEM((n, share, columns), bf16),
            pltpu.VMEM((2, n, share, columns), bf16),
            dma((3, 4, n)),
            dma((5,)),
            dma((n, 2)),
            dma((n, 2)),
            dma((2, 2, n)),
            dma((8,)),
            dma((n, n)),
            dma((n + 1, n)),
            dma((9,)),
            pltpu.VMEM((n, tr, out_rows), bf16),
        ],
        compiler_params=pltpu.CompilerParams(
            collective_id=0, has_side_effects=True, vmem_limit_bytes=40 * 1024 * 1024
        ),
        name="whole_layer",
    )(*(pltpu.with_memory_space_constraint(operand, pltpu.HBM) for operand in operands))
    return result[None]


def splits_well(mesh):
    n = mesh.shape["sp"]
    return n == 4 and mesh.shape["fs"] == 4 and mesh.shape["tp"] == 2


def shards(*arrays):
    n = lax.axis_size("sp")
    conv, query, rope, low_rank = (arrays[i].shape[1] for i in (2, 6, 7, 8))
    heads = query // NOPE
    even = heads == n * 128 // ROPE and all(w % (128 * n) == 0 for w in (conv, query, rope, low_rank))
    if even and arrays[0].shape[1] % 32 == 0 and arrays[15].shape[1] % 128 == 0:
        return split_shards(*arrays)
    return general_shards(*arrays)


def solution(mesh):
    return jax.shard_map(
        shards if splits_well(mesh) else general_shards,
        mesh=mesh,
        in_specs=(
            P("fs", "sp", "tp"),
            P(),
            P(("sp", "fs"), "tp"),
            P(("sp", "fs"), "tp"),
            P(("sp", "fs"), "tp"),
            P(None, "tp"),
            P(("sp", "fs"), "tp"),
            P(("sp", "fs"), "tp"),
            P(("sp", "fs"), None),
            P(),
            P(),
            P(None, "tp"),
            P(None, "tp"),
            P("tp"),
            P("tp", ("sp", "fs")),
            P("tp", ("sp", "fs")),
        ),
        out_specs=P("fs", ("sp", "tp"), None),
        check_vma=False,
    )
```
